128 devices in a mesh: fs: 16 (over z, y), tp: 8 (over x, core).
Axes of the slice: x: 4, y: 4, z: 4, core: 2. Of those that a mesh axis runs over, the one named last changes fastest.
Arguments:
- tokens: bfloat16 [8192, 4096], P('fs'), may hold values from -6 to 6
- norm_gain: float32 [4096], P('fs'), may hold values from 0.1 to 1.9
- gate_train: float32 [16, 4096, 1024], P(None, 'fs', 'tp'), may hold values from -0.09375 to 0.09375
- up_train: float32 [16, 4096, 1024], P(None, 'fs', 'tp'), may hold values from -0.09375 to 0.09375
- down_train: float32 [16, 1024, 4096], P(None, 'fs', 'tp'), may hold values from -0.1875 to 0.1875
- shared_gate_train: float32 [4096, 1024], P('fs', 'tp'), may hold values from -0.09375 to 0.09375
- shared_up_train: float32 [4096, 1024], P('fs', 'tp'), may hold values from -0.09375 to 0.09375
- shared_down_train: float32 [1024, 4096], P('fs', 'tp'), may hold values from -0.1875 to 0.1875
- route_expert: int32 [8192, 2], P('fs'), may hold values from 0 to 15, all different within a row; in each aligned block of 512 rows (0 to 511, 512 to 1023, ...) at most 96 rows name the same one
- route_weight: float32 [8192, 2], P('fs'), may hold values from 0.1 to 1
Outputs:
- expert_gate: bfloat16 [16, 4096, 1024], P('fs', None, 'tp')
- expert_up: bfloat16 [16, 4096, 1024], P('fs', None, 'tp')
- expert_down: bfloat16 [16, 1024, 4096], P('fs', 'tp')
- shared_gate: bfloat16 [4096, 1024], P(None, 'tp')
- shared_up: bfloat16 [4096, 1024], P(None, 'tp')
- shared_down: bfloat16 [1024, 4096], P('tp')
- mixed: bfloat16 [8192, 4096], P('fs', 'tp')
The draws below stay inside these ranges and needn't reach their ends.
Inputs may be any that keep to these rules, and one draw needn't show every extreme that they name: `route_expert`: each row names 2 different experts. Within each aligned block of 512 rows no expert is named by more than 96 rows, a bound that some block reaches in every draw.
All inputs are finite; a program needn't handle non-finite values.
Results may differ from the reference program's by a relative error of at most 0.015.
Values may be sent and summed in bfloat16 or wider, within the bound.
No kernel may reach another device: no remote copies, remote signals or barrier semaphores. Data moves between devices by JAX's collectives and lax.ppermute only.
A program may use at most 128 MiB of HBM per device.

```python
import math
import jax
import jax.numpy as jnp
import numpy as np
from jax import lax

D = 4096
H = 1024
HS = 1024
TOPK = 2
TOK_DEV = 512
EXPERTS = 16
CAP = 96
TOKENS = 8192
N_FS = 16
N_TP = 8


def levels(rng, dims, shards, low, top_value):
    loudness = 1.0
    for axis_at, shards_of in shards:
        draws = jax.random.uniform(jax.random.fold_in(jax.random.fold_in(rng, 6), axis_at), (shards_of,), jnp.float32, low / len(shards), top_value / len(shards))
        loudness = loudness * jnp.repeat(jnp.exp(draws), dims[axis_at] // shards_of).reshape((-1,) + (1,) * (len(dims) - 1 - axis_at))
    return loudness


def shared_out(key, own, number, rows, amount, top, reach, lean):
    sequence = jax.random.permutation(key, amount)
    crowded, ordinary = shares(amount, rows * top, reach, lean, True), shares(amount, rows * top, reach, lean, False)
    places = jnp.arange(amount)

    def named(sizes, rotation):
        used = int((sizes > 0).sum())
        fixed = max(1, used // 4)
        shifted = fixed + (places - fixed + rotation * (used - fixed)) % max(1, amount - fixed)
        return jnp.zeros((amount,), jnp.int32).at[sequence[jnp.where(places < fixed, places, shifted)]].set(jnp.asarray(sizes, jnp.int32))

    sizes = jnp.where(number % 4 == 0, named(crowded, number // 4), named(ordinary, number - number // 4 - 1))
    mixed = jax.random.permutation(jax.random.fold_in(own, 3), amount)
    giver, taker = mixed[0:amount // 2 * 2:2], mixed[1:amount // 2 * 2:2]
    margin = jnp.minimum(sizes[giver] - 1, reach - sizes[taker]) // 2
    margin = jnp.where((giver == sequence[0]) | (taker == sequence[0]) | (sizes[taker] == 0), 0, jnp.maximum(margin, 0))
    shifted = jax.random.randint(jax.random.fold_in(own, 4), (amount // 2,), 0, 1 << 20) % (margin + 1)
    sizes = sizes.at[giver].add(-shifted).at[taker].add(shifted)
    labels = jnp.searchsorted(jnp.cumsum(sizes), jnp.arange(rows * top), side="right").astype(jnp.int32)
    table = labels.reshape(top, rows).T
    table = table[jax.random.permutation(jax.random.fold_in(own, 1), rows)]
    rotation = jax.random.randint(jax.random.fold_in(own, 2), (rows, 1), 0, top)
    return jnp.take_along_axis(table, (jnp.arange(top)[None, :] + rotation) % top, axis=1)


def shares(amount, total, reach, skew, full):
    portions = [(1 << 20) // math.isqrt(standing ** skew) + 1 for standing in range(1, amount + 1)]
    largest = reach if full else min(reach, max(-(-total // amount), total * portions[0] // sum(portions)))
    least = 1 if total - largest >= amount - 1 else 0
    holding, surplus = [largest] + [least] * (amount - 1), total - largest - least * (amount - 1)
    while surplus > 0:
        free = [i for i in range(1, amount) if holding[i] < largest] or [i for i in range(1, amount) if holding[i] < reach]
        whole, left = sum([portions[i] for i in free]), surplus
        for i in free:
            more = min(reach - holding[i], max(1, left * portions[i] // whole), surplus)
            holding[i] = holding[i] + more
            surplus = surplus - more
    return np.array(holding)


def noise(own_key, extent, spread, limit, shards=(), kind=jnp.bfloat16):
    loudness = levels(own_key, extent, shards, -0.22, 0.18) if shards else 1.0
    array = jax.random.normal(own_key, extent, jnp.float32) * spread * loudness
    return jnp.minimum(jnp.maximum(array, -limit), limit).astype(kind)


def setup_inputs(seed: int = 0) -> dict:
    keys = jax.random.split(jax.random.key(seed), 11)
    tokens = noise(keys[0], (TOKENS, D), 1.0, 6.0, ((0, 16),))
    norm_gain = jnp.clip(1.0 + 0.18 * jax.random.normal(keys[1], (D,), jnp.float32), 0.1, 1.9)
    gate_train = noise(keys[2], (EXPERTS, D, H), D ** -0.5, 0.09375, ((1, 16), (2, 8)), jnp.float32)
    up_train = noise(keys[3], (EXPERTS, D, H), D ** -0.5, 0.09375, ((1, 16), (2, 8)), jnp.float32)
    down_train = noise(keys[4], (EXPERTS, H, D), H ** -0.5, 0.1875, ((1, 16), (2, 8)), jnp.float32)
    shared_gate_train = noise(keys[5], (D, HS), D ** -0.5, 0.09375, ((0, 16), (1, 8)), jnp.float32)
    shared_up_train = noise(keys[6], (D, HS), D ** -0.5, 0.09375, ((0, 16), (1, 8)), jnp.float32)
    shared_down_train = noise(keys[7], (HS, D), HS ** -0.5, 0.1875, ((0, 16), (1, 8)), jnp.float32)
    route_expert_keys = jax.random.split(jax.random.fold_in(keys[8], 1), TOKENS // TOK_DEV)
    route_expert_turns = jax.random.permutation(jax.random.fold_in(keys[8], 3), TOKENS // TOK_DEV)
    route_expert = jax.vmap(lambda own, number: shared_out(jax.random.fold_in(keys[8], 2), own, number, TOK_DEV, EXPERTS, TOPK, CAP, 1))(route_expert_keys, route_expert_turns).reshape((TOKENS, TOPK))
    route_weight = jnp.clip(jnp.exp(math.log(1.0) - 2.3025851 * jax.random.uniform(keys[9], (TOKENS, TOPK), jnp.float32) ** levels(keys[9], (TOKENS, TOPK), ((0, 16),), -0.2, 0.2)), 0.1, 1.0)
    return {"tokens": tokens, "norm_gain": norm_gain, "gate_train": gate_train, "up_train": up_train, "down_train": down_train, "shared_gate_train": shared_gate_train, "shared_up_train": shared_up_train, "shared_down_train": shared_down_train, "route_expert": route_expert, "route_weight": route_weight}


norm_eps = 1e-06

def expert_apply(rows, weight_gate, weight_up, weight_down, pieces):
    gate_vals = jnp.dot(rows, weight_gate, preferred_element_type=jnp.float32)
    up_vals = jnp.dot(rows, weight_up, preferred_element_type=jnp.float32)
    hidden = (jax.nn.silu(gate_vals) * up_vals).astype(jnp.bfloat16)
    step_width = hidden.shape[1] // pieces
    total = jnp.zeros((rows.shape[0], weight_down.shape[1]), jnp.float32)
    for block in range(pieces):
        term = jnp.dot(hidden[:, block * step_width:(block + 1) * step_width], weight_down[block * step_width:(block + 1) * step_width], preferred_element_type=jnp.float32)
        total = total + term.astype(jnp.bfloat16).astype(jnp.float32)
    return total

def reference(tokens, norm_gain, gate_train, up_train, down_train, shared_gate_train, shared_up_train, shared_down_train, route_expert, route_weight):
    expert_gate = (norm_gain[None, :, None] * gate_train).astype(jnp.bfloat16)
    expert_up = (norm_gain[None, :, None] * up_train).astype(jnp.bfloat16)
    expert_down = down_train.astype(jnp.bfloat16)
    shared_gate = (norm_gain[:, None] * shared_gate_train).astype(jnp.bfloat16)
    shared_up = (norm_gain[:, None] * shared_up_train).astype(jnp.bfloat16)
    shared_down = shared_down_train.astype(jnp.bfloat16)
    values = tokens.astype(jnp.float32)
    normed = (values * lax.rsqrt(lax.optimization_barrier(jnp.mean(values * values, axis=1, keepdims=True)) + norm_eps)).astype(jnp.bfloat16)
    pairs = route_expert.reshape(N_FS, TOK_DEV * TOPK)
    chosen = (pairs[:, :, None] == jnp.arange(EXPERTS, dtype=jnp.int32)[None, None, :]).astype(jnp.int32)
    earlier = (jnp.cumsum(chosen, axis=1) - chosen).astype(jnp.int32)
    slot = lax.optimization_barrier(jnp.sum(earlier * chosen, axis=2)).astype(jnp.int32)
    place = (jnp.arange(N_FS, dtype=jnp.int32)[:, None] * CAP + slot).reshape(-1).astype(jnp.int32)
    expert_flat = route_expert.reshape(-1).astype(jnp.int32)
    token_of = (jnp.arange(TOKENS * TOPK, dtype=jnp.int32) // TOPK).astype(jnp.int32)
    table = jnp.zeros((EXPERTS, N_FS * CAP), jnp.int32).at[expert_flat, place].set(token_of)

    def one_expert(operands):
        row_index, weight_gate, weight_up, weight_down = operands
        rows = normed[row_index]
        return expert_apply(rows, weight_gate, weight_up, weight_down, N_TP).astype(jnp.bfloat16)
    results = lax.map(one_expert, (table, expert_gate, expert_up, expert_down))
    picked = results[expert_flat, place].reshape(TOKENS, TOPK, D)
    routed = lax.optimization_barrier(jnp.sum(route_weight[:, :, None] * picked.astype(jnp.float32), axis=1))
    shared_result = expert_apply(normed, shared_gate, shared_up, shared_down, N_TP)
    mixed = (routed + shared_result).astype(jnp.bfloat16)
    return (expert_gate, expert_up, expert_down, shared_gate, shared_up, shared_down, mixed)
```

```python
import jax
import jax.numpy as jnp
from jax import lax
from jax.sharding import PartitionSpec as P

norm_eps = 1e-06
bf16 = jnp.bfloat16
f32 = jnp.float32


def dot(a, b):
    return jnp.dot(a, b, preferred_element_type=f32)


def after(value, *others):
    return lax.optimization_barrier((value, *others))[0]


def on_device(
    tokens,
    norm_gain,
    gate_train,
    up_train,
    down_train,
    shared_gate_train,
    shared_up_train,
    shared_down_train,
    route_expert,
    route_weight,
):
    experts = lax.axis_size("fs")
    tp = lax.axis_size("tp")
    t = lax.axis_index("tp")
    chip, core = t // 2, t % 2
    tok_rows, width = tokens.shape
    top_count = route_expert.shape[1]
    cap = 3 * tok_rows * top_count // (2 * experts)
    half = cap // 2
    quarter = width // (tp // 2)
    cols = width // tp

    right = [(i, (i + 2) % tp) for i in range(tp)]
    left = [(i, (i - 2) % tp) for i in range(tp)]
    across = [(i, (i + 4) % tp) for i in range(tp)]
    swap = [(i, i ^ 1) for i in range(tp)]

    def move(a, pairs):
        return lax.ppermute(a, "tp", pairs)

    expert_ids = jnp.arange(experts, dtype=jnp.int32)
    one_hot = [
        (route_expert[:, k][:, None] == expert_ids[None, :]) for k in range(top_count)
    ]
    named = sum(h.astype(bf16) for h in one_hot)
    before = (
        jnp.arange(tok_rows)[:, None] > jnp.arange(tok_rows)[None, :]
    ).astype(bf16)
    earlier = dot(before, named)
    slots = [jnp.sum(jnp.where(h, earlier, 0.0), axis=1).astype(jnp.int32) for h in one_hot]
    spots = jnp.arange(experts * half, dtype=jnp.int32)[None, :]

    def targets(which):
        return [
            jnp.where(
                (s >= which * half) & (s < (which + 1) * half),
                route_expert[:, k] * half + s - which * half,
                -1,
            )
            for k, s in enumerate(slots)
        ]

    own_targets = targets(core)
    placing = sum((w[:, None] == spots).astype(bf16) for w in own_targets)

    values = tokens.astype(f32)
    normed = (
        values * lax.rsqrt(jnp.mean(values * values, axis=1, keepdims=True) + norm_eps)
    ).astype(bf16)
    own_cols = lax.dynamic_slice_in_dim(normed, chip * quarter, quarter, 1)
    outgoing = lax.dot_general(
        placing, own_cols, (((0,), (0,)), ((), ())), preferred_element_type=f32
    ).astype(bf16).reshape(experts, half, quarter)
    arriving = lax.all_to_all(outgoing, "fs", split_axis=0, concat_axis=0, tiled=True)

    gain = norm_gain[:, None]
    shared_gu_local = jnp.concatenate(
        [(gain * shared_gate_train).astype(bf16), (gain * shared_up_train).astype(bf16)], axis=1
    )
    shared_gu = lax.all_gather(shared_gu_local, "fs", axis=0, tiled=True)
    shared_down_cols = lax.all_gather(
        shared_down_train.astype(bf16), "fs", axis=0, tiled=True
    )
    gu_local = jnp.concatenate(
        [(gain[None] * gate_train).astype(bf16), (gain[None] * up_train).astype(bf16)], axis=2
    )
    gu_local, arriving = lax.optimization_barrier((gu_local, arriving))
    gu = lax.all_to_all(gu_local, "fs", split_axis=0, concat_axis=0, tiled=True)
    down_local = after(down_train.astype(bf16), gu)
    down_cols = lax.all_to_all(down_local, "fs", split_axis=0, concat_axis=0, tiled=True)
    hs = gate_train.shape[2]
    gu = gu.reshape(width, 2 * hs)
    gu_other = move(gu, swap)
    hidden_rows = down_train.shape[1] * experts
    down_cols = down_cols.reshape(hidden_rows, cols)
    down_other = move(down_cols, swap)

    rows = experts * half
    h = experts // 2
    from_left = move(arriving, right)
    from_right = move(arriving, left)
    opposite_a = move(from_left[:h], right)
    opposite_b = move(from_right[h:], left)
    opposite = jnp.concatenate([opposite_a, opposite_b], axis=0)

    def part(weight, shift):
        at = ((chip + shift) % (tp // 2)) * quarter
        return lax.dynamic_slice_in_dim(weight, at, quarter, 0)

    pieces = ((arriving, 0), (from_left, -1), (from_right, 1), (opposite, 2))

    def hidden_of(weight):
        total = None
        for block, shift in pieces:
            term = dot(block.reshape(rows, quarter), part(weight, shift))
            total = term if total is None else total + term
        return (jax.nn.silu(total[:, :hs]) * total[:, hs:]).astype(bf16)

    hid_own = hidden_of(gu)
    hid_other = hidden_of(gu_other)
    low = jnp.where(core == 0, hid_own, hid_other)
    high = jnp.where(core == 0, hid_other, hid_own)
    hidden = jnp.concatenate([low, high], axis=1)

    sg = dot(normed, shared_gu)
    shared_hid = (jax.nn.silu(sg[:, :hs]) * sg[:, hs:]).astype(bf16)
    shared_whole = lax.all_gather(shared_hid, "tp", axis=1, tiled=True)

    hid_parts = (
        (hidden, 0),
        (move(hidden, right), -1),
        (move(hidden, left), 1),
        (move(hidden, across), 2),
    )

    def down_of(weight):
        total = None
        for block, shift in hid_parts:
            at = ((chip + shift) % (tp // 2)) * (2 * hs)
            term = dot(block, lax.dynamic_slice_in_dim(weight, at, 2 * hs, 0))
            total = term if total is None else total + term
        return total.astype(bf16)

    low = jnp.where(core == 0, 0, 1)
    sums = jnp.concatenate([down_of(down_cols), down_of(down_other)], axis=1)
    returning = sums.reshape(experts, half, 2 * cols)
    returned = lax.all_to_all(returning, "fs", split_axis=0, concat_axis=0, tiled=True)
    returned = returned.reshape(rows, 2 * cols)
    got_own = returned[:, :cols]
    got_other = move(returned[:, cols:], swap)

    def mixing(which):
        high_part, low_part = 0, 0
        for k, w in enumerate(targets(which)):
            at = w[:, None] == spots
            weight = route_weight[:, k][:, None]
            top = weight.astype(bf16)
            rest = (weight - top.astype(f32)).astype(bf16)
            high_part = high_part + jnp.where(at, top, 0).astype(bf16)
            low_part = low_part + jnp.where(at, rest, 0).astype(bf16)
        return high_part, low_part

    own_high, own_low = mixing(core)
    other_high, other_low = mixing(1 - core)
    mixed = (
        dot(shared_whole, shared_down_cols)
        + dot(own_high, got_own)
        + dot(own_low, got_own)
        + dot(other_high, got_other)
        + dot(other_low, got_other)
    ).astype(bf16)

    both = jnp.concatenate(
        [down_cols.reshape(tp, hs, cols), shared_down_cols.reshape(tp, hs, cols)], axis=1
    )
    both = after(both, sums)
    at_rows = lax.all_to_all(both, "tp", split_axis=0, concat_axis=0, tiled=True)
    at_rows = jnp.swapaxes(at_rows, 0, 1).reshape(2 * hs, width)
    expert_down = at_rows[None, :hs]
    shared_down = at_rows[hs:]
    expert_gate = gu[None, :, :hs]
    expert_up = gu[None, :, hs:]
    shared_gate = shared_gu[:, :hs]
    shared_up = shared_gu[:, hs:]
    return (expert_gate, expert_up, expert_down, shared_gate, shared_up, shared_down, mixed)


def solution(mesh):
    placed = (
        P("fs", None),
        P("fs"),
        P(None, "fs", "tp"),
        P(None, "fs", "tp"),
        P(None, "fs", "tp"),
        P("fs", "tp"),
        P("fs", "tp"),
        P("fs", "tp"),
        P("fs", None),
        P("fs", None),
    )
    return jax.shard_map(
        on_device,
        mesh=mesh,
        in_specs=placed,
        out_specs=(
            P("fs", None, "tp"),
            P("fs", None, "tp"),
            P("fs", "tp", None),
            P(None, "tp"),
            P(None, "tp"),
            P("tp", None),
            P("fs", "tp"),
        ),
        check_vma=False,
    )
```

```python
import functools

import jax
import jax.numpy as jnp
from jax import lax
from jax.experimental import pallas as pl
from jax.experimental.pallas import tpu as pltpu
from jax.sharding import PartitionSpec as P

norm_eps = 1e-06
bf16 = jnp.bfloat16
f32 = jnp.float32


def dot(a, b):
    return jnp.dot(a, b, preferred_element_type=f32)


def together(*values):
    return lax.optimization_barrier(values)


def cost(flops, moved):
    return pl.CostEstimate(flops=flops, bytes_accessed=moved, transcendentals=0)


def vmem_limit(mib):
    return pltpu.CompilerParams(vmem_limit_bytes=mib << 20)


def dispatch_kernel(half, place_ref, route_ref, tok_ref, normed_ref, out_ref, slot_ref, kept, placing):
    step = pl.program_id(0)
    chip, core = place_ref[0], place_ref[1]
    rows, _ = tok_ref.shape
    quarter = out_ref.shape[1]
    spots, tok_rows = placing.shape
    experts = spots // half

    @pl.when(step == 0)
    def _():
        ids = lax.broadcasted_iota(jnp.int32, (experts, tok_rows), 0)
        hot = [route_ref[k : k + 1, :] == ids for k in range(route_ref.shape[0])]
        named = sum(jnp.where(x, 1.0, 0.0) for x in hot).astype(bf16)
        ahead = lax.broadcasted_iota(jnp.int32, (tok_rows, tok_rows), 0) < (
            lax.broadcasted_iota(jnp.int32, (tok_rows, tok_rows), 1)
        )
        earlier = dot(named, jnp.where(ahead, 1.0, 0.0).astype(bf16))
        spot = lax.broadcasted_iota(jnp.int32, (spots, tok_rows), 0)
        total = jnp.zeros((spots, tok_rows), f32)
        for k, x in enumerate(hot):
            slot = jnp.sum(jnp.where(x, earlier, 0.0), axis=0, keepdims=True).astype(jnp.int32)
            slot_ref[k : k + 1, :] = slot
            local = slot - core * half
            here = (local >= 0) & (local < half)
            target = jnp.where(here, route_ref[k : k + 1, :] * half + local, -1)
            total = total + jnp.where(spot == target, 1.0, 0.0)
        placing[...] = total.astype(bf16)

    values = tok_ref[...].astype(f32)
    scale = lax.rsqrt(jnp.mean(values * values, axis=1, keepdims=True) + norm_eps)
    normed_ref[...] = (values * scale).astype(bf16)
    at = pl.multiple_of(chip * quarter, quarter)
    kept[pl.ds(pl.multiple_of(step * rows, rows), rows), :] = normed_ref[:, pl.ds(at, quarter)]

    @pl.when(step == pl.num_programs(0) - 1)
    def _():
        for c in range(0, spots, 256):
            out_ref[c : c + 256, :] = dot(placing[c : c + 256, :], kept[...]).astype(bf16)


def mark_kernel(a_ref, b_ref, out_ref):
    out_ref[...] = a_ref[...] + b_ref[...]


def first_kernel(place_ref, *refs):
    x_refs, (w_own_ref, w_other_ref, _, acc_ref) = refs[:6], refs[6:]
    chip = place_ref[0]
    quarter, wide = x_refs[0].shape[1], w_own_ref.shape[1]
    chips = w_own_ref.shape[0] // quarter
    for part in range(2):
        for half, w_ref in ((0, w_own_ref), (1, w_other_ref)):
            total = None
            for x_ref, shift in zip(x_refs[3 * part : 3 * part + 3], (0, chips - 1, 1)):
                at = pl.multiple_of(lax.rem(chip + shift, chips) * quarter, quarter)
                term = dot(x_ref[...], w_ref[pl.ds(at, quarter), :])
                total = term if total is None else total + term
            acc_ref[part, :, half * wide : (half + 1) * wide] = total


def hidden_kernel(place_ref, far0_ref, far1_ref, acc_ref, w_own_ref, w_other_ref, out_ref):
    core = place_ref[1]
    wide = w_own_ref.shape[1]
    hs = wide // 2
    for part, far_ref in enumerate((far0_ref, far1_ref)):
        for half, w_ref, slot in ((0, w_own_ref, core), (1, w_other_ref, 1 - core)):
            total = acc_ref[part, :, half * wide : (half + 1) * wide]
            total = total + dot(far_ref[...], w_ref[...])
            gate, up = total[:, :hs], total[:, hs:]
            value = (gate / (1.0 + jnp.exp(-gate)) * up).astype(bf16)
            out_ref[part, :, pl.ds(pl.multiple_of(slot * hs, hs), hs)] = value


def down_kernel(place_ref, h0_ref, h1_ref, h2_ref, h3_ref, w_own_ref, w_other_ref, out_ref):
    chip = place_ref[0]
    depth, cols = h0_ref.shape[1], w_own_ref.shape[1]
    chips = w_own_ref.shape[0] // depth
    parts = ((h0_ref, 0), (h1_ref, chips - 1), (h2_ref, 1), (h3_ref, chips // 2))
    for half, w_ref in ((0, w_own_ref), (1, w_other_ref)):
        total = None
        for h_ref, shift in parts:
            at = pl.multiple_of(lax.rem(chip + shift, chips) * depth, depth)
            term = dot(h_ref[...], w_ref[pl.ds(at, depth), :])
            total = term if total is None else total + term
        out_ref[:, half * cols : (half + 1) * cols] = total.astype(bf16)


def mix_kernel(high_ref, low_ref, got_ref, base_ref, out_ref):
    got = got_ref[...]
    total = base_ref[...] + dot(high_ref[...], got) + dot(low_ref[...], got)
    out_ref[...] = total.astype(out_ref.dtype)


def join_kernel(place_ref, p0_ref, p1_ref, p2_ref, p3_ref, routed_ref, shared_ref):
    chip, core = place_ref[0], place_ref[1]
    hs = routed_ref.shape[0]
    cols = p0_ref.shape[1] // 2
    for shift, ref in enumerate((p0_ref, p1_ref, p2_ref, p3_ref)):
        source = lax.rem(chip + 4 - shift, 4)
        for half, lane in ((0, core), (1, 1 - core)):
            at = pl.multiple_of((source * 2 + lane) * cols, cols)
            block = ref[:, half * cols : (half + 1) * cols]
            routed_ref[:, pl.ds(at, cols)] = block[:hs]
            shared_ref[:, pl.ds(at, cols)] = block[hs:]


def whole(shape):
    return pl.BlockSpec(shape, lambda *_: (0,) * len(shape))


def on_device(
    tokens,
    norm_gain,
    gate_train,
    up_train,
    down_train,
    shared_gate_train,
    shared_up_train,
    shared_down_train,
    route_expert,
    route_weight,
):
    experts = lax.axis_size("fs")
    tp = lax.axis_size("tp")
    t = lax.axis_index("tp")
    chips = tp // 2
    chip, core = t // 2, t % 2
    place = jnp.stack([chip, core]).astype(jnp.int32)
    tok_rows, width = tokens.shape
    top_count = route_expert.shape[1]
    cap = 3 * tok_rows * top_count // (2 * experts)
    half = cap // 2
    rows = experts * half
    quarter = width // chips
    cols = width // tp
    hs = gate_train.shape[2]
    deep = down_train.shape[1]

    def shift_by(a, n):
        return lax.ppermute(a, "tp", [(i, (i + 2 * n) % tp) for i in range(tp)])

    def swap(a):
        return lax.ppermute(a, "tp", [(i, i ^ 1) for i in range(tp)])

    gain = norm_gain[:, None]
    shared_local = jnp.concatenate(
        [
            jnp.concatenate(
                [(gain * shared_gate_train).astype(bf16), (gain * shared_up_train).astype(bf16)],
                axis=1,
            ).reshape(-1, deep, 2 * hs),
            jnp.swapaxes(
                shared_down_train.astype(bf16).reshape(deep, -1, 2 * hs), 0, 1
            ),
        ],
        axis=0,
    )
    shared_all = lax.all_gather(shared_local, "fs", axis=0, tiled=False)
    gu_blocks = gain.shape[0] // deep
    shared_gu = shared_all[:, :gu_blocks].reshape(width, 2 * hs)
    shared_cols = jnp.swapaxes(shared_all[:, gu_blocks:], 1, 2).reshape(experts * deep, cols)

    steps = 8
    block = tok_rows // steps
    normed, outgoing, slots = pl.pallas_call(
        functools.partial(dispatch_kernel, half),
        grid_spec=pltpu.PrefetchScalarGridSpec(
            num_scalar_prefetch=1,
            grid=(steps,),
            in_specs=[
                whole((top_count, tok_rows)),
                pl.BlockSpec((block, width), lambda i, s: (i, 0)),
            ],
            out_specs=[
                pl.BlockSpec((block, width), lambda i, s: (i, 0)),
                whole((rows, quarter)),
                whole((top_count, tok_rows)),
            ],
            scratch_shapes=[
                pltpu.VMEM((tok_rows, quarter), bf16),
                pltpu.VMEM((rows, tok_rows), bf16),
            ],
        ),
        out_shape=[
            jax.ShapeDtypeStruct((tok_rows, width), bf16),
            jax.ShapeDtypeStruct((rows, quarter), bf16),
            jax.ShapeDtypeStruct((top_count, tok_rows), jnp.int32),
        ],
        compiler_params=vmem_limit(60),
        cost_estimate=cost(2 * rows * tok_rows * quarter, 4 * tok_rows * width),
    )(place, route_expert.T, tokens)
    arriving = lax.all_to_all(
        outgoing.reshape(experts, half, quarter), "fs", split_axis=0, concat_axis=0, tiled=True
    )

    gu_local = jnp.concatenate(
        [(gain[None] * gate_train).astype(bf16), (gain[None] * up_train).astype(bf16)], axis=2
    )
    mid = rows // 2
    arriving = arriving.reshape(rows, quarter)
    top, bottom = together(arriving[:mid], arriving[mid:])
    gu_local, top, bottom = together(gu_local, top, bottom)
    gu = lax.all_to_all(gu_local, "fs", split_axis=0, concat_axis=0, tiled=True)
    down_local, gu = together(down_train.astype(bf16), gu)
    down_cols = lax.all_to_all(down_local, "fs", split_axis=0, concat_axis=0, tiled=True)
    gu = gu.reshape(width, 2 * hs)
    gu_other = swap(gu)
    down_cols = down_cols.reshape(experts * deep, cols)
    down_other = swap(down_cols)
    shared_other = swap(shared_cols)

    left_top = shift_by(top, 1)
    right_bottom = shift_by(bottom, -1)
    right_top = shift_by(top, -1)
    left_bottom = shift_by(bottom, 1)
    far_top = shift_by(left_top, 1)
    far_bottom = shift_by(right_bottom, -1)

    tile = (16, 128)
    mark = pl.pallas_call(
        mark_kernel,
        grid=(1,),
        in_specs=[whole(tile)] * 2,
        out_specs=whole(tile),
        out_shape=jax.ShapeDtypeStruct(tile, bf16),
        cost_estimate=cost(1 << 20, 1 << 14),
    )(left_top, right_bottom)
    x_spec = pl.BlockSpec((mid // 2, quarter), lambda i, s: (i, 0))
    acc_spec = pl.BlockSpec((2, mid // 2, 4 * hs), lambda i, s: (0, i, 0))
    w_spec = pl.BlockSpec((quarter, 2 * hs), lambda i, s: (lax.rem(s[0] + chips // 2, chips), 0))
    acc = pl.pallas_call(
        first_kernel,
        grid_spec=pltpu.PrefetchScalarGridSpec(
            num_scalar_prefetch=1,
            grid=(2,),
            in_specs=[x_spec] * 6 + [whole((width, 2 * hs))] * 2 + [whole(tile)],
            out_specs=acc_spec,
        ),
        out_shape=jax.ShapeDtypeStruct((2, mid, 4 * hs), f32),
        compiler_params=vmem_limit(32),
        cost_estimate=cost(2 * rows * 3 * quarter * 4 * hs, 8 * width * hs),
    )(place, top, left_top, right_top, bottom, left_bottom, right_bottom, gu, gu_other, mark)
    hidden = pl.pallas_call(
        hidden_kernel,
        grid_spec=pltpu.PrefetchScalarGridSpec(
            num_scalar_prefetch=1,
            grid=(2,),
            in_specs=[x_spec, x_spec, acc_spec, w_spec, w_spec],
            out_specs=pl.BlockSpec((2, mid // 2, 2 * hs), lambda i, s: (0, i, 0)),
        ),
        out_shape=jax.ShapeDtypeStruct((2, mid, 2 * hs), bf16),
        compiler_params=vmem_limit(32),
        cost_estimate=cost(2 * rows * quarter * 4 * hs, 8 * quarter * hs),
    )(place, far_top, far_bottom, acc, gu, gu_other).reshape(rows, 2 * hs)

    sg = dot(normed, shared_gu)
    gate, up = sg[:, :hs], sg[:, hs:]
    shared_hid = (gate / (1.0 + jnp.exp(-gate)) * up).astype(bf16)
    shared_whole = lax.all_gather(shared_hid, "tp", axis=1, tiled=True)

    h_spec = pl.BlockSpec((rows // 3, 2 * hs), lambda i, s: (i, 0))
    sums = pl.pallas_call(
        down_kernel,
        grid_spec=pltpu.PrefetchScalarGridSpec(
            num_scalar_prefetch=1,
            grid=(3,),
            in_specs=[h_spec] * 4 + [whole((experts * deep, cols))] * 2,
            out_specs=pl.BlockSpec((rows // 3, 2 * cols), lambda i, s: (i, 0)),
        ),
        out_shape=jax.ShapeDtypeStruct((rows, 2 * cols), bf16),
        compiler_params=vmem_limit(60),
        cost_estimate=cost(4 * rows * experts * deep * cols, 8 * experts * deep * cols),
    )(
        place,
        hidden,
        shift_by(hidden, 1),
        shift_by(hidden, -1),
        shift_by(hidden, 2),
        down_cols,
        down_other,
    )
    returned = lax.all_to_all(
        sums.reshape(experts, half, 2 * cols), "fs", split_axis=0, concat_axis=0, tiled=True
    ).reshape(rows, 2 * cols)
    got_other = swap(returned[:, cols:])

    spots = jnp.arange(rows, dtype=jnp.int32)[None, :]

    def mixing(which):
        high, low = 0, 0
        for k in range(top_count):
            local = slots[k] - which * half
            here = (local >= 0) & (local < half)
            target = jnp.where(here, route_expert[:, k] * half + local, -1)
            at = target[:, None] == spots
            weight = route_weight[:, k][:, None]
            most = weight.astype(bf16)
            rest = (weight - most.astype(f32)).astype(bf16)
            high = high + jnp.where(at, most, 0)
            low = low + jnp.where(at, rest, 0)
        return together(high.astype(bf16), low.astype(bf16))

    def mix(pair, got, base, dtype):
        return pl.pallas_call(
            mix_kernel,
            grid=(2,),
            in_specs=[
                pl.BlockSpec((tok_rows // 2, rows), lambda i: (i, 0)),
                pl.BlockSpec((tok_rows // 2, rows), lambda i: (i, 0)),
                pl.BlockSpec((rows, cols), lambda i: (0, 0)),
                pl.BlockSpec((tok_rows // 2, cols), lambda i: (i, 0)),
            ],
            out_specs=pl.BlockSpec((tok_rows // 2, cols), lambda i: (i, 0)),
            out_shape=jax.ShapeDtypeStruct((tok_rows, cols), dtype),
            compiler_params=vmem_limit(24),
            cost_estimate=cost(4 * tok_rows * rows * cols, 4 * tok_rows * rows),
        )(*pair, got, base)

    shared_sums = dot(shared_whole, shared_cols)
    part = mix(mixing(core), returned, shared_sums, f32)
    mixed = mix(mixing(1 - core), got_other, part, bf16)

    def chunk(n):
        at = (lax.rem(chip + n, chips) * 2 + core) * hs
        block = [
            lax.dynamic_slice_in_dim(a, at, hs, 0)
            for a in (down_cols, down_other, shared_cols, shared_other)
        ]
        return jnp.concatenate(
            [jnp.concatenate(block[:2], axis=1), jnp.concatenate(block[2:], axis=1)], axis=0
        )

    chunks = together(*(chunk(n) for n in range(chips)), sums)[:chips]
    pieces = [chunks[0]]
    for n in range(1, chips):
        pieces.append(shift_by(chunks[n], n))
    expert_down, shared_down = pl.pallas_call(
        join_kernel,
        grid_spec=pltpu.PrefetchScalarGridSpec(
            num_scalar_prefetch=1,
            grid=(1,),
            in_specs=[whole((2 * hs, 2 * cols))] * 4,
            out_specs=[whole((hs, width))] * 2,
        ),
        out_shape=[jax.ShapeDtypeStruct((hs, width), bf16)] * 2,
        compiler_params=vmem_limit(24),
        cost_estimate=cost(1 << 20, 8 * hs * width),
    )(place, *pieces)
    expert_gate = gu[None, :, :hs]
    expert_up = gu[None, :, hs:]
    shared_gate = shared_gu[:, :hs]
    shared_up = shared_gu[:, hs:]
    return (
        expert_gate,
        expert_up,
        expert_down[None],
        shared_gate,
        shared_up,
        shared_down,
        mixed,
    )


def solution(mesh):
    placed = (
        P("fs", None),
        P("fs"),
        P(None, "fs", "tp"),
        P(None, "fs", "tp"),
        P(None, "fs", "tp"),
        P("fs", "tp"),
        P("fs", "tp"),
        P("fs", "tp"),
        P("fs", None),
        P("fs", None),
    )

    return jax.shard_map(
        on_device,
        mesh=mesh,
        in_specs=placed,
        out_specs=(
            P("fs", None, "tp"),
            P("fs", None, "tp"),
            P("fs", "tp", None),
            P(None, "tp"),
            P(None, "tp"),
            P("tp", None),
            P("fs", "tp"),
        ),
        check_vma=False,
    )
```

```python
import functools

import jax
import jax.numpy as jnp
from jax import lax
from jax.experimental import pallas as pl
from jax.experimental.pallas import tpu as pltpu
from jax.sharding import PartitionSpec as P

norm_eps = 1e-06
bf16 = jnp.bfloat16
f32 = jnp.float32


def dot(a, b):
    return jnp.dot(a, b, preferred_element_type=f32)


def together(*values):
    return lax.optimization_barrier(values)


def cost(flops, moved):
    return pl.CostEstimate(flops=flops, bytes_accessed=moved, transcendentals=0)


def vmem_limit(mib):
    return pltpu.CompilerParams(vmem_limit_bytes=mib << 20)


def dispatch_kernel(half, place_ref, route_ref, tok_ref, normed_ref, out_ref, slot_ref, kept, placing):
    step = pl.program_id(0)
    chip, core = place_ref[0], place_ref[1]
    rows, _ = tok_ref.shape
    quarter = out_ref.shape[1]
    spots, tok_rows = placing.shape
    experts = spots // half

    @pl.when(step == 0)
    def _():
        ids = lax.broadcasted_iota(jnp.int32, (experts, tok_rows), 0)
        hot = [route_ref[k : k + 1, :] == ids for k in range(route_ref.shape[0])]
        named = sum(jnp.where(x, 1.0, 0.0) for x in hot).astype(bf16)
        ahead = lax.broadcasted_iota(jnp.int32, (tok_rows, tok_rows), 0) < (
            lax.broadcasted_iota(jnp.int32, (tok_rows, tok_rows), 1)
        )
        earlier = dot(named, jnp.where(ahead, 1.0, 0.0).astype(bf16))
        spot = lax.broadcasted_iota(jnp.int32, (spots, tok_rows), 0)
        total = jnp.zeros((spots, tok_rows), f32)
        for k, x in enumerate(hot):
            slot = jnp.sum(jnp.where(x, earlier, 0.0), axis=0, keepdims=True).astype(jnp.int32)
            slot_ref[k : k + 1, :] = slot
            local = slot - core * half
            here = (local >= 0) & (local < half)
            target = jnp.where(here, route_ref[k : k + 1, :] * half + local, -1)
            total = total + jnp.where(spot == target, 1.0, 0.0)
        placing[...] = total.astype(bf16)

    for r in range(0, rows, 16):
        values = tok_ref[r : r + 16, :].astype(f32)
        scale = lax.rsqrt(jnp.mean(values * values, axis=1, keepdims=True) + norm_eps)
        normed_ref[r : r + 16, :] = (values * scale).astype(bf16)
    at = pl.multiple_of(chip * quarter, quarter)
    kept[pl.ds(pl.multiple_of(step * rows, rows), rows), :] = normed_ref[:, pl.ds(at, quarter)]

    @pl.when(step == pl.num_programs(0) - 1)
    def _():
        for c in range(0, spots, 256):
            out_ref[c : c + 256, :] = dot(placing[c : c + 256, :], kept[...]).astype(bf16)


def mark_kernel(a_ref, b_ref, out_ref):
    out_ref[...] = a_ref[...] + b_ref[...]


def first_kernel(place_ref, *refs):
    x_refs, (w_own_ref, w_other_ref, _, acc_ref) = refs[:6], refs[6:]
    chip = place_ref[0]
    quarter, wide = x_refs[0].shape[1], w_own_ref.shape[1]
    chips = w_own_ref.shape[0] // quarter
    for part in range(2):
        for half, w_ref in ((0, w_own_ref), (1, w_other_ref)):
            total = None
            for x_ref, shift in zip(x_refs[3 * part : 3 * part + 3], (0, chips - 1, 1)):
                at = pl.multiple_of(lax.rem(chip + shift, chips) * quarter, quarter)
                term = dot(x_ref[...], w_ref[pl.ds(at, quarter), :])
                total = term if total is None else total + term
            acc_ref[part, :, half * wide : (half + 1) * wide] = total


def hidden_kernel(place_ref, far0_ref, far1_ref, acc_ref, w_own_ref, w_other_ref, out_ref):
    core = place_ref[1]
    wide = w_own_ref.shape[1]
    hs = wide // 2
    for part, far_ref in enumerate((far0_ref, far1_ref)):
        for half, w_ref, slot in ((0, w_own_ref, core), (1, w_other_ref, 1 - core)):
            total = acc_ref[part, :, half * wide : (half + 1) * wide]
            total = total + dot(far_ref[...], w_ref[...])
            gate, up = total[:, :hs], total[:, hs:]
            value = (gate / (1.0 + jnp.exp(-gate)) * up).astype(bf16)
            out_ref[part, :, pl.ds(pl.multiple_of(slot * hs, hs), hs)] = value


def down_kernel(place_ref, h0_ref, h1_ref, h2_ref, h3_ref, w_own_ref, w_other_ref, out_ref, line):
    chip = place_ref[0]
    depth, cols = h0_ref.shape[1], w_own_ref.shape[1]
    chips = w_own_ref.shape[0] // depth
    parts = ((h0_ref, 0), (h1_ref, chips - 1), (h2_ref, 1), (h3_ref, chips // 2))
    for h_ref, shift in parts:
        at = pl.multiple_of(lax.rem(chip + shift, chips) * depth, depth)
        line[:, pl.ds(at, depth)] = h_ref[...]
    for part, w_ref in enumerate((w_own_ref, w_other_ref)):
        total = dot(line[...], w_ref[...]).astype(bf16)
        out_ref[:, part] = total.reshape(out_ref.shape[0], out_ref.shape[2], cols)


def shared_kernel(place_ref, x_ref, gu_ref, sd_ref, gate_ref, up_ref, hid_ref, sd_out_ref, acc):
    step = pl.program_id(0)
    core = place_ref[1]
    wide = acc.shape[1]
    hs = wide // 2
    deep = gu_ref.shape[0] // 4
    fold = gu_ref.shape[1] // wide
    for f in range(4):
        block = gu_ref[f * deep : (f + 1) * deep, :]
        weight = jnp.concatenate([block[:, j * wide : (j + 1) * wide] for j in range(fold)], axis=0)
        size = fold * deep
        gate_ref[f * size : (f + 1) * size, :] = weight[:, :hs]
        up_ref[f * size : (f + 1) * size, :] = weight[:, hs:]
        term = dot(x_ref[:, f * size : (f + 1) * size], weight)
        first = (step == 0) if f == 0 else False
        if f == 0:
            @pl.when(first)
            def _():
                acc[...] = term

            @pl.when(step > 0)
            def _():
                acc[...] += term
        else:
            acc[...] += term
    rows = sd_out_ref.shape[0]
    sd_out_ref[...] = sd_ref[pl.ds(pl.multiple_of((1 - core) * rows, rows), rows), :]

    @pl.when(step == pl.num_programs(0) - 1)
    def _():
        gate, up = acc[:, :hs], acc[:, hs:]
        hid_ref[...] = (gate / (1.0 + jnp.exp(-gate)) * up).astype(bf16)


def base_kernel(hid_ref, sd_ref, out_ref):
    out_ref[...] = dot(hid_ref[...], sd_ref[...])


def mix_kernel(weight_ref, got_ref, base_ref, out_ref):
    out_ref[...] = (base_ref[...] + dot(weight_ref[...], got_ref[...])).astype(out_ref.dtype)


def chunk_kernel(place_ref, own_ref, other_ref, sd_ref, sd_other_ref, *out_refs):
    chip, core = place_ref[0], place_ref[1]
    hs, cols = out_refs[0].shape[0] // 2, own_ref.shape[1]
    for n, out_ref in enumerate(out_refs):
        target = lax.rem(chip + n, 4)
        at = pl.ds(pl.multiple_of((target * 2 + core) * hs, hs), hs)
        far = pl.ds(pl.multiple_of(target * hs, hs), hs)
        out_ref[:hs, :cols] = own_ref[at, :]
        out_ref[:hs, cols:] = other_ref[at, :]
        out_ref[hs:, :cols] = sd_ref[at, :]
        out_ref[hs:, cols:] = sd_other_ref[far, :]


def join_kernel(place_ref, p0_ref, p1_ref, p2_ref, p3_ref, routed_ref, shared_ref):
    chip, core = place_ref[0], place_ref[1]
    hs = routed_ref.shape[0]
    cols = p0_ref.shape[1] // 2
    for shift, ref in enumerate((p0_ref, p1_ref, p2_ref, p3_ref)):
        source = lax.rem(chip + 4 - shift, 4)
        for half, lane in ((0, core), (1, 1 - core)):
            at = pl.multiple_of((source * 2 + lane) * cols, cols)
            block = ref[:, half * cols : (half + 1) * cols]
            routed_ref[:, pl.ds(at, cols)] = block[:hs]
            shared_ref[:, pl.ds(at, cols)] = block[hs:]


def whole(shape):
    return pl.BlockSpec(shape, lambda *_: (0,) * len(shape))


def on_device(
    tokens,
    norm_gain,
    gate_train,
    up_train,
    down_train,
    shared_gate_train,
    shared_up_train,
    shared_down_train,
    route_expert,
    route_weight,
):
    experts = lax.axis_size("fs")
    tp = lax.axis_size("tp")
    t = lax.axis_index("tp")
    chips = tp // 2
    chip, core = t // 2, t % 2
    place = jnp.stack([chip, core]).astype(jnp.int32)
    tok_rows, width = tokens.shape
    top_count = route_expert.shape[1]
    cap = 3 * tok_rows * top_count // (2 * experts)
    half = cap // 2
    rows = experts * half
    quarter = width // chips
    cols = width // tp
    hs = gate_train.shape[2]
    deep = down_train.shape[1]

    def shift_by(a, n):
        return lax.ppermute(a, "tp", [(i, (i + 2 * n) % tp) for i in range(tp)])

    def swap(a):
        return lax.ppermute(a, "tp", [(i, i ^ 1) for i in range(tp)])

    gain = norm_gain[:, None]
    shared_gu_local = jnp.concatenate(
        [(gain * shared_gate_train).astype(bf16), (gain * shared_up_train).astype(bf16)], axis=1
    )
    fold = shared_gu_local.shape[0] // deep
    shared_all = lax.all_gather(
        jnp.concatenate(
            [shared_gu_local[j * deep : (j + 1) * deep] for j in range(fold)]
            + [shared_down_train.astype(bf16)],
            axis=1,
        ),
        "fs",
        axis=0,
        tiled=True,
    )

    steps = 8
    block = tok_rows // steps
    normed, outgoing, slots = pl.pallas_call(
        functools.partial(dispatch_kernel, half),
        grid_spec=pltpu.PrefetchScalarGridSpec(
            num_scalar_prefetch=1,
            grid=(steps,),
            in_specs=[
                whole((top_count, tok_rows)),
                pl.BlockSpec((block, width), lambda i, s: (i, 0)),
            ],
            out_specs=[
                pl.BlockSpec((block, width), lambda i, s: (i, 0)),
                whole((rows, quarter)),
                whole((top_count, tok_rows)),
            ],
            scratch_shapes=[
                pltpu.VMEM((tok_rows, quarter), bf16),
                pltpu.VMEM((rows, tok_rows), bf16),
            ],
        ),
        out_shape=[
            jax.ShapeDtypeStruct((tok_rows, width), bf16),
            jax.ShapeDtypeStruct((rows, quarter), bf16),
            jax.ShapeDtypeStruct((top_count, tok_rows), jnp.int32),
        ],
        compiler_params=vmem_limit(60),
        cost_estimate=cost(2 * rows * tok_rows * quarter, 4 * tok_rows * width),
    )(place, route_expert.T, tokens)
    arriving = lax.all_to_all(
        outgoing.reshape(experts, half, quarter), "fs", split_axis=0, concat_axis=0, tiled=True
    )

    gu_local = jnp.concatenate(
        [(gain[None] * gate_train).astype(bf16), (gain[None] * up_train).astype(bf16)], axis=2
    )
    mid = rows // 2
    arriving = arriving.reshape(rows, quarter)
    top, bottom = together(arriving[:mid], arriving[mid:])
    gu_local, top, bottom = together(gu_local, top, bottom)
    gu = lax.all_to_all(gu_local, "fs", split_axis=0, concat_axis=0, tiled=True)
    down_local, gu = together(down_train.astype(bf16), gu)
    down_cols = lax.all_to_all(down_local, "fs", split_axis=0, concat_axis=0, tiled=True)
    gu = gu.reshape(width, 2 * hs)
    gu_other = swap(gu)
    down_cols = down_cols.reshape(experts * deep, cols)
    down_other = swap(down_cols)

    left_top = shift_by(top, 1)
    right_bottom = shift_by(bottom, -1)
    right_top = shift_by(top, -1)
    left_bottom = shift_by(bottom, 1)
    far_top = shift_by(left_top, 1)
    far_bottom = shift_by(right_bottom, -1)

    tile = (16, 128)
    mark = pl.pallas_call(
        mark_kernel,
        grid=(1,),
        in_specs=[whole(tile)] * 2,
        out_specs=whole(tile),
        out_shape=jax.ShapeDtypeStruct(tile, bf16),
        cost_estimate=cost(1 << 20, 1 << 14),
    )(left_top, right_bottom)
    x_spec = pl.BlockSpec((mid // 2, quarter), lambda i, s: (i, 0))
    acc_spec = pl.BlockSpec((2, mid // 2, 4 * hs), lambda i, s: (0, i, 0))
    w_spec = pl.BlockSpec((quarter, 2 * hs), lambda i, s: (lax.rem(s[0] + chips // 2, chips), 0))
    acc = pl.pallas_call(
        first_kernel,
        grid_spec=pltpu.PrefetchScalarGridSpec(
            num_scalar_prefetch=1,
            grid=(2,),
            in_specs=[x_spec] * 6 + [whole((width, 2 * hs))] * 2 + [whole(tile)],
            out_specs=acc_spec,
        ),
        out_shape=jax.ShapeDtypeStruct((2, mid, 4 * hs), f32),
        compiler_params=vmem_limit(32),
        cost_estimate=cost(2 * rows * 3 * quarter * 4 * hs, 8 * width * hs),
    )(place, top, left_top, right_top, bottom, left_bottom, right_bottom, gu, gu_other, mark)
    hidden = pl.pallas_call(
        hidden_kernel,
        grid_spec=pltpu.PrefetchScalarGridSpec(
            num_scalar_prefetch=1,
            grid=(1,),
            in_specs=[whole((mid, quarter))] * 2 + [whole((2, mid, 4 * hs)), w_spec, w_spec],
            out_specs=whole((2, mid, 2 * hs)),
        ),
        out_shape=jax.ShapeDtypeStruct((2, mid, 2 * hs), bf16),
        compiler_params=vmem_limit(32),
        cost_estimate=cost(2 * rows * quarter * 4 * hs, 8 * quarter * hs),
    )(place, far_top, far_bottom, acc, gu, gu_other).reshape(rows, 2 * hs)

    sd_spec = pl.BlockSpec((experts * deep, cols), lambda *_: (0, fold * 2 * hs // cols))
    shared_gate, shared_up, shared_hid, shared_out = pl.pallas_call(
        shared_kernel,
        grid_spec=pltpu.PrefetchScalarGridSpec(
            num_scalar_prefetch=1,
            grid=(experts // 4,),
            in_specs=[
                pl.BlockSpec((tok_rows, 4 * fold * deep), lambda i, s: (0, i)),
                pl.BlockSpec((4 * deep, fold * 2 * hs), lambda i, s: (i, 0)),
                pl.BlockSpec((4 * deep, cols), lambda i, s: (i, fold * 2 * hs // cols)),
            ],
            out_specs=[
                pl.BlockSpec((4 * fold * deep, hs), lambda i, s: (i, 0)),
                pl.BlockSpec((4 * fold * deep, hs), lambda i, s: (i, 0)),
                whole((tok_rows, hs)),
                pl.BlockSpec((2 * deep, cols), lambda i, s: (i, 0)),
            ],
            scratch_shapes=[pltpu.VMEM((tok_rows, 2 * hs), f32)],
        ),
        out_shape=[
            jax.ShapeDtypeStruct((width, hs), bf16),
            jax.ShapeDtypeStruct((width, hs), bf16),
            jax.ShapeDtypeStruct((tok_rows, hs), bf16),
            jax.ShapeDtypeStruct((experts * deep // 2, cols), bf16),
        ],
        compiler_params=vmem_limit(36),
        cost_estimate=cost(4 * tok_rows * width * hs, 8 * width * hs),
    )(place, normed, shared_all, shared_all)
    shared_other = swap(shared_out)
    shared_whole = lax.all_gather(shared_hid, "tp", axis=1, tiled=True)

    hid_left = shift_by(hidden, 1)
    hid_right = shift_by(hidden, -1)
    hid_far = shift_by(hidden, 2)
    sums = pl.pallas_call(
        down_kernel,
        grid_spec=pltpu.PrefetchScalarGridSpec(
            num_scalar_prefetch=1,
            grid=(1,),
            in_specs=[whole((rows, 2 * hs))] * 4 + [whole((experts * deep, cols))] * 2,
            out_specs=whole((experts, 2, half, cols)),
            scratch_shapes=[pltpu.VMEM((rows, experts * deep), bf16)],
        ),
        out_shape=jax.ShapeDtypeStruct((experts, 2, half, cols), bf16),
        compiler_params=vmem_limit(40),
        cost_estimate=cost(4 * rows * experts * deep * cols, 8 * experts * deep * cols),
    )(place, hidden, hid_left, hid_right, hid_far, down_cols, down_other)
    returned = lax.all_to_all(sums, "fs", split_axis=0, concat_axis=0, tiled=True)
    got_other = swap(returned[:, 1].reshape(rows, cols))
    got_own = returned[:, 0].reshape(rows, cols)

    spots = jnp.arange(rows, dtype=jnp.int32)[None, :]

    def mixing(which):
        weights = 0
        for k in range(top_count):
            local = slots[k] - which * half
            here = (local >= 0) & (local < half)
            target = jnp.where(here, route_expert[:, k] * half + local, -1)
            at = target[:, None] == spots
            weights = weights + jnp.where(at, route_weight[:, k][:, None].astype(bf16), 0)
        return weights

    mix_own, mix_other = together(mixing(core), mixing(1 - core))

    def mix(weights, got, base, dtype):
        return pl.pallas_call(
            mix_kernel,
            out_shape=jax.ShapeDtypeStruct((tok_rows, cols), dtype),
            compiler_params=vmem_limit(24),
            cost_estimate=cost(2 * tok_rows * rows * cols, 4 * tok_rows * rows),
        )(weights, got, base)

    base = pl.pallas_call(
        base_kernel,
        grid=(1,),
        in_specs=[whole((tok_rows, experts * deep)), sd_spec],
        out_specs=whole((tok_rows, cols)),
        out_shape=jax.ShapeDtypeStruct((tok_rows, cols), f32),
        compiler_params=vmem_limit(24),
        cost_estimate=cost(2 * tok_rows * experts * deep * cols, 4 * tok_rows * rows),
    )(shared_whole, shared_all)
    part = mix(mix_own, got_own, base, f32)
    mixed = mix(mix_other, got_other, part, bf16)

    chunks = pl.pallas_call(
        chunk_kernel,
        grid_spec=pltpu.PrefetchScalarGridSpec(
            num_scalar_prefetch=1,
            grid=(1,),
            in_specs=[whole((experts * deep, cols))] * 2
            + [sd_spec, whole((experts * deep // 2, cols))],
            out_specs=[whole((2 * hs, 2 * cols))] * chips,
        ),
        out_shape=[jax.ShapeDtypeStruct((2 * hs, 2 * cols), bf16)] * chips,
        compiler_params=vmem_limit(36),
        cost_estimate=cost(1 << 30, 8 * hs * width),
    )(place, down_cols, down_other, shared_all, shared_other)
    pieces = [chunks[0]]
    for n in range(1, chips):
        pieces.append(shift_by(chunks[n], n))
    expert_down, shared_down = pl.pallas_call(
        join_kernel,
        grid_spec=pltpu.PrefetchScalarGridSpec(
            num_scalar_prefetch=1,
            grid=(1,),
            in_specs=[whole((2 * hs, 2 * cols))] * 4,
            out_specs=[whole((hs, width))] * 2,
        ),
        out_shape=[jax.ShapeDtypeStruct((hs, width), bf16)] * 2,
        compiler_params=vmem_limit(24),
        cost_estimate=cost(1 << 20, 8 * hs * width),
    )(place, *pieces)
    expert_gate = gu[None, :, :hs]
    expert_up = gu[None, :, hs:]
    return (
        expert_gate,
        expert_up,
        expert_down[None],
        shared_gate,
        shared_up,
        shared_down,
        mixed,
    )


def solution(mesh):
    placed = (
        P("fs", None),
        P("fs"),
        P(None, "fs", "tp"),
        P(None, "fs", "tp"),
        P(None, "fs", "tp"),
        P("fs", "tp"),
        P("fs", "tp"),
        P("fs", "tp"),
        P("fs", None),
        P("fs", None),
    )

    return jax.shard_map(
        on_device,
        mesh=mesh,
        in_specs=placed,
        out_specs=(
            P("fs", None, "tp"),
            P("fs", None, "tp"),
            P("fs", "tp", None),
            P(None, "tp"),
            P(None, "tp"),
            P("tp", None),
            P("fs", "tp"),
        ),
        check_vma=False,
    )
```

```python
import functools

import jax
import jax.numpy as jnp
from jax import lax
from jax.experimental import pallas as pl
from jax.experimental.pallas import tpu as pltpu
from jax.sharding import PartitionSpec as P

norm_eps = 1e-06
bf16 = jnp.bfloat16
f32 = jnp.float32


def dot(a, b):
    return jnp.dot(a, b, preferred_element_type=f32)


def together(*values):
    return lax.optimization_barrier(values)


def cost(flops, moved):
    return pl.CostEstimate(flops=flops, bytes_accessed=moved, transcendentals=0)


def vmem_limit(mib):
    return pltpu.CompilerParams(vmem_limit_bytes=mib << 20)


def dispatch_kernel(half, place_ref, route_ref, tok_ref, normed_ref, out_ref, slot_ref, *scratch):
    taken, given, kept, placing, in_sem, out_sem = scratch
    chip, core = place_ref[0], place_ref[1]
    steps = in_sem.shape[0]
    tok_rows = taken.shape[0]
    rows = tok_rows // steps
    quarter = out_ref.shape[1]
    spots = placing.shape[0]
    experts = spots // half

    def span(step):
        return pl.ds(step * rows, rows)

    reads = [
        pltpu.make_async_copy(tok_ref.at[span(i)], taken.at[span(i)], in_sem.at[i])
        for i in range(steps)
    ]
    writes = [
        pltpu.make_async_copy(given.at[span(i)], normed_ref.at[span(i)], out_sem.at[i])
        for i in range(steps)
    ]
    for read in reads:
        read.start()

    ids = lax.broadcasted_iota(jnp.int32, (experts, tok_rows), 0)
    hot = [route_ref[k : k + 1, :] == ids for k in range(route_ref.shape[0])]
    named = sum(jnp.where(x, 1.0, 0.0) for x in hot).astype(bf16)
    ahead = lax.broadcasted_iota(jnp.int32, (tok_rows, tok_rows), 0) < (
        lax.broadcasted_iota(jnp.int32, (tok_rows, tok_rows), 1)
    )
    earlier = dot(named, jnp.where(ahead, 1.0, 0.0).astype(bf16))
    spot = lax.broadcasted_iota(jnp.int32, (spots, tok_rows), 0)
    total = jnp.zeros((spots, tok_rows), f32)
    for k, x in enumerate(hot):
        slot = jnp.sum(jnp.where(x, earlier, 0.0), axis=0, keepdims=True).astype(jnp.int32)
        slot_ref[k : k + 1, :] = slot
        local = slot - core * half
        here = (local >= 0) & (local < half)
        target = jnp.where(here, route_ref[k : k + 1, :] * half + local, -1)
        total = total + jnp.where(spot == target, 1.0, 0.0)
    placing[...] = total.astype(bf16)

    at = pl.multiple_of(chip * quarter, quarter)
    for i in range(steps):
        reads[i].wait()
        for r in range(i * rows, (i + 1) * rows, 16):
            values = taken[r : r + 16, :].astype(f32)
            scale = lax.rsqrt(jnp.mean(values * values, axis=1, keepdims=True) + norm_eps)
            given[r : r + 16, :] = (values * scale).astype(bf16)
        kept[i * rows : (i + 1) * rows, :] = given[i * rows : (i + 1) * rows, pl.ds(at, quarter)]
        if i:
            writes[i - 1].start()
    for c in range(0, spots, 256):
        out_ref[c : c + 256, :] = dot(placing[c : c + 256, :], kept[...]).astype(bf16)
    writes[steps - 1].start()
    for write in writes:
        write.wait()


def mark_kernel(a_ref, b_ref, out_ref):
    out_ref[...] = a_ref[...] + b_ref[...]


def first_kernel(place_ref, *refs):
    x_refs, (w_own_ref, w_other_ref, _, acc_ref) = refs[:6], refs[6:]
    chip = place_ref[0]
    quarter, wide = x_refs[0].shape[1], w_own_ref.shape[1]
    chips = w_own_ref.shape[0] // quarter
    for part in range(2):
        for half, w_ref in ((0, w_own_ref), (1, w_other_ref)):
            total = None
            for x_ref, shift in zip(x_refs[3 * part : 3 * part + 3], (0, chips - 1, 1)):
                at = pl.multiple_of(lax.rem(chip + shift, chips) * quarter, quarter)
                term = dot(x_ref[...], w_ref[pl.ds(at, quarter), :])
                total = term if total is None else total + term
            acc_ref[part, :, half * wide : (half + 1) * wide] = total


def hidden_kernel(place_ref, far0_ref, far1_ref, acc_ref, w_own_ref, w_other_ref, out_ref):
    core = place_ref[1]
    wide = w_own_ref.shape[1]
    hs = wide // 2
    for part, far_ref in enumerate((far0_ref, far1_ref)):
        for half, w_ref, slot in ((0, w_own_ref, core), (1, w_other_ref, 1 - core)):
            total = acc_ref[part, :, half * wide : (half + 1) * wide]
            total = total + dot(far_ref[...], w_ref[...])
            gate, up = total[:, :hs], total[:, hs:]
            value = (gate / (1.0 + jnp.exp(-gate)) * up).astype(bf16)
            out_ref[part, :, pl.ds(pl.multiple_of(slot * hs, hs), hs)] = value


def down_kernel(place_ref, h0_ref, h1_ref, h2_ref, h3_ref, w_own_ref, w_other_ref, out_ref, line):
    chip = place_ref[0]
    depth, cols = h0_ref.shape[1], w_own_ref.shape[1]
    chips = w_own_ref.shape[0] // depth
    parts = ((h0_ref, 0), (h1_ref, chips - 1), (h2_ref, 1), (h3_ref, chips // 2))
    for h_ref, shift in parts:
        at = pl.multiple_of(lax.rem(chip + shift, chips) * depth, depth)
        line[:, pl.ds(at, depth)] = h_ref[...]
    for part, w_ref in enumerate((w_own_ref, w_other_ref)):
        total = dot(line[...], w_ref[...]).astype(bf16)
        out_ref[:, part] = total.reshape(out_ref.shape[0], out_ref.shape[2], cols)


def shared_kernel(place_ref, x_ref, *refs):
    groups, outs, (line,) = (refs[:4], refs[4:8]), refs[8:13], refs[13:]
    gate_ref, up_ref, hid_ref, sd_ref, sd_out_ref = outs
    core, z, y = place_ref[1], place_ref[2], place_ref[3]
    hs = gate_ref.shape[1]
    side, size = groups[0][0].shape[0], line.shape[0] // 16
    deep = sd_ref.shape[0] // 16
    for h, out_ref in ((0, gate_ref), (1, up_ref)):
        for m, ref in enumerate(groups[h]):
            for n in range(side):
                dz, dy = (m, n) if h == 0 else (n, m)
                source = lax.rem(z + side - dz, side) * side + lax.rem(y + side - dy, side)
                block = ref[n, :size, :]
                at = pl.ds(pl.multiple_of(source * size, size), size)
                out_ref[at, :] = block
                line[at, h * hs : (h + 1) * hs] = block
                at = pl.ds(pl.multiple_of(source * deep, deep), deep)
                for c in range(2):
                    col = (2 * h + c) * hs
                    sd_ref[at, col : col + hs] = ref[n, size + c * deep : size + (c + 1) * deep, :]
    for c in range(4):
        at = pl.ds(pl.multiple_of((2 * c + 1 - core) * hs, hs), hs)
        sd_out_ref[c * hs : (c + 1) * hs, :] = sd_ref[at, :]
    total = dot(x_ref[...], line[...])
    gate, up = total[:, :hs], total[:, hs:]
    hid_ref[...] = (gate / (1.0 + jnp.exp(-gate)) * up).astype(bf16)


def base_kernel(place_ref, own_ref, other_ref, sd_ref, out_ref, line):
    chip, core = place_ref[0], place_ref[1]
    hs = own_ref.shape[2]
    for ref, lane in ((own_ref, core), (other_ref, 1 - core)):
        for n, shift in enumerate((0, 3, 1, 2)):
            at = pl.multiple_of((lax.rem(chip + shift, 4) * 2 + lane) * hs, hs)
            line[:, pl.ds(at, hs)] = ref[n]
    out_ref[...] = dot(line[...], sd_ref[...])


def mix_kernel(weight_ref, got_ref, base_ref, out_ref):
    out_ref[...] = (base_ref[...] + dot(weight_ref[...], got_ref[...])).astype(out_ref.dtype)


def chunk_kernel(place_ref, own_ref, other_ref, sd_ref, sd_other_ref, *out_refs):
    chip, core = place_ref[0], place_ref[1]
    hs, cols = out_refs[0].shape[0] // 2, own_ref.shape[1]
    for n, out_ref in enumerate(out_refs):
        target = lax.rem(chip + n, 4)
        at = pl.ds(pl.multiple_of((target * 2 + core) * hs, hs), hs)
        far = pl.ds(pl.multiple_of(target * hs, hs), hs)
        out_ref[:hs, :cols] = own_ref[at, :]
        out_ref[:hs, cols:] = other_ref[at, :]
        out_ref[hs:, :cols] = sd_ref[at, :]
        out_ref[hs:, cols:] = sd_other_ref[far, :]


def join_kernel(place_ref, p0_ref, p1_ref, p2_ref, p3_ref, routed_ref, shared_ref):
    chip, core = place_ref[0], place_ref[1]
    hs = routed_ref.shape[0]
    cols = p0_ref.shape[1] // 2
    for shift, ref in enumerate((p0_ref, p1_ref, p2_ref, p3_ref)):
        source = lax.rem(chip + 4 - shift, 4)
        for half, lane in ((0, core), (1, 1 - core)):
            at = pl.multiple_of((source * 2 + lane) * cols, cols)
            block = ref[:, half * cols : (half + 1) * cols]
            routed_ref[:, pl.ds(at, cols)] = block[:hs]
            shared_ref[:, pl.ds(at, cols)] = block[hs:]


def whole(shape):
    return pl.BlockSpec(shape, lambda *_: (0,) * len(shape))


def on_device(
    tokens,
    norm_gain,
    gate_train,
    up_train,
    down_train,
    shared_gate_train,
    shared_up_train,
    shared_down_train,
    route_expert,
    route_weight,
):
    experts = lax.axis_size("fs")
    tp = lax.axis_size("tp")
    t = lax.axis_index("tp")
    chips = tp // 2
    chip, core = t // 2, t % 2
    tok_rows, width = tokens.shape
    top_count = route_expert.shape[1]
    cap = 3 * tok_rows * top_count // (2 * experts)
    half = cap // 2
    rows = experts * half
    quarter = width // chips
    cols = width // tp
    hs = gate_train.shape[2]
    deep = down_train.shape[1]

    def shift_by(a, n):
        return lax.ppermute(a, "tp", [(i, (i + 2 * n) % tp) for i in range(tp)])

    def swap(a):
        return lax.ppermute(a, "tp", [(i, i ^ 1) for i in range(tp)])

    gain = norm_gain[:, None]
    side = 4
    f = lax.axis_index("fs")
    place = jnp.stack([chip, core, f // side, f % side]).astype(jnp.int32)

    def along(a, n, y):
        pairs = []
        for i in range(experts):
            z_at, y_at = i // side, i % side
            to = z_at * side + (y_at + n) % side if y else ((z_at + n) % side) * side + y_at
            pairs.append((i, to))
        return lax.ppermute(a, "fs", pairs)

    shared_down_local = shared_down_train.astype(bf16)

    def pack(train, half_at):
        first_col = half_at * cols // 2
        return jnp.concatenate(
            [(gain * train).astype(bf16)]
            + [shared_down_local[:, first_col + c : first_col + c + hs] for c in (0, hs)],
            axis=0,
        )

    packs = (pack(shared_gate_train, 0), pack(shared_up_train, 1))
    groups = [[p] for p in packs]
    for n in range(1, side):
        for h, group in enumerate(groups):
            group.append(along(packs[h], n, h == 0))
    groups = [[jnp.stack(g)] for g in groups]
    for n in range(1, side):
        for h, group in enumerate(groups):
            group.append(along(group[0], n, h == 1))

    steps = 8
    anywhere = pl.BlockSpec(memory_space=pl.ANY)
    normed, outgoing, slots = pl.pallas_call(
        functools.partial(dispatch_kernel, half),
        grid_spec=pltpu.PrefetchScalarGridSpec(
            num_scalar_prefetch=1,
            grid=(1,),
            in_specs=[whole((top_count, tok_rows)), anywhere],
            out_specs=[anywhere, whole((rows, quarter)), whole((top_count, tok_rows))],
            scratch_shapes=[
                pltpu.VMEM((tok_rows, width), bf16),
                pltpu.VMEM((tok_rows, width), bf16),
                pltpu.VMEM((tok_rows, quarter), bf16),
                pltpu.VMEM((rows, tok_rows), bf16),
                pltpu.SemaphoreType.DMA((steps,)),
                pltpu.SemaphoreType.DMA((steps,)),
            ],
        ),
        out_shape=[
            jax.ShapeDtypeStruct((tok_rows, width), bf16),
            jax.ShapeDtypeStruct((rows, quarter), bf16),
            jax.ShapeDtypeStruct((top_count, tok_rows), jnp.int32),
        ],
        compiler_params=vmem_limit(60),
        cost_estimate=cost(2 * rows * tok_rows * quarter, 4 * tok_rows * width),
    )(place, route_expert.T, tokens)
    arriving = lax.all_to_all(
        outgoing.reshape(experts, half, quarter), "fs", split_axis=0, concat_axis=0, tiled=True
    )

    gu_local = jnp.concatenate(
        [(gain[None] * gate_train).astype(bf16), (gain[None] * up_train).astype(bf16)], axis=2
    )
    mid = rows // 2
    arriving = arriving.reshape(rows, quarter)
    top, bottom = together(arriving[:mid], arriving[mid:])
    gu_local, top, bottom = together(gu_local, top, bottom)
    gu = lax.all_to_all(gu_local, "fs", split_axis=0, concat_axis=0, tiled=True)
    down_local, gu = together(down_train.astype(bf16), gu)
    down_cols = lax.all_to_all(down_local, "fs", split_axis=0, concat_axis=0, tiled=True)
    gu = gu.reshape(width, 2 * hs)
    gu_other = swap(gu)
    down_cols = down_cols.reshape(experts * deep, cols)
    down_other = swap(down_cols)

    left_top = shift_by(top, 1)
    right_bottom = shift_by(bottom, -1)
    right_top = shift_by(top, -1)
    left_bottom = shift_by(bottom, 1)
    far_top = shift_by(left_top, 1)
    far_bottom = shift_by(right_bottom, -1)

    def marker(a, b):
        return pl.pallas_call(
            mark_kernel,
            grid=(1,),
            in_specs=[whole(tile)] * 2,
            out_specs=whole(tile),
            out_shape=jax.ShapeDtypeStruct(tile, bf16),
            cost_estimate=cost(1 << 20, 1 << 14),
        )(a, b)

    tile = (16, 128)
    mark = marker(left_top, right_bottom)
    soon = marker(*packs)
    mark = marker(mark, soon)
    x_spec = pl.BlockSpec((mid // 2, quarter), lambda i, s: (i, 0))
    acc_spec = pl.BlockSpec((2, mid // 2, 4 * hs), lambda i, s: (0, i, 0))
    w_spec = pl.BlockSpec((quarter, 2 * hs), lambda i, s: (lax.rem(s[0] + chips // 2, chips), 0))
    acc = pl.pallas_call(
        first_kernel,
        grid_spec=pltpu.PrefetchScalarGridSpec(
            num_scalar_prefetch=1,
            grid=(2,),
            in_specs=[x_spec] * 6 + [whole((width, 2 * hs))] * 2 + [whole(tile)],
            out_specs=acc_spec,
        ),
        out_shape=jax.ShapeDtypeStruct((2, mid, 4 * hs), f32),
        compiler_params=vmem_limit(32),
        cost_estimate=cost(2 * rows * 3 * quarter * 4 * hs, 8 * width * hs),
    )(place, top, left_top, right_top, bottom, left_bottom, right_bottom, gu, gu_other, mark)
    hidden = pl.pallas_call(
        hidden_kernel,
        grid_spec=pltpu.PrefetchScalarGridSpec(
            num_scalar_prefetch=1,
            grid=(1,),
            in_specs=[whole((mid, quarter))] * 2 + [whole((2, mid, 4 * hs)), w_spec, w_spec],
            out_specs=whole((2, mid, 2 * hs)),
        ),
        out_shape=jax.ShapeDtypeStruct((2, mid, 2 * hs), bf16),
        compiler_params=vmem_limit(32),
        cost_estimate=cost(2 * rows * quarter * 4 * hs, 8 * quarter * hs),
    )(place, far_top, far_bottom, acc, gu, gu_other).reshape(rows, 2 * hs)

    shared_gate, shared_up, shared_hid, shared_cols, shared_out = pl.pallas_call(
        shared_kernel,
        grid_spec=pltpu.PrefetchScalarGridSpec(
            num_scalar_prefetch=1,
            grid=(1,),
            in_specs=[whole((tok_rows, width))] + [whole(groups[0][0].shape)] * 8,
            out_specs=[
                whole((width, hs)),
                whole((width, hs)),
                whole((tok_rows, hs)),
                whole((experts * deep, cols)),
                whole((experts * deep // 2, cols)),
            ],
            scratch_shapes=[pltpu.VMEM((width, 2 * hs), bf16)],
        ),
        out_shape=[
            jax.ShapeDtypeStruct((width, hs), bf16),
            jax.ShapeDtypeStruct((width, hs), bf16),
            jax.ShapeDtypeStruct((tok_rows, hs), bf16),
            jax.ShapeDtypeStruct((experts * deep, cols), bf16),
            jax.ShapeDtypeStruct((experts * deep // 2, cols), bf16),
        ],
        compiler_params=vmem_limit(36),
        cost_estimate=cost(4 * tok_rows * width * hs, 8 * width * hs),
    )(place, normed, *groups[0], *groups[1])
    shared_other = swap(shared_out)
    units = [shared_hid]
    for n in (1, -1, 2):
        units.append(shift_by(shared_hid, n))
    units = jnp.stack(units)
    units_other = swap(units)

    hid_left = shift_by(hidden, 1)
    hid_right = shift_by(hidden, -1)
    hid_far = shift_by(hidden, 2)
    sums = pl.pallas_call(
        down_kernel,
        grid_spec=pltpu.PrefetchScalarGridSpec(
            num_scalar_prefetch=1,
            grid=(1,),
            in_specs=[whole((rows, 2 * hs))] * 4 + [whole((experts * deep, cols))] * 2,
            out_specs=whole((experts, 2, half, cols)),
            scratch_shapes=[pltpu.VMEM((rows, experts * deep), bf16)],
        ),
        out_shape=jax.ShapeDtypeStruct((experts, 2, half, cols), bf16),
        compiler_params=vmem_limit(40),
        cost_estimate=cost(4 * rows * experts * deep * cols, 8 * experts * deep * cols),
    )(place, hidden, hid_left, hid_right, hid_far, down_cols, down_other)
    returned = lax.all_to_all(sums, "fs", split_axis=0, concat_axis=0, tiled=True)
    got_other = swap(returned[:, 1].reshape(rows, cols))
    got_own = returned[:, 0].reshape(rows, cols)

    spots = jnp.arange(rows, dtype=jnp.int32)[None, :]

    def mixing(which):
        weights = 0
        for k in range(top_count):
            local = slots[k] - which * half
            here = (local >= 0) & (local < half)
            target = jnp.where(here, route_expert[:, k] * half + local, -1)
            at = target[:, None] == spots
            weights = weights + jnp.where(at, route_weight[:, k][:, None].astype(bf16), 0)
        return weights

    mix_own, mix_other = together(mixing(core), mixing(1 - core))

    def mix(weights, got, base, dtype):
        return pl.pallas_call(
            mix_kernel,
            out_shape=jax.ShapeDtypeStruct((tok_rows, cols), dtype),
            compiler_params=vmem_limit(24),
            cost_estimate=cost(2 * tok_rows * rows * cols, 4 * tok_rows * rows),
        )(weights, got, base)

    base = pl.pallas_call(
        base_kernel,
        grid_spec=pltpu.PrefetchScalarGridSpec(
            num_scalar_prefetch=1,
            grid=(1,),
            in_specs=[whole((chips, tok_rows, hs))] * 2 + [whole((experts * deep, cols))],
            out_specs=whole((tok_rows, cols)),
            scratch_shapes=[pltpu.VMEM((tok_rows, experts * deep), bf16)],
        ),
        out_shape=jax.ShapeDtypeStruct((tok_rows, cols), f32),
        compiler_params=vmem_limit(24),
        cost_estimate=cost(2 * tok_rows * experts * deep * cols, 4 * tok_rows * rows),
    )(place, units, units_other, shared_cols)
    part = mix(mix_own, got_own, base, f32)
    mixed = mix(mix_other, got_other, part, bf16)

    chunks = pl.pallas_call(
        chunk_kernel,
        grid_spec=pltpu.PrefetchScalarGridSpec(
            num_scalar_prefetch=1,
            grid=(1,),
            in_specs=[whole((experts * deep, cols))] * 2
            + [whole((experts * deep, cols)), whole((experts * deep // 2, cols))],
            out_specs=[whole((2 * hs, 2 * cols))] * chips,
        ),
        out_shape=[jax.ShapeDtypeStruct((2 * hs, 2 * cols), bf16)] * chips,
        compiler_params=vmem_limit(36),
        cost_estimate=cost(1 << 30, 8 * hs * width),
    )(place, down_cols, down_other, shared_cols, shared_other)
    pieces = [chunks[0]]
    for n in range(1, chips):
        pieces.append(shift_by(chunks[n], n))
    expert_down, shared_down = pl.pallas_call(
        join_kernel,
        grid_spec=pltpu.PrefetchScalarGridSpec(
            num_scalar_prefetch=1,
            grid=(1,),
            in_specs=[whole((2 * hs, 2 * cols))] * 4,
            out_specs=[whole((hs, width))] * 2,
        ),
        out_shape=[jax.ShapeDtypeStruct((hs, width), bf16)] * 2,
        compiler_params=vmem_limit(24),
        cost_estimate=cost(1 << 20, 8 * hs * width),
    )(place, *pieces)
    expert_gate = gu[None, :, :hs]
    expert_up = gu[None, :, hs:]
    return (
        expert_gate,
        expert_up,
        expert_down[None],
        shared_gate,
        shared_up,
        shared_down,
        mixed,
    )


def solution(mesh):
    placed = (
        P("fs", None),
        P("fs"),
        P(None, "fs", "tp"),
        P(None, "fs", "tp"),
        P(None, "fs", "tp"),
        P("fs", "tp"),
        P("fs", "tp"),
        P("fs", "tp"),
        P("fs", None),
        P("fs", None),
    )

    return jax.shard_map(
        on_device,
        mesh=mesh,
        in_specs=placed,
        out_specs=(
            P("fs", None, "tp"),
            P("fs", None, "tp"),
            P("fs", "tp", None),
            P(None, "tp"),
            P(None, "tp"),
            P("tp", None),
            P("fs", "tp"),
        ),
        check_vma=False,
    )
```

```python
import functools

import jax
import jax.numpy as jnp
from jax import lax
from jax.experimental import pallas as pl
from jax.experimental.pallas import tpu as pltpu
from jax.sharding import PartitionSpec as P

norm_eps = 1e-06
bf16 = jnp.bfloat16
f32 = jnp.float32


def dot(a, b):
    return jnp.dot(a, b, preferred_element_type=f32)


def together(*values):
    return lax.optimization_barrier(values)


def cost(flops, moved):
    return pl.CostEstimate(flops=flops, bytes_accessed=moved, transcendentals=0)


def vmem_limit(mib):
    return pltpu.CompilerParams(vmem_limit_bytes=mib << 20)


def dispatch_kernel(half, place_ref, route_ref, tok_ref, normed_ref, *refs):
    out_refs, slot_ref, scratch = refs[:2], refs[2], refs[3:]
    taken, given, kept, placing, in_sem, out_sem = scratch
    chip, core = place_ref[0], place_ref[1]
    steps = in_sem.shape[0]
    tok_rows = taken.shape[0]
    rows = tok_rows // steps
    quarter = out_refs[0].shape[1]
    spots = placing.shape[0]
    few = half // 2
    experts = spots // half

    def span(step):
        return pl.ds(step * rows, rows)

    reads = [
        pltpu.make_async_copy(tok_ref.at[span(i)], taken.at[span(i)], in_sem.at[i])
        for i in range(steps)
    ]
    writes = [
        pltpu.make_async_copy(given.at[span(i)], normed_ref.at[span(i)], out_sem.at[i])
        for i in range(steps)
    ]
    for read in reads:
        read.start()

    ids = lax.broadcasted_iota(jnp.int32, (experts, tok_rows), 0)
    hot = [route_ref[k : k + 1, :] == ids for k in range(route_ref.shape[0])]
    named = sum(jnp.where(x, 1.0, 0.0) for x in hot).astype(bf16)
    ahead = lax.broadcasted_iota(jnp.int32, (tok_rows, tok_rows), 0) < (
        lax.broadcasted_iota(jnp.int32, (tok_rows, tok_rows), 1)
    )
    earlier = dot(named, jnp.where(ahead, 1.0, 0.0).astype(bf16))
    spot = lax.broadcasted_iota(jnp.int32, (spots, tok_rows), 0)
    total = jnp.zeros((spots, tok_rows), f32)
    for k, x in enumerate(hot):
        slot = jnp.sum(jnp.where(x, earlier, 0.0), axis=0, keepdims=True).astype(jnp.int32)
        slot_ref[k : k + 1, :] = slot
        local = slot - core * half
        here = (local >= 0) & (local < half)
        line = route_ref[k : k + 1, :] * few + local
        line = jnp.where(local < few, line, line + (spots // 2 - few))
        target = jnp.where(here, line, -1)
        total = total + jnp.where(spot == target, 1.0, 0.0)
    placing[...] = total.astype(bf16)

    at = pl.multiple_of(chip * quarter, quarter)
    for i in range(steps):
        reads[i].wait()
        for r in range(i * rows, (i + 1) * rows, 16):
            values = taken[r : r + 16, :].astype(f32)
            scale = lax.rsqrt(jnp.mean(values * values, axis=1, keepdims=True) + norm_eps)
            given[r : r + 16, :] = (values * scale).astype(bf16)
        kept[i * rows : (i + 1) * rows, :] = given[i * rows : (i + 1) * rows, pl.ds(at, quarter)]
        if i:
            writes[i - 1].start()
    for c in range(0, spots, 192):
        part, at = divmod(c, spots // 2)
        block = dot(placing[c : c + 192, :], kept[...])
        out_refs[part][at : at + 192, :] = block.astype(bf16)
    writes[steps - 1].start()
    for write in writes:
        write.wait()


def mark_kernel(a_ref, b_ref, out_ref):
    out_ref[...] = a_ref[...] + b_ref[...]


def first_kernel(place_ref, *refs):
    x_refs, w_ref, acc_ref = refs[:6], refs[6], refs[-1]
    chip = place_ref[0]
    quarter = x_refs[0].shape[1]
    chips = w_ref.shape[0] // quarter
    for part in range(2):
        total = None
        for x_ref, shift in zip(x_refs[3 * part : 3 * part + 3], (0, chips - 1, 1)):
            at = pl.multiple_of(lax.rem(chip + shift, chips) * quarter, quarter)
            term = dot(x_ref[...], w_ref[pl.ds(at, quarter), :])
            total = term if total is None else total + term
        acc_ref[part] = total


def hidden_kernel(place_ref, far0_ref, far1_ref, acc0_ref, acc1_ref, w0_ref, w1_ref, out_ref):
    core = place_ref[1]
    hs = w0_ref.shape[1] // 2
    for acc_ref, w_ref, slot in ((acc0_ref, w0_ref, core), (acc1_ref, w1_ref, 1 - core)):
        at = pl.ds(pl.multiple_of(slot * hs, hs), hs)
        for part, far_ref in enumerate((far0_ref, far1_ref)):
            total = acc_ref[part] + dot(far_ref[...], w_ref[...])
            gate, up = total[:, :hs], total[:, hs:]
            out_ref[part, :, at] = (gate / (1.0 + jnp.exp(-gate)) * up).astype(bf16)


def down_kernel(place_ref, h0_ref, h1_ref, h2_ref, h3_ref, w_own_ref, w_other_ref, out_ref, line):
    chip = place_ref[0]
    depth, cols = h0_ref.shape[1], w_own_ref.shape[1]
    chips = w_own_ref.shape[0] // depth
    parts = ((h0_ref, 0), (h1_ref, chips - 1), (h2_ref, 1), (h3_ref, chips // 2))
    for h_ref, shift in parts:
        at = pl.multiple_of(lax.rem(chip + shift, chips) * depth, depth)
        line[:, pl.ds(at, depth)] = h_ref[...]
    for part, w_ref in enumerate((w_own_ref, w_other_ref)):
        total = dot(line[...], w_ref[...])
        total = total.reshape(2, out_ref.shape[0], out_ref.shape[3], cols).astype(bf16)
        out_ref[:, part, 0] = total[0]
        out_ref[:, part, 1] = total[1]


def shared_kernel(place_ref, x_ref, *refs):
    groups, outs, (line,) = (refs[:4], refs[4:8]), refs[8:13], refs[13:]
    gate_ref, up_ref, hid_ref, sd_ref, sd_out_ref = outs
    core, z, y = place_ref[1], place_ref[2], place_ref[3]
    hs = gate_ref.shape[1]
    side, size = groups[0][0].shape[0], line.shape[0] // 16
    deep = sd_ref.shape[0] // 16
    for h, out_ref in ((0, gate_ref), (1, up_ref)):
        for m, ref in enumerate(groups[h]):
            for n in range(side):
                dz, dy = (m, n) if h == 0 else (n, m)
                source = lax.rem(z + side - dz, side) * side + lax.rem(y + side - dy, side)
                block = ref[n, :size, :]
                at = pl.ds(pl.multiple_of(source * size, size), size)
                out_ref[at, :] = block
                line[at, h * hs : (h + 1) * hs] = block
                at = pl.ds(pl.multiple_of(source * deep, deep), deep)
                for c in range(2):
                    col = (2 * h + c) * hs
                    sd_ref[at, col : col + hs] = ref[n, size + c * deep : size + (c + 1) * deep, :]
    for c in range(4):
        at = pl.ds(pl.multiple_of((2 * c + 1 - core) * hs, hs), hs)
        sd_out_ref[c * hs : (c + 1) * hs, :] = sd_ref[at, :]
    total = dot(x_ref[...], line[...])
    gate, up = total[:, :hs], total[:, hs:]
    hid_ref[...] = (gate / (1.0 + jnp.exp(-gate)) * up).astype(bf16)


def base_kernel(place_ref, own_ref, other_ref, sd_ref, out_ref, line):
    chip, core = place_ref[0], place_ref[1]
    hs = own_ref.shape[2]
    for ref, lane in ((own_ref, core), (other_ref, 1 - core)):
        for n, shift in enumerate((0, 3, 1, 2)):
            at = pl.multiple_of((lax.rem(chip + shift, 4) * 2 + lane) * hs, hs)
            line[:, pl.ds(at, hs)] = ref[n]
    out_ref[...] = dot(line[...], sd_ref[...])


def mix_kernel(weight_ref, got_ref, base_ref, out_ref):
    got = got_ref[...].reshape(weight_ref.shape[1], out_ref.shape[1])
    out_ref[...] = (base_ref[...] + dot(weight_ref[...], got)).astype(out_ref.dtype)


def chunk_kernel(place_ref, own_ref, other_ref, sd_ref, sd_other_ref, *out_refs):
    chip, core = place_ref[0], place_ref[1]
    hs, cols = out_refs[0].shape[0] // 2, own_ref.shape[1]
    for n, out_ref in enumerate(out_refs):
        target = lax.rem(chip + n, 4)
        at = pl.ds(pl.multiple_of((target * 2 + core) * hs, hs), hs)
        far = pl.ds(pl.multiple_of(target * hs, hs), hs)
        out_ref[:hs, :cols] = own_ref[at, :]
        out_ref[:hs, cols:] = other_ref[at, :]
        out_ref[hs:, :cols] = sd_ref[at, :]
        out_ref[hs:, cols:] = sd_other_ref[far, :]


def join_kernel(place_ref, p0_ref, p1_ref, p2_ref, p3_ref, routed_ref, shared_ref):
    chip, core = place_ref[0], place_ref[1]
    hs = routed_ref.shape[0]
    cols = p0_ref.shape[1] // 2
    for shift, ref in enumerate((p0_ref, p1_ref, p2_ref, p3_ref)):
        source = lax.rem(chip + 4 - shift, 4)
        for half, lane in ((0, core), (1, 1 - core)):
            at = pl.multiple_of((source * 2 + lane) * cols, cols)
            block = ref[:, half * cols : (half + 1) * cols]
            routed_ref[:, pl.ds(at, cols)] = block[:hs]
            shared_ref[:, pl.ds(at, cols)] = block[hs:]


def whole(shape):
    return pl.BlockSpec(shape, lambda *_: (0,) * len(shape))


def on_device(
    tokens,
    norm_gain,
    gate_train,
    up_train,
    down_train,
    shared_gate_train,
    shared_up_train,
    shared_down_train,
    route_expert,
    route_weight,
):
    experts = lax.axis_size("fs")
    tp = lax.axis_size("tp")
    t = lax.axis_index("tp")
    chips = tp // 2
    chip, core = t // 2, t % 2
    tok_rows, width = tokens.shape
    top_count = route_expert.shape[1]
    cap = 3 * tok_rows * top_count // (2 * experts)
    half = cap // 2
    rows = experts * half
    quarter = width // chips
    cols = width // tp
    hs = gate_train.shape[2]
    deep = down_train.shape[1]

    def shift_by(a, n):
        return lax.ppermute(a, "tp", [(i, (i + 2 * n) % tp) for i in range(tp)])

    def swap(a):
        return lax.ppermute(a, "tp", [(i, i ^ 1) for i in range(tp)])

    gain = norm_gain[:, None]
    side = 4
    f = lax.axis_index("fs")
    place = jnp.stack([chip, core, f // side, f % side]).astype(jnp.int32)

    def along(a, n, y):
        pairs = []
        for i in range(experts):
            z_at, y_at = i // side, i % side
            to = z_at * side + (y_at + n) % side if y else ((z_at + n) % side) * side + y_at
            pairs.append((i, to))
        return lax.ppermute(a, "fs", pairs)

    shared_down_local = shared_down_train.astype(bf16)

    def pack(train, half_at):
        first_col = half_at * cols // 2
        return jnp.concatenate(
            [(gain * train).astype(bf16)]
            + [shared_down_local[:, first_col + c : first_col + c + hs] for c in (0, hs)],
            axis=0,
        )

    packs = (pack(shared_gate_train, 0), pack(shared_up_train, 1))
    groups = [[p] for p in packs]
    for n in range(1, side):
        for h, group in enumerate(groups):
            group.append(along(packs[h], n, h == 0))
    groups = [[jnp.stack(g)] for g in groups]
    for n in range(1, side):
        for h, group in enumerate(groups):
            group.append(along(group[0], n, h == 1))

    steps = 8
    anywhere = pl.BlockSpec(memory_space=pl.ANY)
    normed, out_top, out_bottom, slots = pl.pallas_call(
        functools.partial(dispatch_kernel, half),
        grid_spec=pltpu.PrefetchScalarGridSpec(
            num_scalar_prefetch=1,
            grid=(1,),
            in_specs=[whole((top_count, tok_rows)), anywhere],
            out_specs=[
                anywhere,
                whole((rows // 2, quarter)),
                whole((rows // 2, quarter)),
                whole((top_count, tok_rows)),
            ],
            scratch_shapes=[
                pltpu.VMEM((tok_rows, width), bf16),
                pltpu.VMEM((tok_rows, width), bf16),
                pltpu.VMEM((tok_rows, quarter), bf16),
                pltpu.VMEM((rows, tok_rows), bf16),
                pltpu.SemaphoreType.DMA((steps,)),
                pltpu.SemaphoreType.DMA((steps,)),
            ],
        ),
        out_shape=[
            jax.ShapeDtypeStruct((tok_rows, width), bf16),
            jax.ShapeDtypeStruct((rows // 2, quarter), bf16),
            jax.ShapeDtypeStruct((rows // 2, quarter), bf16),
            jax.ShapeDtypeStruct((top_count, tok_rows), jnp.int32),
        ],
        compiler_params=vmem_limit(60),
        cost_estimate=cost(2 * rows * tok_rows * quarter, 4 * tok_rows * width),
    )(place, route_expert.T, tokens)
    mid = rows // 2

    def sent(a):
        a = a.reshape(experts, half // 2, quarter)
        return lax.all_to_all(a, "fs", split_axis=0, concat_axis=0, tiled=True).reshape(mid, quarter)

    top = sent(out_top)
    out_bottom, top = together(out_bottom, top)
    bottom = sent(out_bottom)

    gu_local = jnp.concatenate(
        [(gain[None] * gate_train).astype(bf16), (gain[None] * up_train).astype(bf16)], axis=2
    )
    gu_local, bottom = together(gu_local, bottom)
    gu = lax.all_to_all(gu_local, "fs", split_axis=0, concat_axis=0, tiled=True)
    down_local, gu = together(down_train.astype(bf16), gu)
    down_cols = lax.all_to_all(down_local, "fs", split_axis=0, concat_axis=0, tiled=True)
    gu = gu.reshape(width, 2 * hs)
    gu_other = swap(gu)
    down_cols = down_cols.reshape(experts * deep, cols)
    down_other = swap(down_cols)

    left_top = shift_by(top, 1)
    right_bottom = shift_by(bottom, -1)
    right_top = shift_by(top, -1)
    left_bottom = shift_by(bottom, 1)
    far_top = shift_by(left_top, 1)
    far_bottom = shift_by(right_bottom, -1)

    def marker(a, b):
        return pl.pallas_call(
            mark_kernel,
            grid=(1,),
            in_specs=[whole(tile)] * 2,
            out_specs=whole(tile),
            out_shape=jax.ShapeDtypeStruct(tile, bf16),
            cost_estimate=cost(1 << 20, 1 << 14),
        )(a, b)

    tile = (16, 128)
    mark = marker(left_top, right_bottom)
    soon = marker(*packs)
    mark = marker(mark, soon)
    x_spec = pl.BlockSpec((mid // 2, quarter), lambda i, s: (i, 0))
    acc_spec = pl.BlockSpec((2, mid // 2, 2 * hs), lambda i, s: (0, i, 0))
    w_spec = pl.BlockSpec((quarter, 2 * hs), lambda i, s: (lax.rem(s[0] + chips // 2, chips), 0))

    def first(weight, last):
        blocks = (top, left_top, right_top, bottom, left_bottom, right_bottom)
        return pl.pallas_call(
            first_kernel,
            grid_spec=pltpu.PrefetchScalarGridSpec(
                num_scalar_prefetch=1,
                grid=(2,),
                in_specs=[x_spec] * 6 + [whole((width, 2 * hs)), whole(tile)],
                out_specs=acc_spec,
            ),
            out_shape=jax.ShapeDtypeStruct((2, mid, 2 * hs), f32),
            compiler_params=vmem_limit(32),
            cost_estimate=cost(2 * rows * 3 * quarter * 2 * hs, 4 * width * hs),
        )(place, *blocks, weight, last)

    acc_own = first(gu, mark)
    acc_other = first(gu_other, mark)
    hidden = pl.pallas_call(
        hidden_kernel,
        grid_spec=pltpu.PrefetchScalarGridSpec(
            num_scalar_prefetch=1,
            grid=(1,),
            in_specs=[whole((mid, quarter))] * 2
            + [whole((2, mid, 2 * hs))] * 2
            + [w_spec, w_spec],
            out_specs=whole((2, mid, 2 * hs)),
        ),
        out_shape=jax.ShapeDtypeStruct((2, mid, 2 * hs), bf16),
        compiler_params=vmem_limit(32),
        cost_estimate=cost(2 * rows * quarter * 4 * hs, 8 * quarter * hs),
    )(place, far_top, far_bottom, acc_own, acc_other, gu, gu_other).reshape(rows, 2 * hs)

    shared_gate, shared_up, shared_hid, shared_cols, shared_out = pl.pallas_call(
        shared_kernel,
        grid_spec=pltpu.PrefetchScalarGridSpec(
            num_scalar_prefetch=1,
            grid=(1,),
            in_specs=[whole((tok_rows, width))] + [whole(groups[0][0].shape)] * 8,
            out_specs=[
                whole((width, hs)),
                whole((width, hs)),
                whole((tok_rows, hs)),
                whole((experts * deep, cols)),
                whole((experts * deep // 2, cols)),
            ],
            scratch_shapes=[pltpu.VMEM((width, 2 * hs), bf16)],
        ),
        out_shape=[
            jax.ShapeDtypeStruct((width, hs), bf16),
            jax.ShapeDtypeStruct((width, hs), bf16),
            jax.ShapeDtypeStruct((tok_rows, hs), bf16),
            jax.ShapeDtypeStruct((experts * deep, cols), bf16),
            jax.ShapeDtypeStruct((experts * deep // 2, cols), bf16),
        ],
        compiler_params=vmem_limit(36),
        cost_estimate=cost(4 * tok_rows * width * hs, 8 * width * hs),
    )(place, normed, *groups[0], *groups[1])
    shared_other = swap(shared_out)
    units = [shared_hid]
    for n in (1, -1, 2):
        units.append(shift_by(shared_hid, n))
    units = jnp.stack(units)
    units_other = swap(units)

    hid_left = shift_by(hidden, 1)
    hid_right = shift_by(hidden, -1)
    hid_far = shift_by(hidden, 2)
    sums = pl.pallas_call(
        down_kernel,
        grid_spec=pltpu.PrefetchScalarGridSpec(
            num_scalar_prefetch=1,
            grid=(1,),
            in_specs=[whole((rows, 2 * hs))] * 4 + [whole((experts * deep, cols))] * 2,
            out_specs=whole((experts, 2, 2, half // 2, cols)),
            scratch_shapes=[pltpu.VMEM((rows, experts * deep), bf16)],
        ),
        out_shape=jax.ShapeDtypeStruct((experts, 2, 2, half // 2, cols), bf16),
        compiler_params=vmem_limit(60),
        cost_estimate=cost(4 * rows * experts * deep * cols, 8 * experts * deep * cols),
    )(place, hidden, hid_left, hid_right, hid_far, down_cols, down_other)
    sums = sums.reshape(experts, 2, half, cols)
    returned = lax.all_to_all(sums, "fs", split_axis=0, concat_axis=0, tiled=True)
    got_other = swap(returned[:, 1].reshape(rows, cols))

    spots = jnp.arange(rows, dtype=jnp.int32)[None, :]

    def mixing(which):
        weights = 0
        for k in range(top_count):
            local = slots[k] - which * half
            here = (local >= 0) & (local < half)
            target = jnp.where(here, route_expert[:, k] * half + local, -1)
            at = target[:, None] == spots
            weights = weights + jnp.where(at, route_weight[:, k][:, None].astype(bf16), 0)
        return weights

    mix_own, mix_other = together(mixing(core), mixing(1 - core))

    def mix(weights, got, base, dtype):
        return pl.pallas_call(
            mix_kernel,
            grid=(1,),
            in_specs=[
                whole((tok_rows, rows)),
                whole((experts, 1, half, cols)) if got.ndim == 4 else whole((rows, cols)),
                whole((tok_rows, cols)),
            ],
            out_specs=whole((tok_rows, cols)),
            out_shape=jax.ShapeDtypeStruct((tok_rows, cols), dtype),
            compiler_params=vmem_limit(24),
            cost_estimate=cost(2 * tok_rows * rows * cols, 4 * tok_rows * rows),
        )(weights, got, base)

    base = pl.pallas_call(
        base_kernel,
        grid_spec=pltpu.PrefetchScalarGridSpec(
            num_scalar_prefetch=1,
            grid=(1,),
            in_specs=[whole((chips, tok_rows, hs))] * 2 + [whole((experts * deep, cols))],
            out_specs=whole((tok_rows, cols)),
            scratch_shapes=[pltpu.VMEM((tok_rows, experts * deep), bf16)],
        ),
        out_shape=jax.ShapeDtypeStruct((tok_rows, cols), f32),
        compiler_params=vmem_limit(24),
        cost_estimate=cost(2 * tok_rows * experts * deep * cols, 4 * tok_rows * rows),
    )(place, units, units_other, shared_cols)
    part = mix(mix_own, returned, base, f32)
    mixed = mix(mix_other, got_other, part, bf16)

    chunks = pl.pallas_call(
        chunk_kernel,
        grid_spec=pltpu.PrefetchScalarGridSpec(
            num_scalar_prefetch=1,
            grid=(1,),
            in_specs=[whole((experts * deep, cols))] * 2
            + [whole((experts * deep, cols)), whole((experts * deep // 2, cols))],
            out_specs=[whole((2 * hs, 2 * cols))] * chips,
        ),
        out_shape=[jax.ShapeDtypeStruct((2 * hs, 2 * cols), bf16)] * chips,
        compiler_params=vmem_limit(36),
        cost_estimate=cost(1 << 30, 8 * hs * width),
    )(place, down_cols, down_other, shared_cols, shared_other)
    pieces = [chunks[0]]
    for n in range(1, chips):
        pieces.append(shift_by(chunks[n], n))
    expert_down, shared_down = pl.pallas_call(
        join_kernel,
        grid_spec=pltpu.PrefetchScalarGridSpec(
            num_scalar_prefetch=1,
            grid=(1,),
            in_specs=[whole((2 * hs, 2 * cols))] * 4,
            out_specs=[whole((hs, width))] * 2,
        ),
        out_shape=[jax.ShapeDtypeStruct((hs, width), bf16)] * 2,
        compiler_params=vmem_limit(24),
        cost_estimate=cost(1 << 20, 8 * hs * width),
    )(place, *pieces)
    expert_gate = gu[None, :, :hs]
    expert_up = gu[None, :, hs:]
    return (
        expert_gate,
        expert_up,
        expert_down[None],
        shared_gate,
        shared_up,
        shared_down,
        mixed,
    )


def solution(mesh):
    placed = (
        P("fs", None),
        P("fs"),
        P(None, "fs", "tp"),
        P(None, "fs", "tp"),
        P(None, "fs", "tp"),
        P("fs", "tp"),
        P("fs", "tp"),
        P("fs", "tp"),
        P("fs", None),
        P("fs", None),
    )


    return jax.shard_map(
        on_device,
        mesh=mesh,
        in_specs=placed,
        out_specs=(
            P("fs", None, "tp"),
            P("fs", None, "tp"),
            P("fs", "tp", None),
            P(None, "tp"),
            P(None, "tp"),
            P("tp", None),
            P("fs", "tp"),
        ),
        check_vma=False,
    )
```

```python
import functools

import jax
import jax.numpy as jnp
from jax import lax
from jax.experimental import pallas as pl
from jax.experimental.pallas import tpu as pltpu
from jax.sharding import PartitionSpec as P

norm_eps = 1e-06
bf16 = jnp.bfloat16
f32 = jnp.float32


def dot(a, b):
    return jnp.dot(a, b, preferred_element_type=f32)


def together(*values):
    return lax.optimization_barrier(values)


def cost(flops, moved):
    return pl.CostEstimate(flops=flops, bytes_accessed=moved, transcendentals=0)


def vmem_limit(mib):
    return pltpu.CompilerParams(vmem_limit_bytes=mib << 20)


def dispatch_kernel(half, place_ref, route_ref, tok_ref, normed_ref, out_ref, slot_ref, *scratch):
    taken, given, kept, placing, in_sem, out_sem = scratch
    chip, core = place_ref[0], place_ref[1]
    steps = in_sem.shape[0]
    tok_rows = taken.shape[0]
    rows = tok_rows // steps
    quarter = out_ref.shape[1]
    spots = placing.shape[0]
    experts = spots // half

    def span(step):
        return pl.ds(step * rows, rows)

    reads = [
        pltpu.make_async_copy(tok_ref.at[span(i)], taken.at[span(i)], in_sem.at[i])
        for i in range(steps)
    ]
    writes = [
        pltpu.make_async_copy(given.at[span(i)], normed_ref.at[span(i)], out_sem.at[i])
        for i in range(steps)
    ]
    for read in reads:
        read.start()

    ids = lax.broadcasted_iota(jnp.int32, (experts, tok_rows), 0)
    hot = [route_ref[k : k + 1, :] == ids for k in range(route_ref.shape[0])]
    named = sum(jnp.where(x, 1.0, 0.0) for x in hot).astype(bf16)
    ahead = lax.broadcasted_iota(jnp.int32, (tok_rows, tok_rows), 0) < (
        lax.broadcasted_iota(jnp.int32, (tok_rows, tok_rows), 1)
    )
    earlier = dot(named, jnp.where(ahead, 1.0, 0.0).astype(bf16))
    spot = lax.broadcasted_iota(jnp.int32, (spots, tok_rows), 0)
    total = jnp.zeros((spots, tok_rows), f32)
    for k, x in enumerate(hot):
        slot = jnp.sum(jnp.where(x, earlier, 0.0), axis=0, keepdims=True).astype(jnp.int32)
        slot_ref[k : k + 1, :] = slot
        local = slot - core * half
        here = (local >= 0) & (local < half)
        target = jnp.where(here, route_ref[k : k + 1, :] * half + local, -1)
        total = total + jnp.where(spot == target, 1.0, 0.0)
    placing[...] = total.astype(bf16)

    at = pl.multiple_of(chip * quarter, quarter)
    for i in range(steps):
        reads[i].wait()
        for r in range(i * rows, (i + 1) * rows, 16):
            values = taken[r : r + 16, :].astype(f32)
            scale = lax.rsqrt(jnp.mean(values * values, axis=1, keepdims=True) + norm_eps)
            given[r : r + 16, :] = (values * scale).astype(bf16)
        kept[i * rows : (i + 1) * rows, :] = given[i * rows : (i + 1) * rows, pl.ds(at, quarter)]
        if i:
            writes[i - 1].start()
    for c in range(0, spots, 256):
        out_ref[c : c + 256, :] = dot(placing[c : c + 256, :], kept[...]).astype(bf16)
    writes[steps - 1].start()
    for write in writes:
        write.wait()


def mark_kernel(a_ref, b_ref, out_ref):
    out_ref[...] = a_ref[...] + b_ref[...]


def first_kernel(place_ref, *refs):
    x_refs, (w_own_ref, w_other_ref, _, acc_ref) = refs[:6], refs[6:]
    chip = place_ref[0]
    quarter, wide = x_refs[0].shape[1], w_own_ref.shape[1]
    chips = w_own_ref.shape[0] // quarter
    for part in range(2):
        for half, w_ref in ((0, w_own_ref), (1, w_other_ref)):
            total = None
            for x_ref, shift in zip(x_refs[3 * part : 3 * part + 3], (0, chips - 1, 1)):
                at = pl.multiple_of(lax.rem(chip + shift, chips) * quarter, quarter)
                term = dot(x_ref[...], w_ref[pl.ds(at, quarter), :])
                total = term if total is None else total + term
            acc_ref[part, :, half * wide : (half + 1) * wide] = total


def hidden_kernel(place_ref, far0_ref, far1_ref, acc_ref, w_own_ref, w_other_ref, out_ref):
    core = place_ref[1]
    wide = w_own_ref.shape[1]
    hs = wide // 2
    for part, far_ref in enumerate((far0_ref, far1_ref)):
        for half, w_ref, slot in ((0, w_own_ref, core), (1, w_other_ref, 1 - core)):
            total = acc_ref[part, :, half * wide : (half + 1) * wide]
            total = total + dot(far_ref[...], w_ref[...])
            gate, up = total[:, :hs], total[:, hs:]
            value = (gate / (1.0 + jnp.exp(-gate)) * up).astype(bf16)
            out_ref[part, :, pl.ds(pl.multiple_of(slot * hs, hs), hs)] = value


def down_kernel(place_ref, h0_ref, h1_ref, h2_ref, h3_ref, w_own_ref, w_other_ref, out_ref, line):
    chip = place_ref[0]
    depth, cols = h0_ref.shape[1], w_own_ref.shape[1]
    chips = w_own_ref.shape[0] // depth
    parts = ((h0_ref, 0), (h1_ref, chips - 1), (h2_ref, 1), (h3_ref, chips // 2))

    @pl.when(pl.program_id(0) == 0)
    def _():
        for h_ref, shift in parts:
            at = pl.multiple_of(lax.rem(chip + shift, chips) * depth, depth)
            line[:, pl.ds(at, depth)] = h_ref[...]

    for part, w_ref in enumerate((w_own_ref, w_other_ref)):

        @pl.when(pl.program_id(0) == part)
        def _():
            total = dot(line[...], w_ref[...]).astype(bf16)
            out_ref[:, 0] = total.reshape(out_ref.shape[0], out_ref.shape[2], cols)


def shared_kernel(place_ref, x_ref, *refs):
    groups, outs, (line,) = (refs[:4], refs[4:8]), refs[8:13], refs[13:]
    gate_ref, up_ref, hid_ref, sd_ref, sd_out_ref = outs
    core, z, y = place_ref[1], place_ref[2], place_ref[3]
    hs = gate_ref.shape[1]
    side, size = groups[0][0].shape[0], line.shape[0] // 16
    deep = sd_ref.shape[0] // 16
    for h, out_ref in ((0, gate_ref), (1, up_ref)):
        for m, ref in enumerate(groups[h]):
            for n in range(side):
                dz, dy = (m, n) if h == 0 else (n, m)
                source = lax.rem(z + side - dz, side) * side + lax.rem(y + side - dy, side)
                block = ref[n, :size, :]
                at = pl.ds(pl.multiple_of(source * size, size), size)
                out_ref[at, :] = block
                line[at, h * hs : (h + 1) * hs] = block
                at = pl.ds(pl.multiple_of(source * deep, deep), deep)
                for c in range(2):
                    col = (2 * h + c) * hs
                    sd_ref[at, col : col + hs] = ref[n, size + c * deep : size + (c + 1) * deep, :]
    for c in range(4):
        at = pl.ds(pl.multiple_of((2 * c + 1 - core) * hs, hs), hs)
        sd_out_ref[c * hs : (c + 1) * hs, :] = sd_ref[at, :]
    total = dot(x_ref[...], line[...])
    gate, up = total[:, :hs], total[:, hs:]
    hid_ref[...] = (gate / (1.0 + jnp.exp(-gate)) * up).astype(bf16)


def base_kernel(place_ref, own_ref, other_ref, sd_ref, out_ref, line):
    chip, core = place_ref[0], place_ref[1]
    hs = own_ref.shape[2]
    for ref, lane in ((own_ref, core), (other_ref, 1 - core)):
        for n, shift in enumerate((0, 3, 1, 2)):
            at = pl.multiple_of((lax.rem(chip + shift, 4) * 2 + lane) * hs, hs)
            line[:, pl.ds(at, hs)] = ref[n]
    out_ref[...] = dot(line[...], sd_ref[...])


def mix_kernel(weight_ref, got_ref, base_ref, out_ref):
    got = got_ref[...].reshape(weight_ref.shape[1], out_ref.shape[1])
    out_ref[...] = (base_ref[...] + dot(weight_ref[...], got)).astype(out_ref.dtype)


def chunk_kernel(place_ref, own_ref, other_ref, sd_ref, sd_other_ref, *out_refs):
    chip, core = place_ref[0], place_ref[1]
    hs, cols = out_refs[0].shape[0] // 2, own_ref.shape[1]
    for n, out_ref in enumerate(out_refs):
        target = lax.rem(chip + n, 4)
        at = pl.ds(pl.multiple_of((target * 2 + core) * hs, hs), hs)
        far = pl.ds(pl.multiple_of(target * hs, hs), hs)
        out_ref[:hs, :cols] = own_ref[at, :]
        out_ref[:hs, cols:] = other_ref[at, :]
        out_ref[hs:, :cols] = sd_ref[at, :]
        out_ref[hs:, cols:] = sd_other_ref[far, :]


def join_kernel(place_ref, p0_ref, p1_ref, p2_ref, p3_ref, routed_ref, shared_ref):
    chip, core = place_ref[0], place_ref[1]
    hs = routed_ref.shape[0]
    cols = p0_ref.shape[1] // 2
    for shift, ref in enumerate((p0_ref, p1_ref, p2_ref, p3_ref)):
        source = lax.rem(chip + 4 - shift, 4)
        for half, lane in ((0, core), (1, 1 - core)):
            at = pl.multiple_of((source * 2 + lane) * cols, cols)
            block = ref[:, half * cols : (half + 1) * cols]
            routed_ref[:, pl.ds(at, cols)] = block[:hs]
            shared_ref[:, pl.ds(at, cols)] = block[hs:]


def whole(shape):
    return pl.BlockSpec(shape, lambda *_: (0,) * len(shape))


def on_device(
    tokens,
    norm_gain,
    gate_train,
    up_train,
    down_train,
    shared_gate_train,
    shared_up_train,
    shared_down_train,
    route_expert,
    route_weight,
):
    experts = lax.axis_size("fs")
    tp = lax.axis_size("tp")
    t = lax.axis_index("tp")
    chips = tp // 2
    chip, core = t // 2, t % 2
    tok_rows, width = tokens.shape
    top_count = route_expert.shape[1]
    cap = 3 * tok_rows * top_count // (2 * experts)
    half = cap // 2
    rows = experts * half
    quarter = width // chips
    cols = width // tp
    hs = gate_train.shape[2]
    deep = down_train.shape[1]

    def shift_by(a, n):
        return lax.ppermute(a, "tp", [(i, (i + 2 * n) % tp) for i in range(tp)])

    def swap(a):
        return lax.ppermute(a, "tp", [(i, i ^ 1) for i in range(tp)])

    gain = norm_gain[:, None]
    side = 4
    f = lax.axis_index("fs")
    place = jnp.stack([chip, core, f // side, f % side]).astype(jnp.int32)

    def along(a, n, y):
        pairs = []
        for i in range(experts):
            z_at, y_at = i // side, i % side
            to = z_at * side + (y_at + n) % side if y else ((z_at + n) % side) * side + y_at
            pairs.append((i, to))
        return lax.ppermute(a, "fs", pairs)

    shared_down_local = shared_down_train.astype(bf16)

    def pack(train, half_at):
        first_col = half_at * cols // 2
        return jnp.concatenate(
            [(gain * train).astype(bf16)]
            + [shared_down_local[:, first_col + c : first_col + c + hs] for c in (0, hs)],
            axis=0,
        )

    packs = (pack(shared_gate_train, 0), pack(shared_up_train, 1))
    groups = [[p] for p in packs]
    for n in range(1, side):
        for h, group in enumerate(groups):
            group.append(along(packs[h], n, h == 0))
    groups = [[jnp.stack(g)] for g in groups]
    for n in range(1, side):
        for h, group in enumerate(groups):
            group.append(along(group[0], n, h == 1))

    steps = 8
    anywhere = pl.BlockSpec(memory_space=pl.ANY)
    normed, outgoing, slots = pl.pallas_call(
        functools.partial(dispatch_kernel, half),
        grid_spec=pltpu.PrefetchScalarGridSpec(
            num_scalar_prefetch=1,
            grid=(1,),
            in_specs=[whole((top_count, tok_rows)), anywhere],
            out_specs=[anywhere, whole((rows, quarter)), whole((top_count, tok_rows))],
            scratch_shapes=[
                pltpu.VMEM((tok_rows, width), bf16),
                pltpu.VMEM((tok_rows, width), bf16),
                pltpu.VMEM((tok_rows, quarter), bf16),
                pltpu.VMEM((rows, tok_rows), bf16),
                pltpu.SemaphoreType.DMA((steps,)),
                pltpu.SemaphoreType.DMA((steps,)),
            ],
        ),
        out_shape=[
            jax.ShapeDtypeStruct((tok_rows, width), bf16),
            jax.ShapeDtypeStruct((rows, quarter), bf16),
            jax.ShapeDtypeStruct((top_count, tok_rows), jnp.int32),
        ],
        compiler_params=vmem_limit(60),
        cost_estimate=cost(2 * rows * tok_rows * quarter, 4 * tok_rows * width),
    )(place, route_expert.T, tokens)
    arriving = lax.all_to_all(
        outgoing.reshape(experts, half, quarter), "fs", split_axis=0, concat_axis=0, tiled=True
    )

    gu_local = jnp.concatenate(
        [(gain[None] * gate_train).astype(bf16), (gain[None] * up_train).astype(bf16)], axis=2
    )
    mid = rows // 2
    arriving = arriving.reshape(rows, quarter)
    top, bottom = together(arriving[:mid], arriving[mid:])
    gu_local, top, bottom = together(gu_local, top, bottom)
    gu = lax.all_to_all(gu_local, "fs", split_axis=0, concat_axis=0, tiled=True)
    down_local, gu = together(down_train.astype(bf16), gu)
    down_cols = lax.all_to_all(down_local, "fs", split_axis=0, concat_axis=0, tiled=True)
    gu = gu.reshape(width, 2 * hs)
    gu_other = swap(gu)
    down_cols = down_cols.reshape(experts * deep, cols)
    down_other = swap(down_cols)

    left_top = shift_by(top, 1)
    right_bottom = shift_by(bottom, -1)
    right_top = shift_by(top, -1)
    left_bottom = shift_by(bottom, 1)
    far_top = shift_by(left_top, 1)
    far_bottom = shift_by(right_bottom, -1)

    def marker(a, b):
        return pl.pallas_call(
            mark_kernel,
            grid=(1,),
            in_specs=[whole(tile)] * 2,
            out_specs=whole(tile),
            out_shape=jax.ShapeDtypeStruct(tile, bf16),
            cost_estimate=cost(1 << 20, 1 << 14),
        )(a, b)

    tile = (16, 128)
    mark = marker(left_top, right_bottom)
    soon = marker(*packs)
    mark = marker(mark, soon)
    x_spec = pl.BlockSpec((mid // 2, quarter), lambda i, s: (i, 0))
    acc_spec = pl.BlockSpec((2, mid // 2, 4 * hs), lambda i, s: (0, i, 0))
    w_spec = pl.BlockSpec((quarter, 2 * hs), lambda i, s: (lax.rem(s[0] + chips // 2, chips), 0))
    acc = pl.pallas_call(
        first_kernel,
        grid_spec=pltpu.PrefetchScalarGridSpec(
            num_scalar_prefetch=1,
            grid=(2,),
            in_specs=[x_spec] * 6 + [whole((width, 2 * hs))] * 2 + [whole(tile)],
            out_specs=acc_spec,
        ),
        out_shape=jax.ShapeDtypeStruct((2, mid, 4 * hs), f32),
        compiler_params=vmem_limit(32),
        cost_estimate=cost(2 * rows * 3 * quarter * 4 * hs, 8 * width * hs),
    )(place, top, left_top, right_top, bottom, left_bottom, right_bottom, gu, gu_other, mark)
    hidden = pl.pallas_call(
        hidden_kernel,
        grid_spec=pltpu.PrefetchScalarGridSpec(
            num_scalar_prefetch=1,
            grid=(1,),
            in_specs=[whole((mid, quarter))] * 2 + [whole((2, mid, 4 * hs)), w_spec, w_spec],
            out_specs=whole((2, mid, 2 * hs)),
        ),
        out_shape=jax.ShapeDtypeStruct((2, mid, 2 * hs), bf16),
        compiler_params=vmem_limit(32),
        cost_estimate=cost(2 * rows * quarter * 4 * hs, 8 * quarter * hs),
    )(place, far_top, far_bottom, acc, gu, gu_other).reshape(rows, 2 * hs)

    shared_gate, shared_up, shared_hid, shared_cols, shared_out = pl.pallas_call(
        shared_kernel,
        grid_spec=pltpu.PrefetchScalarGridSpec(
            num_scalar_prefetch=1,
            grid=(1,),
            in_specs=[whole((tok_rows, width))] + [whole(groups[0][0].shape)] * 8,
            out_specs=[
                whole((width, hs)),
                whole((width, hs)),
                whole((tok_rows, hs)),
                whole((experts * deep, cols)),
                whole((experts * deep // 2, cols)),
            ],
            scratch_shapes=[pltpu.VMEM((width, 2 * hs), bf16)],
        ),
        out_shape=[
            jax.ShapeDtypeStruct((width, hs), bf16),
            jax.ShapeDtypeStruct((width, hs), bf16),
            jax.ShapeDtypeStruct((tok_rows, hs), bf16),
            jax.ShapeDtypeStruct((experts * deep, cols), bf16),
            jax.ShapeDtypeStruct((experts * deep // 2, cols), bf16),
        ],
        compiler_params=vmem_limit(36),
        cost_estimate=cost(4 * tok_rows * width * hs, 8 * width * hs),
    )(place, normed, *groups[0], *groups[1])
    shared_other = swap(shared_out)
    units = [shared_hid]
    for n in (1, -1, 2):
        units.append(shift_by(shared_hid, n))
    units = jnp.stack(units)
    units_other = swap(units)

    hid_left = shift_by(hidden, 1)
    hid_right = shift_by(hidden, -1)
    hid_far = shift_by(hidden, 2)
    sums = pl.pallas_call(
        down_kernel,
        grid_spec=pltpu.PrefetchScalarGridSpec(
            num_scalar_prefetch=1,
            grid=(2,),
            in_specs=[whole((rows, 2 * hs))] * 4 + [whole((experts * deep, cols))] * 2,
            out_specs=pl.BlockSpec((experts, 1, half, cols), lambda i, s: (0, i, 0, 0)),
            scratch_shapes=[pltpu.VMEM((rows, experts * deep), bf16)],
        ),
        out_shape=jax.ShapeDtypeStruct((experts, 2, half, cols), bf16),
        compiler_params=vmem_limit(60),
        cost_estimate=cost(4 * rows * experts * deep * cols, 8 * experts * deep * cols),
    )(place, hidden, hid_left, hid_right, hid_far, down_cols, down_other)
    returned = lax.all_to_all(sums, "fs", split_axis=0, concat_axis=0, tiled=True)
    got_other = swap(returned[:, 1].reshape(rows, cols))

    spots = jnp.arange(rows, dtype=jnp.int32)[None, :]

    def mixing(which):
        weights = 0
        for k in range(top_count):
            local = slots[k] - which * half
            here = (local >= 0) & (local < half)
            target = jnp.where(here, route_expert[:, k] * half + local, -1)
            at = target[:, None] == spots
            weights = weights + jnp.where(at, route_weight[:, k][:, None].astype(bf16), 0)
        return weights

    mix_own, mix_other = together(mixing(core), mixing(1 - core))

    def mix(weights, got, base, dtype):
        return pl.pallas_call(
            mix_kernel,
            grid=(1,),
            in_specs=[
                whole((tok_rows, rows)),
                whole((experts, 1, half, cols)) if got.ndim == 4 else whole((rows, cols)),
                whole((tok_rows, cols)),
            ],
            out_specs=whole((tok_rows, cols)),
            out_shape=jax.ShapeDtypeStruct((tok_rows, cols), dtype),
            compiler_params=vmem_limit(24),
            cost_estimate=cost(2 * tok_rows * rows * cols, 4 * tok_rows * rows),
        )(weights, got, base)

    base = pl.pallas_call(
        base_kernel,
        grid_spec=pltpu.PrefetchScalarGridSpec(
            num_scalar_prefetch=1,
            grid=(1,),
            in_specs=[whole((chips, tok_rows, hs))] * 2 + [whole((experts * deep, cols))],
            out_specs=whole((tok_rows, cols)),
            scratch_shapes=[pltpu.VMEM((tok_rows, experts * deep), bf16)],
        ),
        out_shape=jax.ShapeDtypeStruct((tok_rows, cols), f32),
        compiler_params=vmem_limit(24),
        cost_estimate=cost(2 * tok_rows * experts * deep * cols, 4 * tok_rows * rows),
    )(place, units, units_other, shared_cols)
    part = mix(mix_own, returned, base, f32)
    mixed = mix(mix_other, got_other, part, bf16)

    chunks = pl.pallas_call(
        chunk_kernel,
        grid_spec=pltpu.PrefetchScalarGridSpec(
            num_scalar_prefetch=1,
            grid=(1,),
            in_specs=[whole((experts * deep, cols))] * 2
            + [whole((experts * deep, cols)), whole((experts * deep // 2, cols))],
            out_specs=[whole((2 * hs, 2 * cols))] * chips,
        ),
        out_shape=[jax.ShapeDtypeStruct((2 * hs, 2 * cols), bf16)] * chips,
        compiler_params=vmem_limit(36),
        cost_estimate=cost(1 << 30, 8 * hs * width),
    )(place, down_cols, down_other, shared_cols, shared_other)
    pieces = [chunks[0]]
    for n in range(1, chips):
        pieces.append(shift_by(chunks[n], n))
    expert_down, shared_down = pl.pallas_call(
        join_kernel,
        grid_spec=pltpu.PrefetchScalarGridSpec(
            num_scalar_prefetch=1,
            grid=(1,),
            in_specs=[whole((2 * hs, 2 * cols))] * 4,
            out_specs=[whole((hs, width))] * 2,
        ),
        out_shape=[jax.ShapeDtypeStruct((hs, width), bf16)] * 2,
        compiler_params=vmem_limit(24),
        cost_estimate=cost(1 << 20, 8 * hs * width),
    )(place, *pieces)
    expert_gate = gu[None, :, :hs]
    expert_up = gu[None, :, hs:]
    return (
        expert_gate,
        expert_up,
        expert_down[None],
        shared_gate,
        shared_up,
        shared_down,
        mixed,
    )


def solution(mesh):
    placed = (
        P("fs", None),
        P("fs"),
        P(None, "fs", "tp"),
        P(None, "fs", "tp"),
        P(None, "fs", "tp"),
        P("fs", "tp"),
        P("fs", "tp"),
        P("fs", "tp"),
        P("fs", None),
        P("fs", None),
    )


    return jax.shard_map(
        on_device,
        mesh=mesh,
        in_specs=placed,
        out_specs=(
            P("fs", None, "tp"),
            P("fs", None, "tp"),
            P("fs", "tp", None),
            P(None, "tp"),
            P(None, "tp"),
            P("tp", None),
            P("fs", "tp"),
        ),
        check_vma=False,
    )
```

```python
import functools

import jax
import jax.numpy as jnp
from jax import lax
from jax.experimental import pallas as pl
from jax.experimental.pallas import tpu as pltpu
from jax.sharding import PartitionSpec as P

norm_eps = 1e-06
bf16 = jnp.bfloat16
f32 = jnp.float32


def dot(a, b):
    return jnp.dot(a, b, preferred_element_type=f32)


def together(*values):
    return lax.optimization_barrier(values)


def cost(flops, moved):
    return pl.CostEstimate(flops=flops, bytes_accessed=moved, transcendentals=0)


def vmem_limit(mib):
    return pltpu.CompilerParams(vmem_limit_bytes=mib << 20)


def route_kernel(half, route_ref, tok_ref, out_ref, slot_ref, kept, placing, sem):
    t = lax.axis_index("tp")
    chip, core = t // 2, lax.rem(t, 2)
    tok_rows, quarter = kept.shape
    spots = placing.shape[0]
    experts = spots // half
    at = pl.ds(pl.multiple_of(chip * quarter, quarter), quarter)
    read = pltpu.make_async_copy(tok_ref.at[:, at], kept, sem)
    read.start()

    ids = lax.broadcasted_iota(jnp.int32, (experts, tok_rows), 0)
    hot = [route_ref[k : k + 1, :] == ids for k in range(route_ref.shape[0])]
    named = sum(jnp.where(x, 1.0, 0.0) for x in hot).astype(bf16)
    ahead = lax.broadcasted_iota(jnp.int32, (tok_rows, tok_rows), 0) < (
        lax.broadcasted_iota(jnp.int32, (tok_rows, tok_rows), 1)
    )
    earlier = dot(named, jnp.where(ahead, 1.0, 0.0).astype(bf16))
    spot = lax.broadcasted_iota(jnp.int32, (spots, tok_rows), 0)
    total = jnp.zeros((spots, tok_rows), f32)
    for k, x in enumerate(hot):
        slot = jnp.sum(jnp.where(x, earlier, 0.0), axis=0, keepdims=True).astype(jnp.int32)
        slot_ref[k : k + 1, :] = slot
        local = slot - core * half
        here = (local >= 0) & (local < half)
        target = jnp.where(here, route_ref[k : k + 1, :] * half + local, -1)
        total = total + jnp.where(spot == target, 1.0, 0.0)
    placing[...] = total.astype(bf16)
    read.wait()
    for c in range(0, spots, 256):
        out_ref[c : c + 256, :] = dot(placing[c : c + 256, :], kept[...]).astype(bf16)


def norm_kernel(tok_ref, normed_ref, taken, given, in_sem, out_sem):
    steps = in_sem.shape[0]
    rows = taken.shape[0] // steps

    def span(step):
        return pl.ds(step * rows, rows)

    reads = [
        pltpu.make_async_copy(tok_ref.at[span(i)], taken.at[span(i)], in_sem.at[i])
        for i in range(steps)
    ]
    writes = [
        pltpu.make_async_copy(given.at[span(i)], normed_ref.at[span(i)], out_sem.at[i])
        for i in range(steps)
    ]
    for read in reads:
        read.start()
    for i in range(steps):
        reads[i].wait()
        for r in range(i * rows, (i + 1) * rows, 16):
            values = taken[r : r + 16, :].astype(f32)
            scale = lax.rsqrt(jnp.mean(values * values, axis=1, keepdims=True) + norm_eps)
            given[r : r + 16, :] = (values * scale).astype(bf16)
        if i:
            writes[i - 1].start()
    writes[steps - 1].start()
    for write in writes:
        write.wait()


def squares(x_ref):
    total = None
    for c in range(0, x_ref.shape[1], 128):
        values = x_ref[:, c : c + 128].astype(f32)
        total = values * values if total is None else total + values * values
    return total


def mark_kernel(a_ref, b_ref, out_ref):
    out_ref[...] = a_ref[...] + b_ref[...]


def first_kernel(place_ref, *refs):
    x_refs, (w_own_ref, w_other_ref, _, acc_ref, sq_ref) = refs[:6], refs[6:]
    chip = place_ref[0]
    quarter, wide = x_refs[0].shape[1], w_own_ref.shape[1]
    chips = w_own_ref.shape[0] // quarter
    for part in range(2):
        blocks = x_refs[3 * part : 3 * part + 3]
        for half, w_ref in ((0, w_own_ref), (1, w_other_ref)):
            total = None
            for x_ref, shift in zip(blocks, (0, chips - 1, 1)):
                at = pl.multiple_of(lax.rem(chip + shift, chips) * quarter, quarter)
                term = dot(x_ref[...], w_ref[pl.ds(at, quarter), :])
                total = term if total is None else total + term
            acc_ref[part, :, half * wide : (half + 1) * wide] = total
        sq_ref[part] = squares(blocks[0]) + squares(blocks[1]) + squares(blocks[2])


def hidden_kernel(width, place_ref, far0_ref, far1_ref, acc_ref, sq_ref, w0_ref, w1_ref, out_ref):
    core = place_ref[1]
    wide = w0_ref.shape[1]
    hs = wide // 2
    for part, far_ref in enumerate((far0_ref, far1_ref)):
        sums = jnp.sum(sq_ref[part] + squares(far_ref), axis=1, keepdims=True)
        scale = lax.rsqrt(sums * (1.0 / width) + norm_eps)
        for half, w_ref, slot in ((0, w0_ref, core), (1, w1_ref, 1 - core)):
            total = acc_ref[part, :, half * wide : (half + 1) * wide]
            total = (total + dot(far_ref[...], w_ref[...])) * scale
            gate, up = total[:, :hs], total[:, hs:]
            value = (gate / (1.0 + jnp.exp(-gate)) * up).astype(bf16)
            out_ref[part, :, pl.ds(pl.multiple_of(slot * hs, hs), hs)] = value


def down_kernel(place_ref, h0_ref, h1_ref, h2_ref, h3_ref, w_own_ref, w_other_ref, out_ref, line):
    chip = place_ref[0]
    depth, cols = h0_ref.shape[1], w_own_ref.shape[1]
    chips = w_own_ref.shape[0] // depth
    parts = ((h0_ref, 0), (h1_ref, chips - 1), (h2_ref, 1), (h3_ref, chips // 2))
    for h_ref, shift in parts:
        at = pl.multiple_of(lax.rem(chip + shift, chips) * depth, depth)
        line[:, pl.ds(at, depth)] = h_ref[...]
    for part, w_ref in enumerate((w_own_ref, w_other_ref)):
        total = dot(line[...], w_ref[...]).astype(bf16)
        out_ref[:, part] = total.reshape(out_ref.shape[0], out_ref.shape[2], cols)


def shared_kernel(place_ref, x_ref, *refs):
    groups, outs, (line,) = (refs[:4], refs[4:8]), refs[8:13], refs[13:]
    gate_ref, up_ref, hid_ref, sd_ref, sd_out_ref = outs
    core, z, y = place_ref[1], place_ref[2], place_ref[3]
    hs = gate_ref.shape[1]
    side, size = groups[0][0].shape[0], line.shape[0] // 16
    deep = sd_ref.shape[0] // 16
    for h, out_ref in ((0, gate_ref), (1, up_ref)):
        for m, ref in enumerate(groups[h]):
            for n in range(side):
                dz, dy = (m, n) if h == 0 else (n, m)
                source = lax.rem(z + side - dz, side) * side + lax.rem(y + side - dy, side)
                block = ref[n, :size, :]
                at = pl.ds(pl.multiple_of(source * size, size), size)
                out_ref[at, :] = block
                line[at, h * hs : (h + 1) * hs] = block
                at = pl.ds(pl.multiple_of(source * deep, deep), deep)
                for c in range(2):
                    col = (2 * h + c) * hs
                    sd_ref[at, col : col + hs] = ref[n, size + c * deep : size + (c + 1) * deep, :]
    for c in range(4):
        at = pl.ds(pl.multiple_of((2 * c + 1 - core) * hs, hs), hs)
        sd_out_ref[c * hs : (c + 1) * hs, :] = sd_ref[at, :]
    total = dot(x_ref[...], line[...])
    gate, up = total[:, :hs], total[:, hs:]
    hid_ref[...] = (gate / (1.0 + jnp.exp(-gate)) * up).astype(bf16)


def base_kernel(place_ref, own_ref, other_ref, sd_ref, out_ref, line):
    chip, core = place_ref[0], place_ref[1]
    hs = own_ref.shape[2]
    for ref, lane in ((own_ref, core), (other_ref, 1 - core)):
        for n, shift in enumerate((0, 3, 1, 2)):
            at = pl.multiple_of((lax.rem(chip + shift, 4) * 2 + lane) * hs, hs)
            line[:, pl.ds(at, hs)] = ref[n]
    out_ref[...] = dot(line[...], sd_ref[...])


def mix_kernel(weight_ref, got_ref, base_ref, out_ref):
    got = got_ref[...].reshape(weight_ref.shape[1], out_ref.shape[1])
    out_ref[...] = (base_ref[...] + dot(weight_ref[...], got)).astype(out_ref.dtype)


def chunk_kernel(place_ref, own_ref, other_ref, sd_ref, sd_other_ref, *out_refs):
    chip, core = place_ref[0], place_ref[1]
    hs, cols = out_refs[0].shape[0] // 2, own_ref.shape[1]
    for n, out_ref in enumerate(out_refs):
        target = lax.rem(chip + n, 4)
        at = pl.ds(pl.multiple_of((target * 2 + core) * hs, hs), hs)
        far = pl.ds(pl.multiple_of(target * hs, hs), hs)
        out_ref[:hs, :cols] = own_ref[at, :]
        out_ref[:hs, cols:] = other_ref[at, :]
        out_ref[hs:, :cols] = sd_ref[at, :]
        out_ref[hs:, cols:] = sd_other_ref[far, :]


def join_kernel(place_ref, p0_ref, p1_ref, p2_ref, p3_ref, routed_ref, shared_ref, sems):
    chip, core = place_ref[0], place_ref[1]
    hs = routed_ref.shape[0]
    cols = p0_ref.shape[1] // 2
    copies = []
    for shift, ref in enumerate((p0_ref, p1_ref, p2_ref, p3_ref)):
        source = lax.rem(chip + 4 - shift, 4)
        for half, lane in ((0, core), (1, 1 - core)):
            at = pl.ds(pl.multiple_of((source * 2 + lane) * cols, cols), cols)
            part = pl.ds(half * cols, cols)
            for top, out_ref in ((0, routed_ref), (hs, shared_ref)):
                copies.append(
                    pltpu.make_async_copy(
                        ref.at[pl.ds(top, hs), part], out_ref.at[:, at], sems.at[len(copies)]
                    )
                )
    for copy in copies:
        copy.start()
    for copy in copies:
        copy.wait()


def whole(shape):
    return pl.BlockSpec(shape, lambda *_: (0,) * len(shape))


def on_device(
    tokens,
    norm_gain,
    gate_train,
    up_train,
    down_train,
    shared_gate_train,
    shared_up_train,
    shared_down_train,
    route_expert,
    route_weight,
):
    experts = lax.axis_size("fs")
    tp = lax.axis_size("tp")
    t = lax.axis_index("tp")
    chips = tp // 2
    chip, core = t // 2, t % 2
    tok_rows, width = tokens.shape
    top_count = route_expert.shape[1]
    cap = 3 * tok_rows * top_count // (2 * experts)
    half = cap // 2
    rows = experts * half
    quarter = width // chips
    cols = width // tp
    hs = gate_train.shape[2]
    deep = down_train.shape[1]

    def shift_by(a, n):
        return lax.ppermute(a, "tp", [(i, (i + 2 * n) % tp) for i in range(tp)])

    def swap(a):
        return lax.ppermute(a, "tp", [(i, i ^ 1) for i in range(tp)])

    gain = norm_gain[:, None]
    side = 4
    f = lax.axis_index("fs")
    place = jnp.stack([chip, core, f // side, f % side]).astype(jnp.int32)

    def along(a, n, y):
        pairs = []
        for i in range(experts):
            z_at, y_at = i // side, i % side
            to = z_at * side + (y_at + n) % side if y else ((z_at + n) % side) * side + y_at
            pairs.append((i, to))
        return lax.ppermute(a, "fs", pairs)

    shared_down_local = shared_down_train.astype(bf16)

    def pack(train, half_at):
        first_col = half_at * cols // 2
        return jnp.concatenate(
            [(gain * train).astype(bf16)]
            + [shared_down_local[:, first_col + c : first_col + c + hs] for c in (0, hs)],
            axis=0,
        )

    packs = (pack(shared_gate_train, 0), pack(shared_up_train, 1))
    groups = [[p] for p in packs]
    for n in range(1, side):
        for h, group in enumerate(groups):
            group.append(along(packs[h], n, h == 0))
    groups = [[jnp.stack(g)] for g in groups]
    for n in range(1, side):
        for h, group in enumerate(groups):
            group.append(along(group[0], n, h == 1))

    steps = 8
    anywhere = pl.BlockSpec(memory_space=pl.ANY)
    outgoing, slots = pl.pallas_call(
        functools.partial(route_kernel, half),
        grid=(1,),
        in_specs=[whole((top_count, tok_rows)), anywhere],
        out_specs=[whole((rows, quarter)), whole((top_count, tok_rows))],
        out_shape=[
            jax.ShapeDtypeStruct((rows, quarter), bf16),
            jax.ShapeDtypeStruct((top_count, tok_rows), jnp.int32),
        ],
        scratch_shapes=[
            pltpu.VMEM((tok_rows, quarter), bf16),
            pltpu.VMEM((rows, tok_rows), bf16),
            pltpu.SemaphoreType.DMA(()),
        ],
        compiler_params=vmem_limit(60),
        cost_estimate=cost(2 * rows * tok_rows * quarter, 4 * tok_rows * quarter),
    )(route_expert.T, tokens)
    normed = pl.pallas_call(
        norm_kernel,
        grid=(1,),
        in_specs=[anywhere],
        out_specs=anywhere,
        out_shape=jax.ShapeDtypeStruct((tok_rows, width), bf16),
        scratch_shapes=[
            pltpu.VMEM((tok_rows, width), bf16),
            pltpu.VMEM((tok_rows, width), bf16),
            pltpu.SemaphoreType.DMA((steps,)),
            pltpu.SemaphoreType.DMA((steps,)),
        ],
        compiler_params=vmem_limit(60),
        cost_estimate=cost(16 * tok_rows * width, 4 * tok_rows * width),
    )(tokens)
    arriving = lax.all_to_all(
        outgoing.reshape(experts, half, quarter), "fs", split_axis=0, concat_axis=0, tiled=True
    )

    gu_local = jnp.concatenate(
        [(gain[None] * gate_train).astype(bf16), (gain[None] * up_train).astype(bf16)], axis=2
    )
    mid = rows // 2
    arriving = arriving.reshape(rows, quarter)
    top, bottom = together(arriving[:mid], arriving[mid:])
    gu_local, top, bottom = together(gu_local, top, bottom)
    gu = lax.all_to_all(gu_local, "fs", split_axis=0, concat_axis=0, tiled=True)
    down_local, gu = together(down_train.astype(bf16), gu)
    down_cols = lax.all_to_all(down_local, "fs", split_axis=0, concat_axis=0, tiled=True)
    gu = gu.reshape(width, 2 * hs)
    gu_other = swap(gu)
    down_cols = down_cols.reshape(experts * deep, cols)
    down_other = swap(down_cols)

    left_top = shift_by(top, 1)
    right_bottom = shift_by(bottom, -1)
    right_top = shift_by(top, -1)
    left_bottom = shift_by(bottom, 1)
    far_top = shift_by(left_top, 1)
    far_bottom = shift_by(right_bottom, -1)

    def marker(a, b):
        return pl.pallas_call(
            mark_kernel,
            grid=(1,),
            in_specs=[whole(tile)] * 2,
            out_specs=whole(tile),
            out_shape=jax.ShapeDtypeStruct(tile, bf16),
            cost_estimate=cost(1 << 20, 1 << 14),
        )(a, b)

    tile = (16, 128)
    mark = marker(left_top, right_bottom)
    soon = marker(*packs)
    mark = marker(mark, soon)
    x_spec = pl.BlockSpec((mid // 2, quarter), lambda i, s: (i, 0))
    acc_spec = pl.BlockSpec((2, mid // 2, 4 * hs), lambda i, s: (0, i, 0))
    w_spec = pl.BlockSpec((quarter, 2 * hs), lambda i, s: (lax.rem(s[0] + chips // 2, chips), 0))
    acc, sq = pl.pallas_call(
        first_kernel,
        grid_spec=pltpu.PrefetchScalarGridSpec(
            num_scalar_prefetch=1,
            grid=(2,),
            in_specs=[x_spec] * 6 + [whole((width, 2 * hs))] * 2 + [whole(tile)],
            out_specs=[acc_spec, pl.BlockSpec((2, mid // 2, 128), lambda i, s: (0, i, 0))],
        ),
        out_shape=[
            jax.ShapeDtypeStruct((2, mid, 4 * hs), f32),
            jax.ShapeDtypeStruct((2, mid, 128), f32),
        ],
        compiler_params=vmem_limit(32),
        cost_estimate=cost(2 * rows * 3 * quarter * 4 * hs, 8 * width * hs),
    )(place, top, left_top, right_top, bottom, left_bottom, right_bottom, gu, gu_other, mark)
    hidden = pl.pallas_call(
        functools.partial(hidden_kernel, width),
        grid_spec=pltpu.PrefetchScalarGridSpec(
            num_scalar_prefetch=1,
            grid=(1,),
            in_specs=[whole((mid, quarter))] * 2
            + [whole((2, mid, 4 * hs)), whole((2, mid, 128)), w_spec, w_spec],
            out_specs=whole((2, mid, 2 * hs)),
        ),
        out_shape=jax.ShapeDtypeStruct((2, mid, 2 * hs), bf16),
        compiler_params=vmem_limit(32),
        cost_estimate=cost(2 * rows * quarter * 4 * hs, 8 * quarter * hs),
    )(place, far_top, far_bottom, acc, sq, gu, gu_other).reshape(rows, 2 * hs)

    shared_gate, shared_up, shared_hid, shared_cols, shared_out = pl.pallas_call(
        shared_kernel,
        grid_spec=pltpu.PrefetchScalarGridSpec(
            num_scalar_prefetch=1,
            grid=(1,),
            in_specs=[whole((tok_rows, width))] + [whole(groups[0][0].shape)] * 8,
            out_specs=[
                whole((width, hs)),
                whole((width, hs)),
                whole((tok_rows, hs)),
                whole((experts * deep, cols)),
                whole((experts * deep // 2, cols)),
            ],
            scratch_shapes=[pltpu.VMEM((width, 2 * hs), bf16)],
        ),
        out_shape=[
            jax.ShapeDtypeStruct((width, hs), bf16),
            jax.ShapeDtypeStruct((width, hs), bf16),
            jax.ShapeDtypeStruct((tok_rows, hs), bf16),
            jax.ShapeDtypeStruct((experts * deep, cols), bf16),
            jax.ShapeDtypeStruct((experts * deep // 2, cols), bf16),
        ],
        compiler_params=vmem_limit(36),
        cost_estimate=cost(4 * tok_rows * width * hs, 8 * width * hs),
    )(place, normed, *groups[0], *groups[1])
    shared_other = swap(shared_out)
    units = [shared_hid]
    for n in (1, -1, 2):
        units.append(shift_by(shared_hid, n))
    units = jnp.stack(units)
    units_other = swap(units)

    hid_left = shift_by(hidden, 1)
    hid_right = shift_by(hidden, -1)
    hid_far = shift_by(hidden, 2)
    sums = pl.pallas_call(
        down_kernel,
        grid_spec=pltpu.PrefetchScalarGridSpec(
            num_scalar_prefetch=1,
            grid=(1,),
            in_specs=[whole((rows, 2 * hs))] * 4 + [whole((experts * deep, cols))] * 2,
            out_specs=whole((experts, 2, half, cols)),
            scratch_shapes=[pltpu.VMEM((rows, experts * deep), bf16)],
        ),
        out_shape=jax.ShapeDtypeStruct((experts, 2, half, cols), bf16),
        compiler_params=vmem_limit(40),
        cost_estimate=cost(4 * rows * experts * deep * cols, 8 * experts * deep * cols),
    )(place, hidden, hid_left, hid_right, hid_far, down_cols, down_other)
    returned = lax.all_to_all(sums, "fs", split_axis=0, concat_axis=0, tiled=True)
    got_other = swap(returned[:, 1].reshape(rows, cols))

    spots = jnp.arange(rows, dtype=jnp.int32)[None, :]

    def mixing(which):
        weights = 0
        for k in range(top_count):
            local = slots[k] - which * half
            here = (local >= 0) & (local < half)
            target = jnp.where(here, route_expert[:, k] * half + local, -1)
            at = target[:, None] == spots
            weights = weights + jnp.where(at, route_weight[:, k][:, None].astype(bf16), 0)
        return weights

    mix_own, mix_other = together(mixing(core), mixing(1 - core))

    def mix(weights, got, base, dtype):
        return pl.pallas_call(
            mix_kernel,
            grid=(1,),
            in_specs=[
                whole((tok_rows, rows)),
                whole((experts, 1, half, cols)) if got.ndim == 4 else whole((rows, cols)),
                whole((tok_rows, cols)),
            ],
            out_specs=whole((tok_rows, cols)),
            out_shape=jax.ShapeDtypeStruct((tok_rows, cols), dtype),
            compiler_params=vmem_limit(24),
            cost_estimate=cost(2 * tok_rows * rows * cols, 4 * tok_rows * rows),
        )(weights, got, base)

    base = pl.pallas_call(
        base_kernel,
        grid_spec=pltpu.PrefetchScalarGridSpec(
            num_scalar_prefetch=1,
            grid=(1,),
            in_specs=[whole((chips, tok_rows, hs))] * 2 + [whole((experts * deep, cols))],
            out_specs=whole((tok_rows, cols)),
            scratch_shapes=[pltpu.VMEM((tok_rows, experts * deep), bf16)],
        ),
        out_shape=jax.ShapeDtypeStruct((tok_rows, cols), f32),
        compiler_params=vmem_limit(24),
        cost_estimate=cost(2 * tok_rows * experts * deep * cols, 4 * tok_rows * rows),
    )(place, units, units_other, shared_cols)
    part = mix(mix_own, returned, base, f32)
    mixed = mix(mix_other, got_other, part, bf16)

    chunks = pl.pallas_call(
        chunk_kernel,
        grid_spec=pltpu.PrefetchScalarGridSpec(
            num_scalar_prefetch=1,
            grid=(1,),
            in_specs=[whole((experts * deep, cols))] * 2
            + [whole((experts * deep, cols)), whole((experts * deep // 2, cols))],
            out_specs=[whole((2 * hs, 2 * cols))] * chips,
        ),
        out_shape=[jax.ShapeDtypeStruct((2 * hs, 2 * cols), bf16)] * chips,
        compiler_params=vmem_limit(36),
        cost_estimate=cost(1 << 30, 8 * hs * width),
    )(place, down_cols, down_other, shared_cols, shared_other)
    pieces = [chunks[0]]
    for n in range(1, chips):
        pieces.append(shift_by(chunks[n], n))
    expert_down, shared_down = pl.pallas_call(
        join_kernel,
        grid_spec=pltpu.PrefetchScalarGridSpec(
            num_scalar_prefetch=1,
            grid=(1,),
            in_specs=[whole((2 * hs, 2 * cols))] * 4,
            out_specs=[anywhere] * 2,
            scratch_shapes=[pltpu.SemaphoreType.DMA((4 * chips,))],
        ),
        out_shape=[jax.ShapeDtypeStruct((hs, width), bf16)] * 2,
        compiler_params=vmem_limit(24),
        cost_estimate=cost(1 << 20, 8 * hs * width),
    )(place, *pieces)
    expert_gate = gu[None, :, :hs]
    expert_up = gu[None, :, hs:]
    return (
        expert_gate,
        expert_up,
        expert_down[None],
        shared_gate,
        shared_up,
        shared_down,
        mixed,
    )


def solution(mesh):
    placed = (
        P("fs", None),
        P("fs"),
        P(None, "fs", "tp"),
        P(None, "fs", "tp"),
        P(None, "fs", "tp"),
        P("fs", "tp"),
        P("fs", "tp"),
        P("fs", "tp"),
        P("fs", None),
        P("fs", None),
    )


    return jax.shard_map(
        on_device,
        mesh=mesh,
        in_specs=placed,
        out_specs=(
            P("fs", None, "tp"),
            P("fs", None, "tp"),
            P("fs", "tp", None),
            P(None, "tp"),
            P(None, "tp"),
            P("tp", None),
            P("fs", "tp"),
        ),
        check_vma=False,
    )
```

```python
import functools

import jax
import jax.numpy as jnp
from jax import lax
from jax.experimental import pallas as pl
from jax.experimental.pallas import tpu as pltpu
from jax.sharding import PartitionSpec as P

norm_eps = 1e-06
bf16 = jnp.bfloat16
f32 = jnp.float32


def dot(a, b):
    return jnp.dot(a, b, preferred_element_type=f32)


def together(*values):
    return lax.optimization_barrier(values)


def cost(flops, moved):
    return pl.CostEstimate(flops=flops, bytes_accessed=moved, transcendentals=0)


def vmem_limit(mib):
    return pltpu.CompilerParams(vmem_limit_bytes=mib << 20)


def route_kernel(half, route_ref, tok_ref, top_ref, bottom_ref, slot_ref, kept, placing, sem):
    t = lax.axis_index("tp")
    chip, core = t // 2, lax.rem(t, 2)
    tok_rows, quarter = kept.shape
    spots = placing.shape[0]
    experts, few = spots // half, half // 2
    at = pl.ds(pl.multiple_of(chip * quarter, quarter), quarter)
    read = pltpu.make_async_copy(tok_ref.at[:, at], kept, sem)
    read.start()

    ids = lax.broadcasted_iota(jnp.int32, (experts, tok_rows), 0)
    hot = [route_ref[k : k + 1, :] == ids for k in range(route_ref.shape[0])]
    named = sum(jnp.where(x, 1.0, 0.0) for x in hot).astype(bf16)
    ahead = lax.broadcasted_iota(jnp.int32, (tok_rows, tok_rows), 0) < (
        lax.broadcasted_iota(jnp.int32, (tok_rows, tok_rows), 1)
    )
    earlier = dot(named, jnp.where(ahead, 1.0, 0.0).astype(bf16))
    spot = lax.broadcasted_iota(jnp.int32, (spots, tok_rows), 0)
    total = jnp.zeros((spots, tok_rows), f32)
    for k, x in enumerate(hot):
        slot = jnp.sum(jnp.where(x, earlier, 0.0), axis=0, keepdims=True).astype(jnp.int32)
        slot_ref[k : k + 1, :] = slot
        local = slot - core * half
        here = (local >= 0) & (local < half)
        line = route_ref[k : k + 1, :] * few + local
        line = jnp.where(local < few, line, line + (spots // 2 - few))
        target = jnp.where(here, line, -1)
        total = total + jnp.where(spot == target, 1.0, 0.0)
    placing[...] = total.astype(bf16)
    read.wait()
    for c in range(0, spots, 192):
        part, at = divmod(c, spots // 2)
        block = dot(placing[c : c + 192, :], kept[...]).astype(bf16)
        (top_ref, bottom_ref)[part][at : at + 192, :] = block


def norm_kernel(tok_ref, normed_ref, taken, given, in_sem, out_sem):
    steps = in_sem.shape[0]
    rows = taken.shape[0] // steps

    def span(step):
        return pl.ds(step * rows, rows)

    reads = [
        pltpu.make_async_copy(tok_ref.at[span(i)], taken.at[span(i)], in_sem.at[i])
        for i in range(steps)
    ]
    writes = [
        pltpu.make_async_copy(given.at[span(i)], normed_ref.at[span(i)], out_sem.at[i])
        for i in range(steps)
    ]
    for read in reads:
        read.start()
    for i in range(steps):
        reads[i].wait()
        for r in range(i * rows, (i + 1) * rows, 16):
            values = taken[r : r + 16, :].astype(f32)
            scale = lax.rsqrt(jnp.mean(values * values, axis=1, keepdims=True) + norm_eps)
            given[r : r + 16, :] = (values * scale).astype(bf16)
        if i:
            writes[i - 1].start()
    writes[steps - 1].start()
    for write in writes:
        write.wait()


def squares(x_ref):
    total = None
    for c in range(0, x_ref.shape[1], 128):
        values = x_ref[:, c : c + 128].astype(f32)
        total = values * values if total is None else total + values * values
    return total


def square_kernel(*refs):
    x_refs, sq_ref = refs[:6], refs[6]
    for part in range(2):
        blocks = x_refs[3 * part : 3 * part + 3]
        sq_ref[part] = squares(blocks[0]) + squares(blocks[1]) + squares(blocks[2])


def first_kernel(place_ref, *refs):
    x_refs, (w_own_ref, w_other_ref, acc_ref) = refs[:6], refs[6:]
    chip = place_ref[0]
    quarter, wide = x_refs[0].shape[1], w_own_ref.shape[1]
    chips = w_own_ref.shape[0] // quarter
    for part in range(2):
        blocks = x_refs[3 * part : 3 * part + 3]
        for half, w_ref in ((0, w_own_ref), (1, w_other_ref)):
            total = None
            for x_ref, shift in zip(blocks, (0, chips - 1, 1)):
                at = pl.multiple_of(lax.rem(chip + shift, chips) * quarter, quarter)
                term = dot(x_ref[...], w_ref[pl.ds(at, quarter), :])
                total = term if total is None else total + term
            acc_ref[part, :, half * wide : (half + 1) * wide] = total


def hidden_kernel(width, place_ref, far0_ref, far1_ref, acc_ref, sq_ref, w0_ref, w1_ref, out_ref):
    core = place_ref[1]
    wide = w0_ref.shape[1]
    hs = wide // 2
    for part, far_ref in enumerate((far0_ref, far1_ref)):
        sums = jnp.sum(sq_ref[part] + squares(far_ref), axis=1, keepdims=True)
        scale = lax.rsqrt(sums * (1.0 / width) + norm_eps)
        for half, w_ref, slot in ((0, w0_ref, core), (1, w1_ref, 1 - core)):
            total = acc_ref[part, :, half * wide : (half + 1) * wide]
            total = (total + dot(far_ref[...], w_ref[...])) * scale
            gate, up = total[:, :hs], total[:, hs:]
            value = (gate / (1.0 + jnp.exp(-gate)) * up).astype(bf16)
            out_ref[part, :, pl.ds(pl.multiple_of(slot * hs, hs), hs)] = value


def down_kernel(place_ref, h0_ref, h1_ref, h2_ref, h3_ref, w_own_ref, w_other_ref, out_ref, *scratch):
    line, held, sems = scratch
    chip = place_ref[0]
    depth = h0_ref.shape[1]
    chips = w_own_ref.shape[0] // depth
    parts = ((h0_ref, 0), (h1_ref, chips - 1), (h2_ref, 1), (h3_ref, chips // 2))
    for h_ref, shift in parts:
        at = pl.multiple_of(lax.rem(chip + shift, chips) * depth, depth)
        line[:, pl.ds(at, depth)] = h_ref[...]
    copies = []
    for part, w_ref in enumerate((w_own_ref, w_other_ref)):
        total = dot(line[...], w_ref[...]).reshape(held.shape[1:])
        held[part] = total.astype(bf16)
        for half in range(2):
            copy = pltpu.make_async_copy(
                held.at[part, half], out_ref.at[:, part, half], sems.at[part, half]
            )
            copy.start()
            copies.append(copy)
    for copy in copies:
        copy.wait()


def shared_kernel(place_ref, x_ref, *refs):
    groups, outs, (line,) = (refs[:4], refs[4:8]), refs[8:13], refs[13:]
    gate_ref, up_ref, hid_ref, sd_ref, sd_out_ref = outs
    core, z, y = place_ref[1], place_ref[2], place_ref[3]
    hs = gate_ref.shape[1]
    side, size = groups[0][0].shape[0], line.shape[0] // 16
    deep = sd_ref.shape[0] // 16
    for h, out_ref in ((0, gate_ref), (1, up_ref)):
        for m, ref in enumerate(groups[h]):
            for n in range(side):
                dz, dy = (m, n) if h == 0 else (n, m)
                source = lax.rem(z + side - dz, side) * side + lax.rem(y + side - dy, side)
                block = ref[n, :size, :]
                at = pl.ds(pl.multiple_of(source * size, size), size)
                out_ref[at, :] = block
                line[at, h * hs : (h + 1) * hs] = block
                at = pl.ds(pl.multiple_of(source * deep, deep), deep)
                for c in range(2):
                    col = (2 * h + c) * hs
                    sd_ref[at, col : col + hs] = ref[n, size + c * deep : size + (c + 1) * deep, :]
    for c in range(4):
        at = pl.ds(pl.multiple_of((2 * c + 1 - core) * hs, hs), hs)
        sd_out_ref[c * hs : (c + 1) * hs, :] = sd_ref[at, :]
    total = dot(x_ref[...], line[...])
    gate, up = total[:, :hs], total[:, hs:]
    hid_ref[...] = (gate / (1.0 + jnp.exp(-gate)) * up).astype(bf16)


def base_kernel(place_ref, own_ref, other_ref, sd_ref, out_ref, line):
    chip, core = place_ref[0], place_ref[1]
    hs = own_ref.shape[2]
    for ref, lane in ((own_ref, core), (other_ref, 1 - core)):
        for n, shift in enumerate((0, 3, 1, 2)):
            at = pl.multiple_of((lax.rem(chip + shift, 4) * 2 + lane) * hs, hs)
            line[:, pl.ds(at, hs)] = ref[n]
    out_ref[...] = dot(line[...], sd_ref[...])


def mix_kernel(weight_ref, got_ref, base_ref, out_ref):
    got = got_ref[...].reshape(weight_ref.shape[1], out_ref.shape[1])
    out_ref[...] = (base_ref[...] + dot(weight_ref[...], got)).astype(out_ref.dtype)


def chunk_kernel(place_ref, own_ref, other_ref, sd_ref, sd_other_ref, *out_refs):
    chip, core = place_ref[0], place_ref[1]
    hs, cols = out_refs[0].shape[0] // 2, own_ref.shape[1]
    for n, out_ref in enumerate(out_refs):
        target = lax.rem(chip + n, 4)
        at = pl.ds(pl.multiple_of((target * 2 + core) * hs, hs), hs)
        far = pl.ds(pl.multiple_of(target * hs, hs), hs)
        out_ref[:hs, :cols] = own_ref[at, :]
        out_ref[:hs, cols:] = other_ref[at, :]
        out_ref[hs:, :cols] = sd_ref[at, :]
        out_ref[hs:, cols:] = sd_other_ref[far, :]


def join_kernel(place_ref, p0_ref, p1_ref, p2_ref, p3_ref, routed_ref, shared_ref, sems):
    chip, core = place_ref[0], place_ref[1]
    hs = routed_ref.shape[0]
    cols = p0_ref.shape[1] // 2
    copies = []
    for shift, ref in enumerate((p0_ref, p1_ref, p2_ref, p3_ref)):
        source = lax.rem(chip + 4 - shift, 4)
        for half, lane in ((0, core), (1, 1 - core)):
            at = pl.ds(pl.multiple_of((source * 2 + lane) * cols, cols), cols)
            part = pl.ds(half * cols, cols)
            for top, out_ref in ((0, routed_ref), (hs, shared_ref)):
                copies.append(
                    pltpu.make_async_copy(
                        ref.at[pl.ds(top, hs), part], out_ref.at[:, at], sems.at[len(copies)]
                    )
                )
    for copy in copies:
        copy.start()
    for copy in copies:
        copy.wait()


def whole(shape):
    return pl.BlockSpec(shape, lambda *_: (0,) * len(shape))


def on_device(
    tokens,
    norm_gain,
    gate_train,
    up_train,
    down_train,
    shared_gate_train,
    shared_up_train,
    shared_down_train,
    route_expert,
    route_weight,
):
    experts = lax.axis_size("fs")
    tp = lax.axis_size("tp")
    t = lax.axis_index("tp")
    chips = tp // 2
    chip, core = t // 2, t % 2
    tok_rows, width = tokens.shape
    top_count = route_expert.shape[1]
    cap = 3 * tok_rows * top_count // (2 * experts)
    half = cap // 2
    rows = experts * half
    quarter = width // chips
    cols = width // tp
    hs = gate_train.shape[2]
    deep = down_train.shape[1]

    def shift_by(a, n):
        return lax.ppermute(a, "tp", [(i, (i + 2 * n) % tp) for i in range(tp)])

    def swap(a):
        return lax.ppermute(a, "tp", [(i, i ^ 1) for i in range(tp)])

    gain = norm_gain[:, None]
    side = 4
    f = lax.axis_index("fs")
    place = jnp.stack([chip, core, f // side, f % side]).astype(jnp.int32)

    def along(a, n, y):
        pairs = []
        for i in range(experts):
            z_at, y_at = i // side, i % side
            to = z_at * side + (y_at + n) % side if y else ((z_at + n) % side) * side + y_at
            pairs.append((i, to))
        return lax.ppermute(a, "fs", pairs)

    shared_down_local = shared_down_train.astype(bf16)

    def pack(train, half_at):
        first_col = half_at * cols // 2
        return jnp.concatenate(
            [(gain * train).astype(bf16)]
            + [shared_down_local[:, first_col + c : first_col + c + hs] for c in (0, hs)],
            axis=0,
        )

    packs = (pack(shared_gate_train, 0), pack(shared_up_train, 1))
    groups = [[p] for p in packs]
    for n in range(1, side):
        for h, group in enumerate(groups):
            group.append(along(packs[h], n, h == 0))
    groups = [[jnp.stack(g)] for g in groups]
    for n in range(1, side):
        for h, group in enumerate(groups):
            group.append(along(group[0], n, h == 1))

    steps = 8
    anywhere = pl.BlockSpec(memory_space=pl.ANY)
    mid = rows // 2
    out_top, out_bottom, slots = pl.pallas_call(
        functools.partial(route_kernel, half),
        grid=(1,),
        in_specs=[whole((top_count, tok_rows)), anywhere],
        out_specs=[whole((mid, quarter)), whole((mid, quarter)), whole((top_count, tok_rows))],
        out_shape=[
            jax.ShapeDtypeStruct((mid, quarter), bf16),
            jax.ShapeDtypeStruct((mid, quarter), bf16),
            jax.ShapeDtypeStruct((top_count, tok_rows), jnp.int32),
        ],
        scratch_shapes=[
            pltpu.VMEM((tok_rows, quarter), bf16),
            pltpu.VMEM((rows, tok_rows), bf16),
            pltpu.SemaphoreType.DMA(()),
        ],
        compiler_params=vmem_limit(60),
        cost_estimate=cost(2 * rows * tok_rows * quarter, 4 * tok_rows * quarter),
    )(route_expert.T, tokens)
    normed = pl.pallas_call(
        norm_kernel,
        grid=(1,),
        in_specs=[anywhere],
        out_specs=anywhere,
        out_shape=jax.ShapeDtypeStruct((tok_rows, width), bf16),
        scratch_shapes=[
            pltpu.VMEM((tok_rows, width), bf16),
            pltpu.VMEM((tok_rows, width), bf16),
            pltpu.SemaphoreType.DMA((steps,)),
            pltpu.SemaphoreType.DMA((steps,)),
        ],
        compiler_params=vmem_limit(60),
        cost_estimate=cost(16 * tok_rows * width, 4 * tok_rows * width),
    )(tokens)

    def sent(a):
        a = a.reshape(experts, half // 2, quarter)
        return lax.all_to_all(a, "fs", split_axis=0, concat_axis=0, tiled=True).reshape(mid, quarter)

    top = sent(out_top)
    out_bottom, top = together(out_bottom, top)
    bottom = sent(out_bottom)

    gu_local = jnp.concatenate(
        [(gain[None] * gate_train).astype(bf16), (gain[None] * up_train).astype(bf16)], axis=2
    )
    gu_local, bottom = together(gu_local, bottom)
    gu = lax.all_to_all(gu_local, "fs", split_axis=0, concat_axis=0, tiled=True)
    down_local, gu = together(down_train.astype(bf16), gu)
    down_cols = lax.all_to_all(down_local, "fs", split_axis=0, concat_axis=0, tiled=True)
    gu = gu.reshape(width, 2 * hs)
    gu_other = swap(gu)
    down_cols = down_cols.reshape(experts * deep, cols)
    down_other = swap(down_cols)

    left_top = shift_by(top, 1)
    right_bottom = shift_by(bottom, -1)
    right_top = shift_by(top, -1)
    left_bottom = shift_by(bottom, 1)
    far_top = shift_by(left_top, 1)
    far_bottom = shift_by(right_bottom, -1)

    x_spec = pl.BlockSpec((mid // 2, quarter), lambda i, s: (i, 0))
    acc_spec = pl.BlockSpec((2, mid // 2, 4 * hs), lambda i, s: (0, i, 0))
    w_spec = pl.BlockSpec((quarter, 2 * hs), lambda i, s: (lax.rem(s[0] + chips // 2, chips), 0))
    blocks = (top, left_top, right_top, bottom, left_bottom, right_bottom)
    sq = pl.pallas_call(
        square_kernel,
        grid=(2,),
        in_specs=[pl.BlockSpec((mid // 2, quarter), lambda i: (i, 0))] * 6,
        out_specs=pl.BlockSpec((2, mid // 2, 128), lambda i: (0, i, 0)),
        out_shape=jax.ShapeDtypeStruct((2, mid, 128), f32),
        compiler_params=vmem_limit(32),
        cost_estimate=cost(6 * rows * width, 2 * rows * width),
    )(*blocks)
    acc = pl.pallas_call(
        first_kernel,
        grid_spec=pltpu.PrefetchScalarGridSpec(
            num_scalar_prefetch=1,
            grid=(2,),
            in_specs=[x_spec] * 6 + [whole((width, 2 * hs))] * 2,
            out_specs=acc_spec,
        ),
        out_shape=jax.ShapeDtypeStruct((2, mid, 4 * hs), f32),
        compiler_params=vmem_limit(32),
        cost_estimate=cost(2 * rows * 3 * quarter * 4 * hs, 8 * width * hs),
    )(place, *blocks, gu, gu_other)
    hidden = pl.pallas_call(
        functools.partial(hidden_kernel, width),
        grid_spec=pltpu.PrefetchScalarGridSpec(
            num_scalar_prefetch=1,
            grid=(1,),
            in_specs=[whole((mid, quarter))] * 2
            + [whole((2, mid, 4 * hs)), whole((2, mid, 128)), w_spec, w_spec],
            out_specs=whole((2, mid, 2 * hs)),
        ),
        out_shape=jax.ShapeDtypeStruct((2, mid, 2 * hs), bf16),
        compiler_params=vmem_limit(32),
        cost_estimate=cost(2 * rows * quarter * 4 * hs, 8 * quarter * hs),
    )(place, far_top, far_bottom, acc, sq, gu, gu_other).reshape(rows, 2 * hs)

    shared_gate, shared_up, shared_hid, shared_cols, shared_out = pl.pallas_call(
        shared_kernel,
        grid_spec=pltpu.PrefetchScalarGridSpec(
            num_scalar_prefetch=1,
            grid=(1,),
            in_specs=[whole((tok_rows, width))] + [whole(groups[0][0].shape)] * 8,
            out_specs=[
                whole((width, hs)),
                whole((width, hs)),
                whole((tok_rows, hs)),
                whole((experts * deep, cols)),
                whole((experts * deep // 2, cols)),
            ],
            scratch_shapes=[pltpu.VMEM((width, 2 * hs), bf16)],
        ),
        out_shape=[
            jax.ShapeDtypeStruct((width, hs), bf16),
            jax.ShapeDtypeStruct((width, hs), bf16),
            jax.ShapeDtypeStruct((tok_rows, hs), bf16),
            jax.ShapeDtypeStruct((experts * deep, cols), bf16),
            jax.ShapeDtypeStruct((experts * deep // 2, cols), bf16),
        ],
        compiler_params=vmem_limit(36),
        cost_estimate=cost(4 * tok_rows * width * hs, 8 * width * hs),
    )(place, normed, *groups[0], *groups[1])
    shared_other = swap(shared_out)
    units = [shared_hid]
    for n in (1, -1, 2):
        units.append(shift_by(shared_hid, n))
    units = jnp.stack(units)
    units_other = swap(units)

    hid_left = shift_by(hidden, 1)
    hid_right = shift_by(hidden, -1)
    hid_far = shift_by(hidden, 2)
    sums = pl.pallas_call(
        down_kernel,
        grid_spec=pltpu.PrefetchScalarGridSpec(
            num_scalar_prefetch=1,
            grid=(1,),
            in_specs=[whole((rows, 2 * hs))] * 4 + [whole((experts * deep, cols))] * 2,
            out_specs=pl.BlockSpec(memory_space=pltpu.HBM),
            scratch_shapes=[
                pltpu.VMEM((rows, experts * deep), bf16),
                pltpu.VMEM((2, 2, experts, half // 2, cols), bf16),
                pltpu.SemaphoreType.DMA((2, 2)),
            ],
        ),
        out_shape=jax.ShapeDtypeStruct((experts, 2, 2, half // 2, cols), bf16),
        compiler_params=vmem_limit(40),
        cost_estimate=cost(4 * rows * experts * deep * cols, 8 * experts * deep * cols),
    )(place, hidden, hid_left, hid_right, hid_far, down_cols, down_other)
    sums = sums.reshape(experts, 2, half, cols)
    returned = lax.all_to_all(sums, "fs", split_axis=0, concat_axis=0, tiled=True)
    got_other = swap(returned[:, 1].reshape(rows, cols))

    spots = jnp.arange(rows, dtype=jnp.int32)[None, :]

    def mixing(which):
        weights = 0
        for k in range(top_count):
            local = slots[k] - which * half
            here = (local >= 0) & (local < half)
            target = jnp.where(here, route_expert[:, k] * half + local, -1)
            at = target[:, None] == spots
            weights = weights + jnp.where(at, route_weight[:, k][:, None].astype(bf16), 0)
        return weights

    mix_own, mix_other = together(mixing(core), mixing(1 - core))

    def mix(weights, got, base, dtype):
        return pl.pallas_call(
            mix_kernel,
            grid=(1,),
            in_specs=[
                whole((tok_rows, rows)),
                whole((experts, 1, half, cols)) if got.ndim == 4 else whole((rows, cols)),
                whole((tok_rows, cols)),
            ],
            out_specs=whole((tok_rows, cols)),
            out_shape=jax.ShapeDtypeStruct((tok_rows, cols), dtype),
            compiler_params=vmem_limit(24),
            cost_estimate=cost(2 * tok_rows * rows * cols, 4 * tok_rows * rows),
        )(weights, got, base)

    base = pl.pallas_call(
        base_kernel,
        grid_spec=pltpu.PrefetchScalarGridSpec(
            num_scalar_prefetch=1,
            grid=(1,),
            in_specs=[whole((chips, tok_rows, hs))] * 2 + [whole((experts * deep, cols))],
            out_specs=whole((tok_rows, cols)),
            scratch_shapes=[pltpu.VMEM((tok_rows, experts * deep), bf16)],
        ),
        out_shape=jax.ShapeDtypeStruct((tok_rows, cols), f32),
        compiler_params=vmem_limit(24),
        cost_estimate=cost(2 * tok_rows * experts * deep * cols, 4 * tok_rows * rows),
    )(place, units, units_other, shared_cols)
    part = mix(mix_own, returned, base, f32)
    mixed = mix(mix_other, got_other, part, bf16)

    chunks = pl.pallas_call(
        chunk_kernel,
        grid_spec=pltpu.PrefetchScalarGridSpec(
            num_scalar_prefetch=1,
            grid=(1,),
            in_specs=[whole((experts * deep, cols))] * 2
            + [whole((experts * deep, cols)), whole((experts * deep // 2, cols))],
            out_specs=[whole((2 * hs, 2 * cols))] * chips,
        ),
        out_shape=[jax.ShapeDtypeStruct((2 * hs, 2 * cols), bf16)] * chips,
        compiler_params=vmem_limit(36),
        cost_estimate=cost(1 << 30, 8 * hs * width),
    )(place, down_cols, down_other, shared_cols, shared_other)
    pieces = [chunks[0]]
    for n in range(1, chips):
        pieces.append(shift_by(chunks[n], n))
    expert_down, shared_down = pl.pallas_call(
        join_kernel,
        grid_spec=pltpu.PrefetchScalarGridSpec(
            num_scalar_prefetch=1,
            grid=(1,),
            in_specs=[whole((2 * hs, 2 * cols))] * 4,
            out_specs=[anywhere] * 2,
            scratch_shapes=[pltpu.SemaphoreType.DMA((4 * chips,))],
        ),
        out_shape=[jax.ShapeDtypeStruct((hs, width), bf16)] * 2,
        compiler_params=vmem_limit(24),
        cost_estimate=cost(1 << 20, 8 * hs * width),
    )(place, *pieces)
    expert_gate = gu[None, :, :hs]
    expert_up = gu[None, :, hs:]
    return (
        expert_gate,
        expert_up,
        expert_down[None],
        shared_gate,
        shared_up,
        shared_down,
        mixed,
    )


def solution(mesh):
    placed = (
        P("fs", None),
        P("fs"),
        P(None, "fs", "tp"),
        P(None, "fs", "tp"),
        P(None, "fs", "tp"),
        P("fs", "tp"),
        P("fs", "tp"),
        P("fs", "tp"),
        P("fs", None),
        P("fs", None),
    )


    return jax.shard_map(
        on_device,
        mesh=mesh,
        in_specs=placed,
        out_specs=(
            P("fs", None, "tp"),
            P("fs", None, "tp"),
            P("fs", "tp", None),
            P(None, "tp"),
            P(None, "tp"),
            P("tp", None),
            P("fs", "tp"),
        ),
        check_vma=False,
    )
```

```python
import functools

import jax
import jax.numpy as jnp
from jax import lax
from jax.experimental import pallas as pl
from jax.experimental.pallas import tpu as pltpu
from jax.sharding import PartitionSpec as P

norm_eps = 1e-06
bf16 = jnp.bfloat16
f32 = jnp.float32


def dot(a, b):
    return jnp.dot(a, b, preferred_element_type=f32)


def together(*values):
    return lax.optimization_barrier(values)


def cost(flops, moved):
    return pl.CostEstimate(flops=flops, bytes_accessed=moved, transcendentals=0)


def vmem_limit(mib):
    return pltpu.CompilerParams(vmem_limit_bytes=mib << 20)


def route_kernel(half, route_ref, tok_ref, out_ref, slot_ref, kept, placing, sem):
    t = lax.axis_index("tp")
    chip, core = t // 2, lax.rem(t, 2)
    tok_rows, quarter = kept.shape
    spots = placing.shape[0]
    experts = spots // half
    at = pl.ds(pl.multiple_of(chip * quarter, quarter), quarter)
    read = pltpu.make_async_copy(tok_ref.at[:, at], kept, sem)
    read.start()

    ids = lax.broadcasted_iota(jnp.int32, (experts, tok_rows), 0)
    hot = [route_ref[k : k + 1, :] == ids for k in range(route_ref.shape[0])]
    named = sum(jnp.where(x, 1.0, 0.0) for x in hot).astype(bf16)
    ahead = lax.broadcasted_iota(jnp.int32, (tok_rows, tok_rows), 0) < (
        lax.broadcasted_iota(jnp.int32, (tok_rows, tok_rows), 1)
    )
    earlier = dot(named, jnp.where(ahead, 1.0, 0.0).astype(bf16))
    spot = lax.broadcasted_iota(jnp.int32, (spots, tok_rows), 0)
    total = jnp.zeros((spots, tok_rows), f32)
    for k, x in enumerate(hot):
        slot = jnp.sum(jnp.where(x, earlier, 0.0), axis=0, keepdims=True).astype(jnp.int32)
        slot_ref[k : k + 1, :] = slot
        local = slot - core * half
        here = (local >= 0) & (local < half)
        target = jnp.where(here, route_ref[k : k + 1, :] * half + local, -1)
        total = total + jnp.where(spot == target, 1.0, 0.0)
    placing[...] = total.astype(bf16)
    read.wait()
    for c in range(0, spots, 256):
        out_ref[c : c + 256, :] = dot(placing[c : c + 256, :], kept[...]).astype(bf16)


def norm_kernel(tok_ref, normed_ref, taken, given, in_sem, out_sem):
    steps = in_sem.shape[0]
    rows = taken.shape[0] // steps

    def span(step):
        return pl.ds(step * rows, rows)

    reads = [
        pltpu.make_async_copy(tok_ref.at[span(i)], taken.at[span(i)], in_sem.at[i])
        for i in range(steps)
    ]
    writes = [
        pltpu.make_async_copy(given.at[span(i)], normed_ref.at[span(i)], out_sem.at[i])
        for i in range(steps)
    ]
    for read in reads:
        read.start()
    for i in range(steps):
        reads[i].wait()
        for r in range(i * rows, (i + 1) * rows, 16):
            values = taken[r : r + 16, :].astype(f32)
            scale = lax.rsqrt(jnp.mean(values * values, axis=1, keepdims=True) + norm_eps)
            given[r : r + 16, :] = (values * scale).astype(bf16)
        if i:
            writes[i - 1].start()
    writes[steps - 1].start()
    for write in writes:
        write.wait()


def squares(x_ref):
    total = None
    for c in range(0, x_ref.shape[1], 128):
        values = x_ref[:, c : c + 128].astype(f32)
        total = values * values if total is None else total + values * values
    return total


def mark_kernel(a_ref, b_ref, out_ref):
    out_ref[...] = a_ref[...] + b_ref[...]


def first_kernel(place_ref, *refs):
    x_refs, (w_own_ref, w_other_ref, _, acc_ref, sq_ref) = refs[:6], refs[6:]
    chip = place_ref[0]
    quarter, wide = x_refs[0].shape[1], w_own_ref.shape[1]
    chips = w_own_ref.shape[0] // quarter
    for part in range(2):
        blocks = x_refs[3 * part : 3 * part + 3]
        for half, w_ref in ((0, w_own_ref), (1, w_other_ref)):
            total = None
            for x_ref, shift in zip(blocks, (0, chips - 1, 1)):
                at = pl.multiple_of(lax.rem(chip + shift, chips) * quarter, quarter)
                term = dot(x_ref[...], w_ref[pl.ds(at, quarter), :])
                total = term if total is None else total + term
            acc_ref[part, :, half * wide : (half + 1) * wide] = total
        sq_ref[part] = squares(blocks[0]) + squares(blocks[1]) + squares(blocks[2])


def hidden_kernel(width, place_ref, far0_ref, far1_ref, acc_ref, sq_ref, w0_ref, w1_ref, out_ref):
    core = place_ref[1]
    wide = w0_ref.shape[1]
    hs = wide // 2
    for part, far_ref in enumerate((far0_ref, far1_ref)):
        sums = jnp.sum(sq_ref[part] + squares(far_ref), axis=1, keepdims=True)
        scale = lax.rsqrt(sums * (1.0 / width) + norm_eps)
        for half, w_ref, slot in ((0, w0_ref, core), (1, w1_ref, 1 - core)):
            total = acc_ref[part, :, half * wide : (half + 1) * wide]
            total = (total + dot(far_ref[...], w_ref[...])) * scale
            gate, up = total[:, :hs], total[:, hs:]
            value = (gate / (1.0 + jnp.exp(-gate)) * up).astype(bf16)
            out_ref[part, :, pl.ds(pl.multiple_of(slot * hs, hs), hs)] = value


def down_kernel(place_ref, h0_ref, h1_ref, h2_ref, h3_ref, w_own_ref, w_other_ref, out_ref, *scratch):
    line, held, sems = scratch
    chip = place_ref[0]
    depth = h0_ref.shape[1]
    chips = w_own_ref.shape[0] // depth
    parts = ((h0_ref, 0), (h1_ref, chips - 1), (h2_ref, 1), (h3_ref, chips // 2))
    for h_ref, shift in parts:
        at = pl.multiple_of(lax.rem(chip + shift, chips) * depth, depth)
        line[:, pl.ds(at, depth)] = h_ref[...]
    copies = []
    for part, w_ref in enumerate((w_own_ref, w_other_ref)):
        total = dot(line[...], w_ref[...]).astype(bf16)
        held[part] = total.reshape(held.shape[1:])
        copies.append(
            pltpu.make_async_copy(held.at[part], out_ref.at[:, part], sems.at[part])
        )
        copies[part].start()
    for copy in copies:
        copy.wait()


def shared_kernel(place_ref, x_ref, *refs):
    groups, outs, (line, sems) = (refs[:4], refs[4:8]), refs[8:13], refs[13:]
    gate_ref, up_ref, hid_ref, sd_ref, sd_out_ref = outs
    core, z, y = place_ref[1], place_ref[2], place_ref[3]
    hs = gate_ref.shape[1]
    side, size = groups[0][0].shape[0], line.shape[0] // 16
    deep = sd_ref.shape[0] // 16
    for h in range(2):
        for m, ref in enumerate(groups[h]):
            for n in range(side):
                dz, dy = (m, n) if h == 0 else (n, m)
                source = lax.rem(z + side - dz, side) * side + lax.rem(y + side - dy, side)
                block = ref[n, :size, :]
                at = pl.ds(pl.multiple_of(source * size, size), size)
                line[at, h * hs : (h + 1) * hs] = block
                at = pl.ds(pl.multiple_of(source * deep, deep), deep)
                for c in range(2):
                    col = (2 * h + c) * hs
                    sd_ref[at, col : col + hs] = ref[n, size + c * deep : size + (c + 1) * deep, :]
    for c in range(4):
        at = pl.ds(pl.multiple_of((2 * c + 1 - core) * hs, hs), hs)
        sd_out_ref[c * hs : (c + 1) * hs, :] = sd_ref[at, :]
    copies = [
        pltpu.make_async_copy(line.at[:, pl.ds(h * hs, hs)], out_ref, sems.at[h])
        for h, out_ref in enumerate((gate_ref, up_ref))
    ]
    for copy in copies:
        copy.start()
    total = dot(x_ref[...], line[...])
    gate, up = total[:, :hs], total[:, hs:]
    hid_ref[...] = (gate / (1.0 + jnp.exp(-gate)) * up).astype(bf16)
    for copy in copies:
        copy.wait()


def base_kernel(place_ref, own_ref, other_ref, sd_ref, out_ref, line):
    chip, core = place_ref[0], place_ref[1]
    hs = own_ref.shape[2]
    for ref, lane in ((own_ref, core), (other_ref, 1 - core)):
        for n, shift in enumerate((0, 3, 1, 2)):
            at = pl.multiple_of((lax.rem(chip + shift, 4) * 2 + lane) * hs, hs)
            line[:, pl.ds(at, hs)] = ref[n]
    out_ref[...] = dot(line[...], sd_ref[...])


def mix_kernel(weight_ref, got_ref, base_ref, out_ref):
    got = got_ref[...].reshape(weight_ref.shape[1], out_ref.shape[1])
    out_ref[...] = (base_ref[...] + dot(weight_ref[...], got)).astype(out_ref.dtype)


def chunk_kernel(place_ref, own_ref, other_ref, sd_ref, sd_other_ref, *out_refs):
    chip, core = place_ref[0], place_ref[1]
    hs, cols = out_refs[0].shape[0] // 2, own_ref.shape[1]
    for n, out_ref in enumerate(out_refs):
        target = lax.rem(chip + n, 4)
        at = pl.ds(pl.multiple_of((target * 2 + core) * hs, hs), hs)
        far = pl.ds(pl.multiple_of(target * hs, hs), hs)
        out_ref[:hs, :cols] = own_ref[at, :]
        out_ref[:hs, cols:] = other_ref[at, :]
        out_ref[hs:, :cols] = sd_ref[at, :]
        out_ref[hs:, cols:] = sd_other_ref[far, :]


def join_kernel(place_ref, p0_ref, p1_ref, p2_ref, p3_ref, routed_ref, shared_ref, sems):
    chip, core = place_ref[0], place_ref[1]
    hs = routed_ref.shape[0]
    cols = p0_ref.shape[1] // 2
    copies = []
    for shift, ref in enumerate((p0_ref, p1_ref, p2_ref, p3_ref)):
        source = lax.rem(chip + 4 - shift, 4)
        for half, lane in ((0, core), (1, 1 - core)):
            at = pl.ds(pl.multiple_of((source * 2 + lane) * cols, cols), cols)
            part = pl.ds(half * cols, cols)
            for top, out_ref in ((0, routed_ref), (hs, shared_ref)):
                copies.append(
                    pltpu.make_async_copy(
                        ref.at[pl.ds(top, hs), part], out_ref.at[:, at], sems.at[len(copies)]
                    )
                )
    for copy in copies:
        copy.start()
    for copy in copies:
        copy.wait()


def whole(shape):
    return pl.BlockSpec(shape, lambda *_: (0,) * len(shape))


def on_device(
    tokens,
    norm_gain,
    gate_train,
    up_train,
    down_train,
    shared_gate_train,
    shared_up_train,
    shared_down_train,
    route_expert,
    route_weight,
):
    experts = lax.axis_size("fs")
    tp = lax.axis_size("tp")
    t = lax.axis_index("tp")
    chips = tp // 2
    chip, core = t // 2, t % 2
    tok_rows, width = tokens.shape
    top_count = route_expert.shape[1]
    cap = 3 * tok_rows * top_count // (2 * experts)
    half = cap // 2
    rows = experts * half
    quarter = width // chips
    cols = width // tp
    hs = gate_train.shape[2]
    deep = down_train.shape[1]

    def shift_by(a, n):
        return lax.ppermute(a, "tp", [(i, (i + 2 * n) % tp) for i in range(tp)])

    def swap(a):
        return lax.ppermute(a, "tp", [(i, i ^ 1) for i in range(tp)])

    gain = norm_gain[:, None]
    side = 4
    f = lax.axis_index("fs")
    place = jnp.stack([chip, core, f // side, f % side]).astype(jnp.int32)

    def along(a, n, y):
        pairs = []
        for i in range(experts):
            z_at, y_at = i // side, i % side
            to = z_at * side + (y_at + n) % side if y else ((z_at + n) % side) * side + y_at
            pairs.append((i, to))
        return lax.ppermute(a, "fs", pairs)

    shared_down_local = shared_down_train.astype(bf16)

    def pack(train, half_at):
        first_col = half_at * cols // 2
        return jnp.concatenate(
            [(gain * train).astype(bf16)]
            + [shared_down_local[:, first_col + c : first_col + c + hs] for c in (0, hs)],
            axis=0,
        )

    packs = (pack(shared_gate_train, 0), pack(shared_up_train, 1))
    groups = [[p] for p in packs]
    for n in range(1, side):
        for h, group in enumerate(groups):
            group.append(along(packs[h], n, h == 0))
    groups = [[jnp.stack(g)] for g in groups]
    for n in range(1, side):
        for h, group in enumerate(groups):
            group.append(along(group[0], n, h == 1))

    steps = 8
    anywhere = pl.BlockSpec(memory_space=pl.ANY)
    outgoing, slots = pl.pallas_call(
        functools.partial(route_kernel, half),
        grid=(1,),
        in_specs=[whole((top_count, tok_rows)), anywhere],
        out_specs=[whole((rows, quarter)), whole((top_count, tok_rows))],
        out_shape=[
            jax.ShapeDtypeStruct((rows, quarter), bf16),
            jax.ShapeDtypeStruct((top_count, tok_rows), jnp.int32),
        ],
        scratch_shapes=[
            pltpu.VMEM((tok_rows, quarter), bf16),
            pltpu.VMEM((rows, tok_rows), bf16),
            pltpu.SemaphoreType.DMA(()),
        ],
        compiler_params=vmem_limit(60),
        cost_estimate=cost(2 * rows * tok_rows * quarter, 4 * tok_rows * quarter),
    )(route_expert.T, tokens)
    normed = pl.pallas_call(
        norm_kernel,
        grid=(1,),
        in_specs=[anywhere],
        out_specs=anywhere,
        out_shape=jax.ShapeDtypeStruct((tok_rows, width), bf16),
        scratch_shapes=[
            pltpu.VMEM((tok_rows, width), bf16),
            pltpu.VMEM((tok_rows, width), bf16),
            pltpu.SemaphoreType.DMA((steps,)),
            pltpu.SemaphoreType.DMA((steps,)),
        ],
        compiler_params=vmem_limit(60),
        cost_estimate=cost(16 * tok_rows * width, 4 * tok_rows * width),
    )(tokens)
    arriving = lax.all_to_all(
        outgoing.reshape(experts, half, quarter), "fs", split_axis=0, concat_axis=0, tiled=True
    )

    gu_local = jnp.concatenate(
        [(gain[None] * gate_train).astype(bf16), (gain[None] * up_train).astype(bf16)], axis=2
    )
    mid = rows // 2
    arriving = arriving.reshape(rows, quarter)
    top, bottom = together(arriving[:mid], arriving[mid:])
    gu_local, top, bottom = together(gu_local, top, bottom)
    gu = lax.all_to_all(gu_local, "fs", split_axis=0, concat_axis=0, tiled=True)
    down_local, gu = together(down_train.astype(bf16), gu)
    down_cols = lax.all_to_all(down_local, "fs", split_axis=0, concat_axis=0, tiled=True)
    gu = gu.reshape(width, 2 * hs)
    gu_other = swap(gu)
    down_cols = down_cols.reshape(experts * deep, cols)
    down_other = swap(down_cols)

    left_top = shift_by(top, 1)
    right_bottom = shift_by(bottom, -1)
    right_top = shift_by(top, -1)
    left_bottom = shift_by(bottom, 1)
    far_top = shift_by(left_top, 1)
    far_bottom = shift_by(right_bottom, -1)

    def marker(a, b):
        return pl.pallas_call(
            mark_kernel,
            grid=(1,),
            in_specs=[whole(tile)] * 2,
            out_specs=whole(tile),
            out_shape=jax.ShapeDtypeStruct(tile, bf16),
            cost_estimate=cost(1 << 20, 1 << 14),
        )(a, b)

    tile = (16, 128)
    mark = marker(left_top, right_bottom)
    soon = marker(*packs)
    mark = marker(mark, soon)
    x_spec = pl.BlockSpec((mid // 2, quarter), lambda i, s: (i, 0))
    acc_spec = pl.BlockSpec((2, mid // 2, 4 * hs), lambda i, s: (0, i, 0))
    w_spec = pl.BlockSpec((quarter, 2 * hs), lambda i, s: (lax.rem(s[0] + chips // 2, chips), 0))
    acc, sq = pl.pallas_call(
        first_kernel,
        grid_spec=pltpu.PrefetchScalarGridSpec(
            num_scalar_prefetch=1,
            grid=(2,),
            in_specs=[x_spec] * 6 + [whole((width, 2 * hs))] * 2 + [whole(tile)],
            out_specs=[acc_spec, pl.BlockSpec((2, mid // 2, 128), lambda i, s: (0, i, 0))],
        ),
        out_shape=[
            jax.ShapeDtypeStruct((2, mid, 4 * hs), f32),
            jax.ShapeDtypeStruct((2, mid, 128), f32),
        ],
        compiler_params=vmem_limit(24),
        cost_estimate=cost(2 * rows * 3 * quarter * 4 * hs, 8 * width * hs),
    )(place, top, left_top, right_top, bottom, left_bottom, right_bottom, gu, gu_other, mark)
    hidden = pl.pallas_call(
        functools.partial(hidden_kernel, width),
        grid_spec=pltpu.PrefetchScalarGridSpec(
            num_scalar_prefetch=1,
            grid=(1,),
            in_specs=[whole((mid, quarter))] * 2
            + [whole((2, mid, 4 * hs)), whole((2, mid, 128)), w_spec, w_spec],
            out_specs=whole((2, mid, 2 * hs)),
        ),
        out_shape=jax.ShapeDtypeStruct((2, mid, 2 * hs), bf16),
        compiler_params=vmem_limit(24),
        cost_estimate=cost(2 * rows * quarter * 4 * hs, 8 * quarter * hs),
    )(place, far_top, far_bottom, acc, sq, gu, gu_other).reshape(rows, 2 * hs)

    shared_gate, shared_up, shared_hid, shared_cols, shared_out = pl.pallas_call(
        shared_kernel,
        grid_spec=pltpu.PrefetchScalarGridSpec(
            num_scalar_prefetch=1,
            grid=(1,),
            in_specs=[whole((tok_rows, width))] + [whole(groups[0][0].shape)] * 8,
            out_specs=[
                pl.BlockSpec(memory_space=pltpu.HBM),
                pl.BlockSpec(memory_space=pltpu.HBM),
                whole((tok_rows, hs)),
                whole((experts * deep, cols)),
                whole((experts * deep // 2, cols)),
            ],
            scratch_shapes=[
                pltpu.VMEM((width, 2 * hs), bf16),
                pltpu.SemaphoreType.DMA((2,)),
            ],
        ),
        out_shape=[
            jax.ShapeDtypeStruct((width, hs), bf16),
            jax.ShapeDtypeStruct((width, hs), bf16),
            jax.ShapeDtypeStruct((tok_rows, hs), bf16),
            jax.ShapeDtypeStruct((experts * deep, cols), bf16),
            jax.ShapeDtypeStruct((experts * deep // 2, cols), bf16),
        ],
        compiler_params=vmem_limit(60),
        cost_estimate=cost(4 * tok_rows * width * hs, 8 * width * hs),
    )(place, normed, *groups[0], *groups[1])
    shared_other = swap(shared_out)
    units = [shared_hid]
    for n in (1, -1, 2):
        units.append(shift_by(shared_hid, n))
    units = jnp.stack(units)
    units_other = swap(units)

    hid_left = shift_by(hidden, 1)
    hid_right = shift_by(hidden, -1)
    hid_far = shift_by(hidden, 2)
    sums = pl.pallas_call(
        down_kernel,
        grid_spec=pltpu.PrefetchScalarGridSpec(
            num_scalar_prefetch=1,
            grid=(1,),
            in_specs=[whole((rows, 2 * hs))] * 4 + [whole((experts * deep, cols))] * 2,
            out_specs=pl.BlockSpec(memory_space=pltpu.HBM),
            scratch_shapes=[
                pltpu.VMEM((rows, experts * deep), bf16),
                pltpu.VMEM((2, experts, half, cols), bf16),
                pltpu.SemaphoreType.DMA((2,)),
            ],
        ),
        out_shape=jax.ShapeDtypeStruct((experts, 2, half, cols), bf16),
        compiler_params=vmem_limit(60),
        cost_estimate=cost(4 * rows * experts * deep * cols, 8 * experts * deep * cols),
    )(place, hidden, hid_left, hid_right, hid_far, down_cols, down_other)
    returned = lax.all_to_all(sums, "fs", split_axis=0, concat_axis=0, tiled=True)
    got_other = swap(returned[:, 1].reshape(rows, cols))

    spots = jnp.arange(rows, dtype=jnp.int32)[None, :]

    def mixing(which):
        weights = 0
        for k in range(top_count):
            local = slots[k] - which * half
            here = (local >= 0) & (local < half)
            target = jnp.where(here, route_expert[:, k] * half + local, -1)
            at = target[:, None] == spots
            weights = weights + jnp.where(at, route_weight[:, k][:, None].astype(bf16), 0)
        return weights

    mix_own, mix_other = together(mixing(core), mixing(1 - core))

    def mix(weights, got, base, dtype):
        return pl.pallas_call(
            mix_kernel,
            grid=(1,),
            in_specs=[
                whole((tok_rows, rows)),
                whole((experts, 1, half, cols)) if got.ndim == 4 else whole((rows, cols)),
                whole((tok_rows, cols)),
            ],
            out_specs=whole((tok_rows, cols)),
            out_shape=jax.ShapeDtypeStruct((tok_rows, cols), dtype),
            compiler_params=vmem_limit(14),
            cost_estimate=cost(2 * tok_rows * rows * cols, 4 * tok_rows * rows),
        )(weights, got, base)

    base = pl.pallas_call(
        base_kernel,
        grid_spec=pltpu.PrefetchScalarGridSpec(
            num_scalar_prefetch=1,
            grid=(1,),
            in_specs=[whole((chips, tok_rows, hs))] * 2 + [whole((experts * deep, cols))],
            out_specs=whole((tok_rows, cols)),
            scratch_shapes=[pltpu.VMEM((tok_rows, experts * deep), bf16)],
        ),
        out_shape=jax.ShapeDtypeStruct((tok_rows, cols), f32),
        compiler_params=vmem_limit(14),
        cost_estimate=cost(2 * tok_rows * experts * deep * cols, 4 * tok_rows * rows),
    )(place, units, units_other, shared_cols)
    part = mix(mix_own, returned, base, f32)
    mixed = mix(mix_other, got_other, part, bf16)

    chunks = pl.pallas_call(
        chunk_kernel,
        grid_spec=pltpu.PrefetchScalarGridSpec(
            num_scalar_prefetch=1,
            grid=(1,),
            in_specs=[whole((experts * deep, cols))] * 2
            + [whole((experts * deep, cols)), whole((experts * deep // 2, cols))],
            out_specs=[whole((2 * hs, 2 * cols))] * chips,
        ),
        out_shape=[jax.ShapeDtypeStruct((2 * hs, 2 * cols), bf16)] * chips,
        compiler_params=vmem_limit(60),
        cost_estimate=cost(1 << 30, 8 * hs * width),
    )(place, down_cols, down_other, shared_cols, shared_other)
    pieces = [chunks[0]]
    for n in range(1, chips):
        pieces.append(shift_by(chunks[n], n))
    expert_down, shared_down = pl.pallas_call(
        join_kernel,
        grid_spec=pltpu.PrefetchScalarGridSpec(
            num_scalar_prefetch=1,
            grid=(1,),
            in_specs=[whole((2 * hs, 2 * cols))] * 4,
            out_specs=[anywhere] * 2,
            scratch_shapes=[pltpu.SemaphoreType.DMA((4 * chips,))],
        ),
        out_shape=[jax.ShapeDtypeStruct((hs, width), bf16)] * 2,
        compiler_params=vmem_limit(14),
        cost_estimate=cost(1 << 20, 8 * hs * width),
    )(place, *pieces)
    expert_gate = gu[None, :, :hs]
    expert_up = gu[None, :, hs:]
    return (
        expert_gate,
        expert_up,
        expert_down[None],
        shared_gate,
        shared_up,
        shared_down,
        mixed,
    )


def solution(mesh):
    placed = (
        P("fs", None),
        P("fs"),
        P(None, "fs", "tp"),
        P(None, "fs", "tp"),
        P(None, "fs", "tp"),
        P("fs", "tp"),
        P("fs", "tp"),
        P("fs", "tp"),
        P("fs", None),
        P("fs", None),
    )


    return jax.shard_map(
        on_device,
        mesh=mesh,
        in_specs=placed,
        out_specs=(
            P("fs", None, "tp"),
            P("fs", None, "tp"),
            P("fs", "tp", None),
            P(None, "tp"),
            P(None, "tp"),
            P("tp", None),
            P("fs", "tp"),
        ),
        check_vma=False,
    )
```

```python
import functools

import jax
import jax.numpy as jnp
from jax import lax
from jax.experimental import pallas as pl
from jax.experimental.pallas import tpu as pltpu
from jax.sharding import PartitionSpec as P

norm_eps = 1e-06
bf16 = jnp.bfloat16
f32 = jnp.float32


def dot(a, b):
    return jnp.dot(a, b, preferred_element_type=f32)


def together(*values):
    return lax.optimization_barrier(values)


def cost(flops, moved):
    return pl.CostEstimate(flops=flops, bytes_accessed=moved, transcendentals=0)


def vmem_limit(mib):
    return pltpu.CompilerParams(vmem_limit_bytes=mib << 20)


def route_kernel(half, route_ref, tok_ref, out_ref, slot_ref, kept, placing, sem):
    t = lax.axis_index("tp")
    chip, core = t // 2, lax.rem(t, 2)
    tok_rows, quarter = kept.shape
    spots = placing.shape[0]
    experts = spots // half
    at = pl.ds(pl.multiple_of(chip * quarter, quarter), quarter)
    read = pltpu.make_async_copy(tok_ref.at[:, at], kept, sem)
    read.start()

    ids = lax.broadcasted_iota(jnp.int32, (experts, tok_rows), 0)
    hot = [route_ref[k : k + 1, :] == ids for k in range(route_ref.shape[0])]
    named = sum(jnp.where(x, 1.0, 0.0) for x in hot).astype(bf16)
    ahead = lax.broadcasted_iota(jnp.int32, (tok_rows, tok_rows), 0) < (
        lax.broadcasted_iota(jnp.int32, (tok_rows, tok_rows), 1)
    )
    earlier = dot(named, jnp.where(ahead, 1.0, 0.0).astype(bf16))
    spot = lax.broadcasted_iota(jnp.int32, (spots, tok_rows), 0)
    total = jnp.zeros((spots, tok_rows), f32)
    for k, x in enumerate(hot):
        slot = jnp.sum(jnp.where(x, earlier, 0.0), axis=0, keepdims=True).astype(jnp.int32)
        slot_ref[k : k + 1, :] = slot
        local = slot - core * half
        here = (local >= 0) & (local < half)
        target = jnp.where(here, route_ref[k : k + 1, :] * half + local, -1)
        total = total + jnp.where(spot == target, 1.0, 0.0)
    placing[...] = total.astype(bf16)
    read.wait()
    for c in range(0, spots, 256):
        out_ref[c : c + 256, :] = dot(placing[c : c + 256, :], kept[...]).astype(bf16)


def norm_kernel(tok_ref, normed_ref, taken, given, in_sem, out_sem):
    steps = in_sem.shape[0]
    rows = taken.shape[0] // steps

    def span(step):
        return pl.ds(step * rows, rows)

    reads = [
        pltpu.make_async_copy(tok_ref.at[span(i)], taken.at[span(i)], in_sem.at[i])
        for i in range(steps)
    ]
    writes = [
        pltpu.make_async_copy(given.at[span(i)], normed_ref.at[span(i)], out_sem.at[i])
        for i in range(steps)
    ]
    for read in reads:
        read.start()
    for i in range(steps):
        reads[i].wait()
        for r in range(i * rows, (i + 1) * rows, 16):
            values = taken[r : r + 16, :].astype(f32)
            scale = lax.rsqrt(jnp.mean(values * values, axis=1, keepdims=True) + norm_eps)
            given[r : r + 16, :] = (values * scale).astype(bf16)
        if i:
            writes[i - 1].start()
    writes[steps - 1].start()
    for write in writes:
        write.wait()


def squares(x_ref):
    total = None
    for c in range(0, x_ref.shape[1], 128):
        values = x_ref[:, c : c + 128].astype(f32)
        total = values * values if total is None else total + values * values
    return total


def square_kernel(a_ref, b_ref, c_ref, d_ref, sq_ref):
    sq_ref[0] = squares(a_ref) + squares(b_ref)
    sq_ref[1] = squares(c_ref) + squares(d_ref)


def first_kernel(place_ref, *refs):
    x_refs, (w_own_ref, w_other_ref, some_ref, acc_ref, sq_ref) = refs[:6], refs[6:]
    chip = place_ref[0]
    quarter, wide = x_refs[0].shape[1], w_own_ref.shape[1]
    chips = w_own_ref.shape[0] // quarter
    for part in range(2):
        blocks = x_refs[3 * part : 3 * part + 3]
        for half, w_ref in ((0, w_own_ref), (1, w_other_ref)):
            total = None
            for x_ref, shift in zip(blocks, (0, chips - 1, 1)):
                at = pl.multiple_of(lax.rem(chip + shift, chips) * quarter, quarter)
                term = dot(x_ref[...], w_ref[pl.ds(at, quarter), :])
                total = term if total is None else total + term
            acc_ref[part, :, half * wide : (half + 1) * wide] = total
        sq_ref[part] = some_ref[part] + squares(blocks[2 - part])


def hidden_kernel(width, place_ref, far0_ref, far1_ref, acc_ref, sq_ref, w0_ref, w1_ref, out_ref):
    core = place_ref[1]
    wide = w0_ref.shape[1]
    hs = wide // 2
    for part, far_ref in enumerate((far0_ref, far1_ref)):
        sums = jnp.sum(sq_ref[part] + squares(far_ref), axis=1, keepdims=True)
        scale = lax.rsqrt(sums * (1.0 / width) + norm_eps)
        for half, w_ref, slot in ((0, w0_ref, core), (1, w1_ref, 1 - core)):
            total = acc_ref[part, :, half * wide : (half + 1) * wide]
            total = (total + dot(far_ref[...], w_ref[...])) * scale
            gate, up = total[:, :hs], total[:, hs:]
            value = (gate / (1.0 + jnp.exp(-gate)) * up).astype(bf16)
            out_ref[part, :, pl.ds(pl.multiple_of(slot * hs, hs), hs)] = value


def down_kernel(place_ref, h0_ref, h1_ref, h2_ref, h3_ref, w_own_ref, w_other_ref, out_ref, *scratch):
    line, held, sems = scratch
    chip = place_ref[0]
    depth = h0_ref.shape[1]
    chips = w_own_ref.shape[0] // depth
    parts = ((h0_ref, 0), (h1_ref, chips - 1), (h2_ref, 1), (h3_ref, chips // 2))
    for h_ref, shift in parts:
        at = pl.multiple_of(lax.rem(chip + shift, chips) * depth, depth)
        line[:, pl.ds(at, depth)] = h_ref[...]
    copies = []
    for part, w_ref in enumerate((w_own_ref, w_other_ref)):
        total = dot(line[...], w_ref[...]).astype(bf16)
        held[part] = total.reshape(held.shape[1:])
        copies.append(
            pltpu.make_async_copy(held.at[part], out_ref.at[:, part], sems.at[part])
        )
        copies[part].start()
    for copy in copies:
        copy.wait()


def shared_kernel(place_ref, x_ref, *refs):
    groups, outs, (line, sems) = (refs[:4], refs[4:8]), refs[8:13], refs[13:]
    gate_ref, up_ref, hid_ref, sd_ref, sd_out_ref = outs
    core, z, y = place_ref[1], place_ref[2], place_ref[3]
    hs = gate_ref.shape[1]
    side, size = groups[0][0].shape[0], line.shape[0] // 16
    deep = sd_ref.shape[0] // 16
    for h in range(2):
        for m, ref in enumerate(groups[h]):
            for n in range(side):
                dz, dy = (m, n) if h == 0 else (n, m)
                source = lax.rem(z + side - dz, side) * side + lax.rem(y + side - dy, side)
                block = ref[n, :size, :]
                at = pl.ds(pl.multiple_of(source * size, size), size)
                line[at, h * hs : (h + 1) * hs] = block
                at = pl.ds(pl.multiple_of(source * deep, deep), deep)
                for c in range(2):
                    col = (2 * h + c) * hs
                    sd_ref[at, col : col + hs] = ref[n, size + c * deep : size + (c + 1) * deep, :]
    for c in range(4):
        at = pl.ds(pl.multiple_of((2 * c + 1 - core) * hs, hs), hs)
        sd_out_ref[c * hs : (c + 1) * hs, :] = sd_ref[at, :]
    copies = [
        pltpu.make_async_copy(line.at[:, pl.ds(h * hs, hs)], out_ref, sems.at[h])
        for h, out_ref in enumerate((gate_ref, up_ref))
    ]
    for copy in copies:
        copy.start()
    total = dot(x_ref[...], line[...])
    gate, up = total[:, :hs], total[:, hs:]
    hid_ref[...] = (gate / (1.0 + jnp.exp(-gate)) * up).astype(bf16)
    for copy in copies:
        copy.wait()


def base_kernel(place_ref, own_ref, other_ref, sd_ref, out_ref, line):
    chip, core = place_ref[0], place_ref[1]
    hs = own_ref.shape[2]
    for ref, lane in ((own_ref, core), (other_ref, 1 - core)):
        for n, shift in enumerate((0, 3, 1, 2)):
            at = pl.multiple_of((lax.rem(chip + shift, 4) * 2 + lane) * hs, hs)
            line[:, pl.ds(at, hs)] = ref[n]
    out_ref[...] = dot(line[...], sd_ref[...])


def mix_kernel(weight_ref, got_ref, base_ref, out_ref):
    got = got_ref[...].reshape(weight_ref.shape[1], out_ref.shape[1])
    out_ref[...] = (base_ref[...] + dot(weight_ref[...], got)).astype(out_ref.dtype)


def chunk_kernel(place_ref, own_ref, other_ref, sd_ref, sd_other_ref, *out_refs):
    chip, core = place_ref[0], place_ref[1]
    hs, cols = out_refs[0].shape[0] // 2, own_ref.shape[1]
    for n, out_ref in enumerate(out_refs):
        target = lax.rem(chip + n, 4)
        at = pl.ds(pl.multiple_of((target * 2 + core) * hs, hs), hs)
        far = pl.ds(pl.multiple_of(target * hs, hs), hs)
        out_ref[:hs, :cols] = own_ref[at, :]
        out_ref[:hs, cols:] = other_ref[at, :]
        out_ref[hs:, :cols] = sd_ref[at, :]
        out_ref[hs:, cols:] = sd_other_ref[far, :]


def join_kernel(place_ref, p0_ref, p1_ref, p2_ref, p3_ref, routed_ref, shared_ref, sems):
    chip, core = place_ref[0], place_ref[1]
    hs = routed_ref.shape[0]
    cols = p0_ref.shape[1] // 2
    copies = []
    for shift, ref in enumerate((p0_ref, p1_ref, p2_ref, p3_ref)):
        source = lax.rem(chip + 4 - shift, 4)
        for half, lane in ((0, core), (1, 1 - core)):
            at = pl.ds(pl.multiple_of((source * 2 + lane) * cols, cols), cols)
            part = pl.ds(half * cols, cols)
            for top, out_ref in ((0, routed_ref), (hs, shared_ref)):
                copies.append(
                    pltpu.make_async_copy(
                        ref.at[pl.ds(top, hs), part], out_ref.at[:, at], sems.at[len(copies)]
                    )
                )
    for copy in copies:
        copy.start()
    for copy in copies:
        copy.wait()


def whole(shape):
    return pl.BlockSpec(shape, lambda *_: (0,) * len(shape))


def on_device(
    tokens,
    norm_gain,
    gate_train,
    up_train,
    down_train,
    shared_gate_train,
    shared_up_train,
    shared_down_train,
    route_expert,
    route_weight,
):
    experts = lax.axis_size("fs")
    tp = lax.axis_size("tp")
    t = lax.axis_index("tp")
    chips = tp // 2
    chip, core = t // 2, t % 2
    tok_rows, width = tokens.shape
    top_count = route_expert.shape[1]
    cap = 3 * tok_rows * top_count // (2 * experts)
    half = cap // 2
    rows = experts * half
    quarter = width // chips
    cols = width // tp
    hs = gate_train.shape[2]
    deep = down_train.shape[1]

    def shift_by(a, n):
        return lax.ppermute(a, "tp", [(i, (i + 2 * n) % tp) for i in range(tp)])

    def swap(a):
        return lax.ppermute(a, "tp", [(i, i ^ 1) for i in range(tp)])

    gain = norm_gain[:, None]
    side = 4
    f = lax.axis_index("fs")
    place = jnp.stack([chip, core, f // side, f % side]).astype(jnp.int32)

    def along(a, n, y):
        pairs = []
        for i in range(experts):
            z_at, y_at = i // side, i % side
            to = z_at * side + (y_at + n) % side if y else ((z_at + n) % side) * side + y_at
            pairs.append((i, to))
        return lax.ppermute(a, "fs", pairs)

    shared_down_local = shared_down_train.astype(bf16)

    def pack(train, half_at):
        first_col = half_at * cols // 2
        return jnp.concatenate(
            [(gain * train).astype(bf16)]
            + [shared_down_local[:, first_col + c : first_col + c + hs] for c in (0, hs)],
            axis=0,
        )

    packs = (pack(shared_gate_train, 0), pack(shared_up_train, 1))
    groups = [[p] for p in packs]
    for n in range(1, side):
        for h, group in enumerate(groups):
            group.append(along(packs[h], n, h == 0))
    groups = [[jnp.stack(g)] for g in groups]
    for n in range(1, side):
        for h, group in enumerate(groups):
            group.append(along(group[0], n, h == 1))

    steps = 8
    anywhere = pl.BlockSpec(memory_space=pl.ANY)
    outgoing, slots = pl.pallas_call(
        functools.partial(route_kernel, half),
        grid=(1,),
        in_specs=[whole((top_count, tok_rows)), anywhere],
        out_specs=[whole((rows, quarter)), whole((top_count, tok_rows))],
        out_shape=[
            jax.ShapeDtypeStruct((rows, quarter), bf16),
            jax.ShapeDtypeStruct((top_count, tok_rows), jnp.int32),
        ],
        scratch_shapes=[
            pltpu.VMEM((tok_rows, quarter), bf16),
            pltpu.VMEM((rows, tok_rows), bf16),
            pltpu.SemaphoreType.DMA(()),
        ],
        compiler_params=vmem_limit(60),
        cost_estimate=cost(2 * rows * tok_rows * quarter, 4 * tok_rows * quarter),
    )(route_expert.T, tokens)
    normed = pl.pallas_call(
        norm_kernel,
        grid=(1,),
        in_specs=[anywhere],
        out_specs=anywhere,
        out_shape=jax.ShapeDtypeStruct((tok_rows, width), bf16),
        scratch_shapes=[
            pltpu.VMEM((tok_rows, width), bf16),
            pltpu.VMEM((tok_rows, width), bf16),
            pltpu.SemaphoreType.DMA((steps,)),
            pltpu.SemaphoreType.DMA((steps,)),
        ],
        compiler_params=vmem_limit(60),
        cost_estimate=cost(16 * tok_rows * width, 4 * tok_rows * width),
    )(tokens)
    arriving = lax.all_to_all(
        outgoing.reshape(experts, half, quarter), "fs", split_axis=0, concat_axis=0, tiled=True
    )

    gu_local = jnp.concatenate(
        [(gain[None] * gate_train).astype(bf16), (gain[None] * up_train).astype(bf16)], axis=2
    )
    mid = rows // 2
    arriving = arriving.reshape(rows, quarter)
    top, bottom = together(arriving[:mid], arriving[mid:])
    gu_local, top, bottom = together(gu_local, top, bottom)
    gu = lax.all_to_all(gu_local, "fs", split_axis=0, concat_axis=0, tiled=True)
    down_local = down_train.astype(bf16)
    down_local, gu = together(down_local, gu)
    down_cols = lax.all_to_all(down_local, "fs", split_axis=0, concat_axis=0, tiled=True)
    gu = gu.reshape(width, 2 * hs)
    gu_other = swap(gu)
    down_cols = down_cols.reshape(experts * deep, cols)
    down_other = swap(down_cols)

    left_top = shift_by(top, 1)
    right_bottom = shift_by(bottom, -1)
    right_top = shift_by(top, -1)
    left_bottom = shift_by(bottom, 1)
    far_top = shift_by(left_top, 1)
    far_bottom = shift_by(right_bottom, -1)

    x_spec = pl.BlockSpec((mid // 2, quarter), lambda i, s: (i, 0))
    acc_spec = pl.BlockSpec((2, mid // 2, 4 * hs), lambda i, s: (0, i, 0))
    w_spec = pl.BlockSpec((quarter, 2 * hs), lambda i, s: (lax.rem(s[0] + chips // 2, chips), 0))
    sq_spec = pl.BlockSpec((2, mid // 2, 128), lambda i, *s: (0, i, 0))
    some = pl.pallas_call(
        square_kernel,
        grid=(2,),
        in_specs=[pl.BlockSpec((mid // 2, quarter), lambda i: (i, 0))] * 4,
        out_specs=sq_spec,
        out_shape=jax.ShapeDtypeStruct((2, mid, 128), f32),
        compiler_params=vmem_limit(24),
        cost_estimate=cost(4 * rows * width, rows * width),
    )(top, left_top, bottom, right_bottom)
    acc, sq = pl.pallas_call(
        first_kernel,
        grid_spec=pltpu.PrefetchScalarGridSpec(
            num_scalar_prefetch=1,
            grid=(2,),
            in_specs=[x_spec] * 6 + [whole((width, 2 * hs))] * 2 + [sq_spec],
            out_specs=[acc_spec, pl.BlockSpec((2, mid // 2, 128), lambda i, s: (0, i, 0))],
        ),
        out_shape=[
            jax.ShapeDtypeStruct((2, mid, 4 * hs), f32),
            jax.ShapeDtypeStruct((2, mid, 128), f32),
        ],
        compiler_params=vmem_limit(24),
        cost_estimate=cost(2 * rows * 3 * quarter * 4 * hs, 8 * width * hs),
    )(place, top, left_top, right_top, bottom, left_bottom, right_bottom, gu, gu_other, some)
    hidden = pl.pallas_call(
        functools.partial(hidden_kernel, width),
        grid_spec=pltpu.PrefetchScalarGridSpec(
            num_scalar_prefetch=1,
            grid=(1,),
            in_specs=[whole((mid, quarter))] * 2
            + [whole((2, mid, 4 * hs)), whole((2, mid, 128)), w_spec, w_spec],
            out_specs=whole((2, mid, 2 * hs)),
        ),
        out_shape=jax.ShapeDtypeStruct((2, mid, 2 * hs), bf16),
        compiler_params=vmem_limit(24),
        cost_estimate=cost(2 * rows * quarter * 4 * hs, 8 * quarter * hs),
    )(place, far_top, far_bottom, acc, sq, gu, gu_other).reshape(rows, 2 * hs)

    shared_gate, shared_up, shared_hid, shared_cols, shared_out = pl.pallas_call(
        shared_kernel,
        grid_spec=pltpu.PrefetchScalarGridSpec(
            num_scalar_prefetch=1,
            grid=(1,),
            in_specs=[whole((tok_rows, width))] + [whole(groups[0][0].shape)] * 8,
            out_specs=[
                pl.BlockSpec(memory_space=pltpu.HBM),
                pl.BlockSpec(memory_space=pltpu.HBM),
                whole((tok_rows, hs)),
                whole((experts * deep, cols)),
                whole((experts * deep // 2, cols)),
            ],
            scratch_shapes=[
                pltpu.VMEM((width, 2 * hs), bf16),
                pltpu.SemaphoreType.DMA((2,)),
            ],
        ),
        out_shape=[
            jax.ShapeDtypeStruct((width, hs), bf16),
            jax.ShapeDtypeStruct((width, hs), bf16),
            jax.ShapeDtypeStruct((tok_rows, hs), bf16),
            jax.ShapeDtypeStruct((experts * deep, cols), bf16),
            jax.ShapeDtypeStruct((experts * deep // 2, cols), bf16),
        ],
        compiler_params=vmem_limit(60),
        cost_estimate=cost(4 * tok_rows * width * hs, 8 * width * hs),
    )(place, normed, *groups[0], *groups[1])
    shared_other = swap(shared_out)
    units = [shared_hid]
    for n in (1, -1, 2):
        units.append(shift_by(shared_hid, n))
    units = jnp.stack(units)
    units_other = swap(units)

    hid_left = shift_by(hidden, 1)
    hid_right = shift_by(hidden, -1)
    hid_far = shift_by(hidden, 2)
    sums = pl.pallas_call(
        down_kernel,
        grid_spec=pltpu.PrefetchScalarGridSpec(
            num_scalar_prefetch=1,
            grid=(1,),
            in_specs=[whole((rows, 2 * hs))] * 4 + [whole((experts * deep, cols))] * 2,
            out_specs=pl.BlockSpec(memory_space=pltpu.HBM),
            scratch_shapes=[
                pltpu.VMEM((rows, experts * deep), bf16),
                pltpu.VMEM((2, experts, half, cols), bf16),
                pltpu.SemaphoreType.DMA((2,)),
            ],
        ),
        out_shape=jax.ShapeDtypeStruct((experts, 2, half, cols), bf16),
        compiler_params=vmem_limit(60),
        cost_estimate=cost(4 * rows * experts * deep * cols, 8 * experts * deep * cols),
    )(place, hidden, hid_left, hid_right, hid_far, down_cols, down_other)
    returned = lax.all_to_all(sums, "fs", split_axis=0, concat_axis=0, tiled=True)
    got_other = swap(returned[:, 1].reshape(rows, cols))

    spots = jnp.arange(rows, dtype=jnp.int32)[None, :]

    def mixing(which):
        weights = 0
        for k in range(top_count):
            local = slots[k] - which * half
            here = (local >= 0) & (local < half)
            target = jnp.where(here, route_expert[:, k] * half + local, -1)
            at = target[:, None] == spots
            weights = weights + jnp.where(at, route_weight[:, k][:, None].astype(bf16), 0)
        return weights

    mix_own, mix_other = together(mixing(core), mixing(1 - core))

    def mix(weights, got, base, dtype):
        return pl.pallas_call(
            mix_kernel,
            grid=(1,),
            in_specs=[
                whole((tok_rows, rows)),
                whole((experts, 1, half, cols)) if got.ndim == 4 else whole((rows, cols)),
                whole((tok_rows, cols)),
            ],
            out_specs=whole((tok_rows, cols)),
            out_shape=jax.ShapeDtypeStruct((tok_rows, cols), dtype),
            compiler_params=vmem_limit(14),
            cost_estimate=cost(2 * tok_rows * rows * cols, 4 * tok_rows * rows),
        )(weights, got, base)

    base = pl.pallas_call(
        base_kernel,
        grid_spec=pltpu.PrefetchScalarGridSpec(
            num_scalar_prefetch=1,
            grid=(1,),
            in_specs=[whole((chips, tok_rows, hs))] * 2 + [whole((experts * deep, cols))],
            out_specs=whole((tok_rows, cols)),
            scratch_shapes=[pltpu.VMEM((tok_rows, experts * deep), bf16)],
        ),
        out_shape=jax.ShapeDtypeStruct((tok_rows, cols), f32),
        compiler_params=vmem_limit(14),
        cost_estimate=cost(2 * tok_rows * experts * deep * cols, 4 * tok_rows * rows),
    )(place, units, units_other, shared_cols)
    part = mix(mix_own, returned, base, f32)
    mixed = mix(mix_other, got_other, part, bf16)

    chunks = pl.pallas_call(
        chunk_kernel,
        grid_spec=pltpu.PrefetchScalarGridSpec(
            num_scalar_prefetch=1,
            grid=(1,),
            in_specs=[whole((experts * deep, cols))] * 2
            + [whole((experts * deep, cols)), whole((experts * deep // 2, cols))],
            out_specs=[whole((2 * hs, 2 * cols))] * chips,
        ),
        out_shape=[jax.ShapeDtypeStruct((2 * hs, 2 * cols), bf16)] * chips,
        compiler_params=vmem_limit(60),
        cost_estimate=cost(1 << 30, 8 * hs * width),
    )(place, down_cols, down_other, shared_cols, shared_other)
    pieces = [chunks[0]]
    for n in range(1, chips):
        pieces.append(shift_by(chunks[n], n))
    expert_down, shared_down = pl.pallas_call(
        join_kernel,
        grid_spec=pltpu.PrefetchScalarGridSpec(
            num_scalar_prefetch=1,
            grid=(1,),
            in_specs=[whole((2 * hs, 2 * cols))] * 4,
            out_specs=[anywhere] * 2,
            scratch_shapes=[pltpu.SemaphoreType.DMA((4 * chips,))],
        ),
        out_shape=[jax.ShapeDtypeStruct((hs, width), bf16)] * 2,
        compiler_params=vmem_limit(14),
        cost_estimate=cost(1 << 20, 8 * hs * width),
    )(place, *pieces)
    expert_gate = gu[None, :, :hs]
    expert_up = gu[None, :, hs:]
    return (
        expert_gate,
        expert_up,
        expert_down[None],
        shared_gate,
        shared_up,
        shared_down,
        mixed,
    )


def solution(mesh):
    placed = (
        P("fs", None),
        P("fs"),
        P(None, "fs", "tp"),
        P(None, "fs", "tp"),
        P(None, "fs", "tp"),
        P("fs", "tp"),
        P("fs", "tp"),
        P("fs", "tp"),
        P("fs", None),
        P("fs", None),
    )


    return jax.shard_map(
        on_device,
        mesh=mesh,
        in_specs=placed,
        out_specs=(
            P("fs", None, "tp"),
            P("fs", None, "tp"),
            P("fs", "tp", None),
            P(None, "tp"),
            P(None, "tp"),
            P("tp", None),
            P("fs", "tp"),
        ),
        check_vma=False,
    )
```

```python
import functools

import jax
import jax.numpy as jnp
from jax import lax
from jax.experimental import pallas as pl
from jax.experimental.pallas import tpu as pltpu
from jax.sharding import PartitionSpec as P

norm_eps = 1e-06
bf16 = jnp.bfloat16
f32 = jnp.float32


def dot(a, b):
    return jnp.dot(a, b, preferred_element_type=f32)


def together(*values):
    return lax.optimization_barrier(values)


def cost(flops, moved):
    return pl.CostEstimate(flops=flops, bytes_accessed=moved, transcendentals=0)


def vmem_limit(mib):
    return pltpu.CompilerParams(vmem_limit_bytes=mib << 20)


def route_kernel(half, routes_ref, tok_ref, out_ref, slots_ref, *scratch):
    route_ref, slot_ref, kept, placing, held, sems = scratch
    t = lax.axis_index("tp")
    chip, core = t // 2, lax.rem(t, 2)
    tok_rows, quarter = kept.shape
    spots = placing.shape[0]
    experts = spots // half
    at = pl.ds(pl.multiple_of(chip * quarter, quarter), quarter)
    read = pltpu.make_async_copy(tok_ref.at[:, at], kept, sems.at[0])
    routes = pltpu.make_async_copy(routes_ref, route_ref, sems.at[1])
    routes.start()
    read.start()
    routes.wait()

    ids = lax.broadcasted_iota(jnp.int32, (experts, tok_rows), 0)
    hot = [route_ref[k : k + 1, :] == ids for k in range(route_ref.shape[0])]
    named = sum(jnp.where(x, 1.0, 0.0) for x in hot).astype(bf16)
    ahead = lax.broadcasted_iota(jnp.int32, (tok_rows, tok_rows), 0) < (
        lax.broadcasted_iota(jnp.int32, (tok_rows, tok_rows), 1)
    )
    earlier = dot(named, jnp.where(ahead, 1.0, 0.0).astype(bf16))
    spot = lax.broadcasted_iota(jnp.int32, (spots, tok_rows), 0)
    total = jnp.zeros((spots, tok_rows), f32)
    for k, x in enumerate(hot):
        slot = jnp.sum(jnp.where(x, earlier, 0.0), axis=0, keepdims=True).astype(jnp.int32)
        slot_ref[k : k + 1, :] = slot
        local = slot - core * half
        here = (local >= 0) & (local < half)
        target = jnp.where(here, route_ref[k : k + 1, :] * half + local, -1)
        total = total + jnp.where(spot == target, 1.0, 0.0)
    writes = [pltpu.make_async_copy(slot_ref, slots_ref, sems.at[2])]
    placing[...] = total.astype(bf16)
    writes[0].start()
    read.wait()
    for n, c in enumerate(range(0, spots, 256)):
        span = pl.ds(c, 256)
        held[c : c + 256, :] = dot(placing[c : c + 256, :], kept[...]).astype(bf16)
        writes.append(pltpu.make_async_copy(held.at[span], out_ref.at[span], sems.at[3 + n]))
        writes[-1].start()
    for write in writes:
        write.wait()


def norm_kernel(tok_ref, normed_ref, taken, given, in_sem, out_sem):
    steps = in_sem.shape[0]
    rows = taken.shape[0] // steps

    def span(step):
        return pl.ds(step * rows, rows)

    reads = [
        pltpu.make_async_copy(tok_ref.at[span(i)], taken.at[span(i)], in_sem.at[i])
        for i in range(steps)
    ]
    writes = [
        pltpu.make_async_copy(given.at[span(i)], normed_ref.at[span(i)], out_sem.at[i])
        for i in range(steps)
    ]
    for read in reads:
        read.start()
    for i in range(steps):
        reads[i].wait()
        for r in range(i * rows, (i + 1) * rows, 16):
            values = taken[r : r + 16, :].astype(f32)
            scale = lax.rsqrt(jnp.mean(values * values, axis=1, keepdims=True) + norm_eps)
            given[r : r + 16, :] = (values * scale).astype(bf16)
        if i:
            writes[i - 1].start()
    writes[steps - 1].start()
    for write in writes:
        write.wait()


def squares(x_ref):
    total = None
    for c in range(0, x_ref.shape[1], 128):
        values = x_ref[:, c : c + 128].astype(f32)
        total = values * values if total is None else total + values * values
    return total


def mark_kernel(a_ref, b_ref, out_ref):
    out_ref[...] = a_ref[...] + b_ref[...]


def first_kernel(place_ref, *refs):
    x_refs, (w_own_ref, w_other_ref, _, acc_ref, sq_ref) = refs[:6], refs[6:]
    chip = place_ref[0]
    quarter, wide = x_refs[0].shape[1], w_own_ref.shape[1]
    chips = w_own_ref.shape[0] // quarter
    for part in range(2):
        blocks = x_refs[3 * part : 3 * part + 3]
        for half, w_ref in ((0, w_own_ref), (1, w_other_ref)):
            total = None
            for x_ref, shift in zip(blocks, (0, chips - 1, 1)):
                at = pl.multiple_of(lax.rem(chip + shift, chips) * quarter, quarter)
                term = dot(x_ref[...], w_ref[pl.ds(at, quarter), :])
                total = term if total is None else total + term
            acc_ref[part, :, half * wide : (half + 1) * wide] = total
        sq_ref[part] = squares(blocks[0]) + squares(blocks[1]) + squares(blocks[2])


def hidden_kernel(width, place_ref, far0_ref, far1_ref, acc_ref, sq_ref, w0_ref, w1_ref, out_ref):
    core = place_ref[1]
    wide = w0_ref.shape[1]
    hs = wide // 2
    for part, far_ref in enumerate((far0_ref, far1_ref)):
        sums = jnp.sum(sq_ref[part] + squares(far_ref), axis=1, keepdims=True)
        scale = lax.rsqrt(sums * (1.0 / width) + norm_eps)
        for half, w_ref, slot in ((0, w0_ref, core), (1, w1_ref, 1 - core)):
            total = acc_ref[part, :, half * wide : (half + 1) * wide]
            total = (total + dot(far_ref[...], w_ref[...])) * scale
            gate, up = total[:, :hs], total[:, hs:]
            value = (gate / (1.0 + jnp.exp(-gate)) * up).astype(bf16)
            out_ref[part, :, pl.ds(pl.multiple_of(slot * hs, hs), hs)] = value


def down_kernel(place_ref, h0_ref, h1_ref, h2_ref, h3_ref, w_own_ref, w_other_ref, out_ref, *scratch):
    line, held, sems = scratch
    chip = place_ref[0]
    depth = h0_ref.shape[1]
    chips = w_own_ref.shape[0] // depth
    parts = ((h0_ref, 0), (h1_ref, chips - 1), (h2_ref, 1), (h3_ref, chips // 2))
    for h_ref, shift in parts:
        at = pl.multiple_of(lax.rem(chip + shift, chips) * depth, depth)
        line[:, pl.ds(at, depth)] = h_ref[...]
    copies = []
    for part, w_ref in enumerate((w_own_ref, w_other_ref)):
        total = dot(line[...], w_ref[...]).astype(bf16)
        held[part] = total.reshape(held.shape[1:])
        copies.append(
            pltpu.make_async_copy(held.at[part], out_ref.at[:, part], sems.at[part])
        )
        copies[part].start()
    for copy in copies:
        copy.wait()


def shared_kernel(place_ref, x_ref, *refs):
    groups, outs, (line, sems) = (refs[:4], refs[4:8]), refs[8:13], refs[13:]
    gate_ref, up_ref, hid_ref, sd_ref, sd_out_ref = outs
    core, z, y = place_ref[1], place_ref[2], place_ref[3]
    hs = gate_ref.shape[1]
    side, size = groups[0][0].shape[0], line.shape[0] // 16
    deep = sd_ref.shape[0] // 16
    for h in range(2):
        for m, ref in enumerate(groups[h]):
            for n in range(side):
                dz, dy = (m, n) if h == 0 else (n, m)
                source = lax.rem(z + side - dz, side) * side + lax.rem(y + side - dy, side)
                block = ref[n, :size, :]
                at = pl.ds(pl.multiple_of(source * size, size), size)
                line[at, h * hs : (h + 1) * hs] = block
                at = pl.ds(pl.multiple_of(source * deep, deep), deep)
                for c in range(2):
                    col = (2 * h + c) * hs
                    sd_ref[at, col : col + hs] = ref[n, size + c * deep : size + (c + 1) * deep, :]
    for c in range(4):
        at = pl.ds(pl.multiple_of((2 * c + 1 - core) * hs, hs), hs)
        sd_out_ref[c * hs : (c + 1) * hs, :] = sd_ref[at, :]
    copies = [
        pltpu.make_async_copy(line.at[:, pl.ds(h * hs, hs)], out_ref, sems.at[h])
        for h, out_ref in enumerate((gate_ref, up_ref))
    ]
    for copy in copies:
        copy.start()
    total = dot(x_ref[...], line[...])
    gate, up = total[:, :hs], total[:, hs:]
    hid_ref[...] = (gate / (1.0 + jnp.exp(-gate)) * up).astype(bf16)
    for copy in copies:
        copy.wait()


def base_kernel(place_ref, own_ref, other_ref, sd_ref, out_ref, line):
    chip, core = place_ref[0], place_ref[1]
    hs = own_ref.shape[2]
    for ref, lane in ((own_ref, core), (other_ref, 1 - core)):
        for n, shift in enumerate((0, 3, 1, 2)):
            at = pl.multiple_of((lax.rem(chip + shift, 4) * 2 + lane) * hs, hs)
            line[:, pl.ds(at, hs)] = ref[n]
    out_ref[...] = dot(line[...], sd_ref[...])


def mix_kernel(weight_ref, got_ref, base_ref, out_ref):
    got = got_ref[...].reshape(weight_ref.shape[1], out_ref.shape[1])
    out_ref[...] = (base_ref[...] + dot(weight_ref[...], got)).astype(out_ref.dtype)


def chunk_kernel(place_ref, own_ref, other_ref, sd_ref, sd_other_ref, *out_refs):
    chip, core = place_ref[0], place_ref[1]
    hs, cols = out_refs[0].shape[0] // 2, own_ref.shape[1]
    for n, out_ref in enumerate(out_refs):
        target = lax.rem(chip + n, 4)
        at = pl.ds(pl.multiple_of((target * 2 + core) * hs, hs), hs)
        far = pl.ds(pl.multiple_of(target * hs, hs), hs)
        out_ref[:hs, :cols] = own_ref[at, :]
        out_ref[:hs, cols:] = other_ref[at, :]
        out_ref[hs:, :cols] = sd_ref[at, :]
        out_ref[hs:, cols:] = sd_other_ref[far, :]


def join_kernel(place_ref, p0_ref, p1_ref, p2_ref, p3_ref, routed_ref, shared_ref, sems):
    chip, core = place_ref[0], place_ref[1]
    hs = routed_ref.shape[0]
    cols = p0_ref.shape[1] // 2
    copies = []
    for shift, ref in enumerate((p0_ref, p1_ref, p2_ref, p3_ref)):
        source = lax.rem(chip + 4 - shift, 4)
        for half, lane in ((0, core), (1, 1 - core)):
            at = pl.ds(pl.multiple_of((source * 2 + lane) * cols, cols), cols)
            part = pl.ds(half * cols, cols)
            for top, out_ref in ((0, routed_ref), (hs, shared_ref)):
                copies.append(
                    pltpu.make_async_copy(
                        ref.at[pl.ds(top, hs), part], out_ref.at[:, at], sems.at[len(copies)]
                    )
                )
    for copy in copies:
        copy.start()
    for copy in copies:
        copy.wait()


def whole(shape):
    return pl.BlockSpec(shape, lambda *_: (0,) * len(shape))


def on_device(
    tokens,
    norm_gain,
    gate_train,
    up_train,
    down_train,
    shared_gate_train,
    shared_up_train,
    shared_down_train,
    route_expert,
    route_weight,
):
    experts = lax.axis_size("fs")
    tp = lax.axis_size("tp")
    t = lax.axis_index("tp")
    chips = tp // 2
    chip, core = t // 2, t % 2
    tok_rows, width = tokens.shape
    top_count = route_expert.shape[1]
    cap = 3 * tok_rows * top_count // (2 * experts)
    half = cap // 2
    rows = experts * half
    quarter = width // chips
    cols = width // tp
    hs = gate_train.shape[2]
    deep = down_train.shape[1]

    def shift_by(a, n):
        return lax.ppermute(a, "tp", [(i, (i + 2 * n) % tp) for i in range(tp)])

    def swap(a):
        return lax.ppermute(a, "tp", [(i, i ^ 1) for i in range(tp)])

    gain = norm_gain[:, None]
    side = 4
    f = lax.axis_index("fs")
    place = jnp.stack([chip, core, f // side, f % side]).astype(jnp.int32)

    def along(a, n, y):
        pairs = []
        for i in range(experts):
            z_at, y_at = i // side, i % side
            to = z_at * side + (y_at + n) % side if y else ((z_at + n) % side) * side + y_at
            pairs.append((i, to))
        return lax.ppermute(a, "fs", pairs)

    shared_down_local = shared_down_train.astype(bf16)

    def pack(train, half_at):
        first_col = half_at * cols // 2
        return jnp.concatenate(
            [(gain * train).astype(bf16)]
            + [shared_down_local[:, first_col + c : first_col + c + hs] for c in (0, hs)],
            axis=0,
        )

    packs = (pack(shared_gate_train, 0), pack(shared_up_train, 1))
    groups = [[p] for p in packs]
    for n in range(1, side):
        for h, group in enumerate(groups):
            group.append(along(packs[h], n, h == 0))
    groups = [[jnp.stack(g)] for g in groups]
    for n in range(1, side):
        for h, group in enumerate(groups):
            group.append(along(group[0], n, h == 1))

    steps = 8
    anywhere = pl.BlockSpec(memory_space=pl.ANY)
    outgoing, slots = pl.pallas_call(
        functools.partial(route_kernel, half),
        grid=(1,),
        in_specs=[anywhere, anywhere],
        out_specs=[anywhere, anywhere],
        out_shape=[
            jax.ShapeDtypeStruct((rows, quarter), bf16),
            jax.ShapeDtypeStruct((top_count, tok_rows), jnp.int32),
        ],
        scratch_shapes=[
            pltpu.VMEM((top_count, tok_rows), jnp.int32),
            pltpu.VMEM((top_count, tok_rows), jnp.int32),
            pltpu.VMEM((tok_rows, quarter), bf16),
            pltpu.VMEM((rows, tok_rows), bf16),
            pltpu.VMEM((rows, quarter), bf16),
            pltpu.SemaphoreType.DMA((3 + rows // 256,)),
        ],
        compiler_params=vmem_limit(60),
        cost_estimate=cost(2 * rows * tok_rows * quarter, 4 * tok_rows * quarter),
    )(route_expert.T, tokens)
    normed = pl.pallas_call(
        norm_kernel,
        grid=(1,),
        in_specs=[anywhere],
        out_specs=anywhere,
        out_shape=jax.ShapeDtypeStruct((tok_rows, width), bf16),
        scratch_shapes=[
            pltpu.VMEM((tok_rows, width), bf16),
            pltpu.VMEM((tok_rows, width), bf16),
            pltpu.SemaphoreType.DMA((steps,)),
            pltpu.SemaphoreType.DMA((steps,)),
        ],
        compiler_params=vmem_limit(60),
        cost_estimate=cost(16 * tok_rows * width, 4 * tok_rows * width),
    )(tokens)
    arriving = lax.all_to_all(
        outgoing.reshape(experts, half, quarter), "fs", split_axis=0, concat_axis=0, tiled=True
    )

    gu_local = jnp.concatenate(
        [(gain[None] * gate_train).astype(bf16), (gain[None] * up_train).astype(bf16)], axis=2
    )
    mid = rows // 2
    arriving = arriving.reshape(rows, quarter)
    top, bottom = together(arriving[:mid], arriving[mid:])
    gu_local, top, bottom = together(gu_local, top, bottom)
    gu = lax.all_to_all(gu_local, "fs", split_axis=0, concat_axis=0, tiled=True)
    down_local, gu = together(down_train.astype(bf16), gu)
    down_cols = lax.all_to_all(down_local, "fs", split_axis=0, concat_axis=0, tiled=True)
    gu = gu.reshape(width, 2 * hs)
    gu_other = swap(gu)
    down_cols = down_cols.reshape(experts * deep, cols)
    down_other = swap(down_cols)

    left_top = shift_by(top, 1)
    right_bottom = shift_by(bottom, -1)
    right_top = shift_by(top, -1)
    left_bottom = shift_by(bottom, 1)
    far_top = shift_by(left_top, 1)
    far_bottom = shift_by(right_bottom, -1)

    def marker(a, b):
        return pl.pallas_call(
            mark_kernel,
            grid=(1,),
            in_specs=[whole(tile)] * 2,
            out_specs=whole(tile),
            out_shape=jax.ShapeDtypeStruct(tile, bf16),
            cost_estimate=cost(1 << 20, 1 << 14),
        )(a, b)

    tile = (16, 128)
    mark = marker(left_top, right_bottom)
    soon = marker(*packs)
    mark = marker(mark, soon)
    x_spec = pl.BlockSpec((mid // 2, quarter), lambda i, s: (i, 0))
    acc_spec = pl.BlockSpec((2, mid // 2, 4 * hs), lambda i, s: (0, i, 0))
    w_spec = pl.BlockSpec((quarter, 2 * hs), lambda i, s: (lax.rem(s[0] + chips // 2, chips), 0))
    acc, sq = pl.pallas_call(
        first_kernel,
        grid_spec=pltpu.PrefetchScalarGridSpec(
            num_scalar_prefetch=1,
            grid=(2,),
            in_specs=[x_spec] * 6 + [whole((width, 2 * hs))] * 2 + [whole(tile)],
            out_specs=[acc_spec, pl.BlockSpec((2, mid // 2, 128), lambda i, s: (0, i, 0))],
        ),
        out_shape=[
            jax.ShapeDtypeStruct((2, mid, 4 * hs), f32),
            jax.ShapeDtypeStruct((2, mid, 128), f32),
        ],
        compiler_params=vmem_limit(24),
        cost_estimate=cost(2 * rows * 3 * quarter * 4 * hs, 8 * width * hs),
    )(place, top, left_top, right_top, bottom, left_bottom, right_bottom, gu, gu_other, mark)
    hidden = pl.pallas_call(
        functools.partial(hidden_kernel, width),
        grid_spec=pltpu.PrefetchScalarGridSpec(
            num_scalar_prefetch=1,
            grid=(1,),
            in_specs=[whole((mid, quarter))] * 2
            + [whole((2, mid, 4 * hs)), whole((2, mid, 128)), w_spec, w_spec],
            out_specs=whole((2, mid, 2 * hs)),
        ),
        out_shape=jax.ShapeDtypeStruct((2, mid, 2 * hs), bf16),
        compiler_params=vmem_limit(24),
        cost_estimate=cost(2 * rows * quarter * 4 * hs, 8 * quarter * hs),
    )(place, far_top, far_bottom, acc, sq, gu, gu_other).reshape(rows, 2 * hs)

    shared_gate, shared_up, shared_hid, shared_cols, shared_out = pl.pallas_call(
        shared_kernel,
        grid_spec=pltpu.PrefetchScalarGridSpec(
            num_scalar_prefetch=1,
            grid=(1,),
            in_specs=[whole((tok_rows, width))] + [whole(groups[0][0].shape)] * 8,
            out_specs=[
                pl.BlockSpec(memory_space=pltpu.HBM),
                pl.BlockSpec(memory_space=pltpu.HBM),
                whole((tok_rows, hs)),
                whole((experts * deep, cols)),
                whole((experts * deep // 2, cols)),
            ],
            scratch_shapes=[
                pltpu.VMEM((width, 2 * hs), bf16),
                pltpu.SemaphoreType.DMA((2,)),
            ],
        ),
        out_shape=[
            jax.ShapeDtypeStruct((width, hs), bf16),
            jax.ShapeDtypeStruct((width, hs), bf16),
            jax.ShapeDtypeStruct((tok_rows, hs), bf16),
            jax.ShapeDtypeStruct((experts * deep, cols), bf16),
            jax.ShapeDtypeStruct((experts * deep // 2, cols), bf16),
        ],
        compiler_params=vmem_limit(60),
        cost_estimate=cost(4 * tok_rows * width * hs, 8 * width * hs),
    )(place, normed, *groups[0], *groups[1])
    shared_other = swap(shared_out)
    units = [shared_hid]
    for n in (1, -1, 2):
        units.append(shift_by(shared_hid, n))
    units = jnp.stack(units)
    units_other = swap(units)

    hid_left = shift_by(hidden, 1)
    hid_right = shift_by(hidden, -1)
    hid_far = shift_by(hidden, 2)
    sums = pl.pallas_call(
        down_kernel,
        grid_spec=pltpu.PrefetchScalarGridSpec(
            num_scalar_prefetch=1,
            grid=(1,),
            in_specs=[whole((rows, 2 * hs))] * 4 + [whole((experts * deep, cols))] * 2,
            out_specs=pl.BlockSpec(memory_space=pltpu.HBM),
            scratch_shapes=[
                pltpu.VMEM((rows, experts * deep), bf16),
                pltpu.VMEM((2, experts, half, cols), bf16),
                pltpu.SemaphoreType.DMA((2,)),
            ],
        ),
        out_shape=jax.ShapeDtypeStruct((experts, 2, half, cols), bf16),
        compiler_params=vmem_limit(60),
        cost_estimate=cost(4 * rows * experts * deep * cols, 8 * experts * deep * cols),
    )(place, hidden, hid_left, hid_right, hid_far, down_cols, down_other)
    returned = lax.all_to_all(sums, "fs", split_axis=0, concat_axis=0, tiled=True)
    got_other = swap(returned[:, 1].reshape(rows, cols))

    spots = jnp.arange(rows, dtype=jnp.int32)[None, :]

    def mixing(which):
        weights = 0
        for k in range(top_count):
            local = slots[k] - which * half
            here = (local >= 0) & (local < half)
            target = jnp.where(here, route_expert[:, k] * half + local, -1)
            at = target[:, None] == spots
            weights = weights + jnp.where(at, route_weight[:, k][:, None].astype(bf16), 0)
        return weights

    mix_own, mix_other = together(mixing(core), mixing(1 - core))

    def mix(weights, got, base, dtype):
        return pl.pallas_call(
            mix_kernel,
            grid=(1,),
            in_specs=[
                whole((tok_rows, rows)),
                whole((experts, 1, half, cols)) if got.ndim == 4 else whole((rows, cols)),
                whole((tok_rows, cols)),
            ],
            out_specs=whole((tok_rows, cols)),
            out_shape=jax.ShapeDtypeStruct((tok_rows, cols), dtype),
            compiler_params=vmem_limit(14),
            cost_estimate=cost(2 * tok_rows * rows * cols, 4 * tok_rows * rows),
        )(weights, got, base)

    base = pl.pallas_call(
        base_kernel,
        grid_spec=pltpu.PrefetchScalarGridSpec(
            num_scalar_prefetch=1,
            grid=(1,),
            in_specs=[whole((chips, tok_rows, hs))] * 2 + [whole((experts * deep, cols))],
            out_specs=whole((tok_rows, cols)),
            scratch_shapes=[pltpu.VMEM((tok_rows, experts * deep), bf16)],
        ),
        out_shape=jax.ShapeDtypeStruct((tok_rows, cols), f32),
        compiler_params=vmem_limit(14),
        cost_estimate=cost(2 * tok_rows * experts * deep * cols, 4 * tok_rows * rows),
    )(place, units, units_other, shared_cols)
    part = mix(mix_own, returned, base, f32)
    mixed = mix(mix_other, got_other, part, bf16)

    chunks = pl.pallas_call(
        chunk_kernel,
        grid_spec=pltpu.PrefetchScalarGridSpec(
            num_scalar_prefetch=1,
            grid=(1,),
            in_specs=[whole((experts * deep, cols))] * 2
            + [whole((experts * deep, cols)), whole((experts * deep // 2, cols))],
            out_specs=[whole((2 * hs, 2 * cols))] * chips,
        ),
        out_shape=[jax.ShapeDtypeStruct((2 * hs, 2 * cols), bf16)] * chips,
        compiler_params=vmem_limit(60),
        cost_estimate=cost(1 << 30, 8 * hs * width),
    )(place, down_cols, down_other, shared_cols, shared_other)
    pieces = [chunks[0]]
    for n in range(1, chips):
        pieces.append(shift_by(chunks[n], n))
    expert_down, shared_down = pl.pallas_call(
        join_kernel,
        grid_spec=pltpu.PrefetchScalarGridSpec(
            num_scalar_prefetch=1,
            grid=(1,),
            in_specs=[whole((2 * hs, 2 * cols))] * 4,
            out_specs=[anywhere] * 2,
            scratch_shapes=[pltpu.SemaphoreType.DMA((4 * chips,))],
        ),
        out_shape=[jax.ShapeDtypeStruct((hs, width), bf16)] * 2,
        compiler_params=vmem_limit(14),
        cost_estimate=cost(1 << 20, 8 * hs * width),
    )(place, *pieces)
    expert_gate = gu[None, :, :hs]
    expert_up = gu[None, :, hs:]
    return (
        expert_gate,
        expert_up,
        expert_down[None],
        shared_gate,
        shared_up,
        shared_down,
        mixed,
    )


def solution(mesh):
    placed = (
        P("fs", None),
        P("fs"),
        P(None, "fs", "tp"),
        P(None, "fs", "tp"),
        P(None, "fs", "tp"),
        P("fs", "tp"),
        P("fs", "tp"),
        P("fs", "tp"),
        P("fs", None),
        P("fs", None),
    )


    return jax.shard_map(
        on_device,
        mesh=mesh,
        in_specs=placed,
        out_specs=(
            P("fs", None, "tp"),
            P("fs", None, "tp"),
            P("fs", "tp", None),
            P(None, "tp"),
            P(None, "tp"),
            P("tp", None),
            P("fs", "tp"),
        ),
        check_vma=False,
    )
```
